256 devices in a mesh: grp: 2 (over z), st: 16 (over y, core), tp: 8 (over x).
Axes of the slice: x: 8, y: 8, z: 2, core: 2. Of those that a mesh axis runs over, the one named last changes fastest.
The devices are a block of a 8x8x16 slice.
Arguments:
- tokens: bfloat16 [8192, 2048], P(('grp', 'st')), parts along dimension 0, may hold values from -6 to 6
- pre_gain: float32 [2048], replicated, may hold values from 0.1 to 1.9
- w_gated: bfloat16 [2048, 1536], P(None, 'tp'), may hold values from -0.125 to 0.125
- w_mixed: bfloat16 [2048, 1536], P(None, 'tp'), may hold values from -0.125 to 0.125
- mix_weight: bfloat16 [8, 128, 128], P('tp'), may hold values from -0.5 to 0.5
- w_query: bfloat16 [2048, 1024], P(None, 'tp'), may hold values from -0.125 to 0.125
- w_gate_mix: bfloat16 [2048, 1536], P(None, 'tp'), may hold values from -0.125 to 0.125
- w_gate_read: bfloat16 [2048, 1024], P(None, 'tp'), may hold values from -0.125 to 0.125
- store: bfloat16 [256, 128, 2048], P(('grp', 'st')), parts along dimension 0, may hold values from -6 to 6
- mem_gain: float32 [2048], replicated, may hold values from 1 to 80
- w_key: bfloat16 [2048, 1024], P(None, 'tp'), may hold values from -0.125 to 0.125
- w_value: bfloat16 [2048, 1024], P(None, 'tp'), may hold values from -0.125 to 0.125
- passage_ids: int32 [128, 4], P(('grp', 'st')), parts along dimension 0, may hold values from 0 to 127, as said below
- w_out_mix: bfloat16 [1536, 2048], P('tp'), may hold values from -0.125 to 0.125
- w_out_read: bfloat16 [1024, 2048], P('tp'), may hold values from -0.125 to 0.125
Outputs:
- mixed_out: bfloat16 [8192, 2048], P(('grp', 'st', 'tp')), parts along dimension 0
The draws below stay inside these ranges and needn't reach their ends.
There are 2 independent parts, one for each index of `grp`. The reference program is written for one: setup_inputs(seed, part) draws one part's arguments, and reference() takes and returns one part's arrays. A program takes and returns all parts, laid end to end along the dimension named above; an argument that names none is the same for every part. Nothing has to cross between parts.
Inputs may be any that keep to these rules, and one draw needn't show every extreme that they name: `passage_ids`: passage p is held by index p // 8 of st. The 16 entries of one index of st name at most 2 passages held by any one index of st, and that most is reached in every draw.
All inputs are finite; a program needn't handle non-finite values.
Results may differ from the reference program's by a relative error of at most 0.015.
The reference program's roundings to bfloat16 on the way count: a program that leaves them out, or rounds other values in their place, can miss the bound.
Values may be sent and summed in bfloat16 or wider, within the bound.
A program may use at most 128 MiB of HBM per device.

```python
import jax
import jax.numpy as jnp
from jax import lax

D = 2048
GROUPS = 8
GW = 192
SW = 1536
XH = 8
HD = 128
XW = 1024
SPAN = 128
RBLOCK = 64
NPB = 4
PROWS = 128
PASS_DEV = 8
TOKENS = 4096
PASSAGES = 128
BLOCKS = 64
REQ = 16
CAP = 2
N_TP = 8


def draw_mem_gain(key, part):
    low_end = 1.0
    high_end = 4.0
    unit = jax.random.uniform(key, (D,), jnp.float32)
    return jnp.exp(jnp.log(low_end) + unit * (jnp.log(high_end) - jnp.log(low_end)))


def draw_passage_ids(key, part):
    readers = PASSAGES // PASS_DEV
    key_pop, key_rest = jax.random.split(jax.random.fold_in(key, 17))
    popular = jax.random.randint(key_pop, (readers,), 0, 4)
    slot_count = readers * CAP
    slot_owner = jnp.arange(slot_count, dtype=jnp.int32) // CAP
    slot_copy = jnp.arange(slot_count, dtype=jnp.int32) % CAP

    def one_reader(reader, reader_key):
        key_noise, key_left, key_right, key_order = jax.random.split(reader_key, 4)
        noise = jax.random.randint(key_noise, (slot_count,), 0, 64)
        score = popular[slot_owner] * 64 + noise
        before = slot_owner == (reader + readers - 1) % readers
        across = (slot_owner == (reader + readers // 2) % readers) & (slot_copy == 0)
        score = jnp.where(before | across, 100000, score)
        score = score * 4096 + jnp.arange(slot_count, dtype=jnp.int32)
        ranking = jnp.argsort(-score, stable=True)
        chosen = slot_owner[ranking[:REQ]]
        within = jnp.minimum(jax.random.randint(key_left, (REQ,), 0, PASS_DEV), jax.random.randint(key_right, (REQ,), 0, PASS_DEV))
        picked = (chosen * PASS_DEV + within).astype(jnp.int32)
        return picked[jax.random.permutation(key_order, REQ)]
    reader_keys = jax.random.split(key_rest, readers)
    every = jax.vmap(one_reader)(jnp.arange(readers, dtype=jnp.int32), reader_keys)
    return every.reshape(BLOCKS, NPB).astype(jnp.int32)


def block_levels(rng, shape, cuts, low, top_value):
    def one(position, parts):
        draws = jax.random.uniform(jax.random.fold_in(jax.random.fold_in(rng, 6), position), (parts,), jnp.float32, low / len(cuts), top_value / len(cuts))
        return jnp.repeat(jnp.exp(draws), shape[position] // parts).reshape((-1,) + (1,) * (len(shape) - position - 1))

    loudness = one(*cuts[0])
    for cut in cuts[1:]:
        loudness = loudness * one(*cut)
    return loudness


def gaussian(key, extent, scale, bound, pieces=(), held_as=jnp.bfloat16):
    result = scale * jax.random.normal(key, extent, jnp.float32)
    if pieces:
        result = result * block_levels(key, extent, pieces, -0.22, 0.18)
    return jnp.clip(result, -bound, bound).astype(held_as)


def setup_inputs(seed: int = 0, part: int = 0) -> dict:
    key_list = jax.random.split(jax.random.key(seed), 16)
    part_keys = jax.random.split(jax.random.fold_in(key_list[15], part), 16)
    tokens = gaussian(part_keys[0], (TOKENS, D), 1.0, 6.0, ((0, 16),))
    pre_gain = jnp.clip(1.0 + 0.18 * jax.random.normal(key_list[1], (D,), jnp.float32), 0.1, 1.9)
    w_gated = gaussian(key_list[2], (D, SW), D ** -0.5, 0.125, ((1, 8),))
    w_mixed = gaussian(key_list[3], (D, SW), D ** -0.5, 0.125, ((1, 8),))
    mix_weight = gaussian(key_list[4], (GROUPS, SPAN, SPAN), SPAN ** -0.5, 0.5, ((0, 8),))
    w_query = gaussian(key_list[5], (D, XW), D ** -0.5, 0.125, ((1, 8),))
    w_gate_mix = gaussian(key_list[6], (D, SW), D ** -0.5, 0.125, ((1, 8),))
    w_gate_read = gaussian(key_list[7], (D, XW), D ** -0.5, 0.125, ((1, 8),))
    store = gaussian(part_keys[8], (PASSAGES, PROWS, D), 1.0, 6.0, ((0, 16),))
    mem_gain = draw_mem_gain(jax.random.fold_in(key_list[15], 71), part)
    w_key = gaussian(key_list[10], (D, XW), D ** -0.5, 0.125, ((1, 8),))
    w_value = gaussian(key_list[11], (D, XW), D ** -0.5, 0.125, ((1, 8),))
    passage_ids = draw_passage_ids(jax.random.fold_in(jax.random.fold_in(key_list[15], part), 71), part)
    w_out_mix = gaussian(key_list[13], (SW, D), (SW + XW) ** -0.5, 0.125, ((0, 8),))
    w_out_read = gaussian(key_list[14], (XW, D), (SW + XW) ** -0.5, 0.125, ((0, 8),))
    return dict(tokens=tokens, pre_gain=pre_gain, w_gated=w_gated, w_mixed=w_mixed, mix_weight=mix_weight, w_query=w_query, w_gate_mix=w_gate_mix, w_gate_read=w_gate_read, store=store, mem_gain=mem_gain, w_key=w_key, w_value=w_value, passage_ids=passage_ids, w_out_mix=w_out_mix, w_out_read=w_out_read)


eps = 1e-06

def reference(tokens, pre_gain, w_gated, w_mixed, mix_weight, w_query, w_gate_mix, w_gate_read, store, mem_gain, w_key, w_value, passage_ids, w_out_mix, w_out_read):
    inputs = tokens.astype(jnp.float32)
    normed = (inputs * lax.rsqrt(lax.optimization_barrier(jnp.mean(inputs * inputs, axis=-1, keepdims=True)) + eps) * pre_gain).astype(jnp.bfloat16)
    gated = jnp.dot(normed, w_gated, preferred_element_type=jnp.float32)
    mixed_in = jnp.dot(normed, w_mixed, preferred_element_type=jnp.float32)
    grouped = mixed_in.reshape(TOKENS, GROUPS, GW)
    group_mean = lax.optimization_barrier(jnp.mean(grouped, axis=-1, keepdims=True))
    centred = grouped - group_mean
    group_var = lax.optimization_barrier(jnp.mean(centred * centred, axis=-1, keepdims=True))
    mixed_norm = (centred * lax.rsqrt(group_var + eps)).astype(jnp.bfloat16)
    causal = jnp.tril(jnp.ones((SPAN, SPAN), dtype=bool))
    mix_masked = jnp.where(causal[None], mix_weight.astype(jnp.float32), 0.0)
    blocked = mixed_norm.reshape(TOKENS // SPAN, SPAN, GROUPS, GW).astype(jnp.float32)
    spatial = jnp.einsum('hts,nshd->nthd', mix_masked, blocked).reshape(TOKENS, SW)
    branch_mix = gated * spatial
    query = jnp.dot(normed, w_query, preferred_element_type=jnp.float32).astype(jnp.bfloat16)
    read_rows = store[passage_ids.reshape(-1)].astype(jnp.float32)
    passage_norm = (read_rows * lax.rsqrt(lax.optimization_barrier(jnp.mean(read_rows * read_rows, axis=-1, keepdims=True)) + eps) * mem_gain).astype(jnp.bfloat16)
    flat_rows = passage_norm.reshape(-1, D)
    keys = jnp.dot(flat_rows, w_key, preferred_element_type=jnp.float32).astype(jnp.bfloat16).reshape(BLOCKS, NPB * PROWS, XH, HD)
    values = jnp.dot(flat_rows, w_value, preferred_element_type=jnp.float32).astype(jnp.bfloat16).reshape(BLOCKS, NPB * PROWS, XH, HD)
    query_blocks = query.reshape(BLOCKS, RBLOCK, XH, HD).astype(jnp.float32)
    scores = jnp.einsum('btha,bkha->bhtk', query_blocks, keys.astype(jnp.float32)) * HD ** (-0.5)
    probs = jax.nn.softmax(scores, axis=-1).astype(jnp.bfloat16)
    branch_read = jnp.einsum('bhtk,bkha->btha', probs.astype(jnp.float32), values.astype(jnp.float32)).reshape(TOKENS, XW)
    gate_mix = jnp.dot(normed, w_gate_mix, preferred_element_type=jnp.float32)
    gate_read = jnp.dot(normed, w_gate_read, preferred_element_type=jnp.float32)
    out_mix = (branch_mix * jax.nn.silu(gate_mix)).astype(jnp.bfloat16)
    out_read = (branch_read * jax.nn.silu(gate_read)).astype(jnp.bfloat16)
    mix_cols = SW // N_TP
    read_cols = XW // N_TP
    total = jnp.zeros((TOKENS, D), jnp.float32)
    for shard in range(N_TP):
        partial_value = jnp.dot(out_mix[:, shard * mix_cols:(shard + 1) * mix_cols], w_out_mix[shard * mix_cols:(shard + 1) * mix_cols], preferred_element_type=jnp.float32)
        partial_value = partial_value + jnp.dot(out_read[:, shard * read_cols:(shard + 1) * read_cols], w_out_read[shard * read_cols:(shard + 1) * read_cols], preferred_element_type=jnp.float32)
        total = total + lax.optimization_barrier(partial_value.astype(jnp.bfloat16)).astype(jnp.float32)
    return total.astype(jnp.bfloat16)
```

```python
import functools

import jax
import jax.numpy as jnp
from jax import lax
from jax.experimental import pallas as pl
from jax.experimental.pallas import tpu as pltpu
from jax.sharding import PartitionSpec as P

HD = 128
SPAN = 128
RBLOCK = 64
NPB = 4
PROWS = 128
NORM_ROWS = 32
PIECES = 4

MESH = pl.DeviceIdType.MESH
eps = 1e-06
F32 = jnp.float32
BF16 = jnp.bfloat16


def dot(a, b, dims=((1,), (0,))):
    return lax.dot_general(a, b, (dims, ((), ())), preferred_element_type=F32)


def row_norm(source, gain, target, rows):
    def some(i, carry):
        at = pl.ds(pl.multiple_of(i * NORM_ROWS, NORM_ROWS), NORM_ROWS)
        wide = source[at, :].astype(F32)
        scale = lax.rsqrt(jnp.mean(wide * wide, axis=-1, keepdims=True) + eps)
        target[at, :] = (wide * scale * gain).astype(BF16)
        return carry

    lax.fori_loop(0, rows // NORM_ROWS, some, 0)


def kernel(
    n_st,
    n_tp,
    tokens,
    pre_gain,
    w_gated,
    w_mixed,
    mix_weight,
    w_query,
    w_gate_mix,
    w_gate_read,
    store,
    mem_gain,
    w_key,
    w_value,
    ids,
    w_out_mix,
    w_out_read,
    out,
    tok,
    normed,
    wg,
    wm,
    wgm,
    mixw,
    wq,
    wgr,
    wkv,
    wom,
    wor,
    rows_in,
    rows_norm,
    key_of,
    value_of,
    q_ring,
    q_sib,
    ids_all,
    o_send,
    s_send,
    ret_o,
    ret_s,
    gate_t,
    out_mix,
    out_read,
    part,
    rs_send,
    rs_recv,
    in_sem,
    row_sem,
    ids_send_sem,
    ids_recv_sem,
    ring_send_sem,
    ring_recv_sem,
    sib_send_sem,
    sib_recv_sem,
    ret_send_sem,
    ret_recv_sem,
    stat_send_sem,
    stat_recv_sem,
    rs_send_sem,
    rs_recv_sem,
):
    grp, st, tp = lax.axis_index("grp"), lax.axis_index("st"), lax.axis_index("tp")
    n_y = n_st // 2
    half_y, half_tp = n_y // 2, n_tp // 2
    y, core = st // 2, lax.rem(st, 2)
    count = tok.shape[0]
    blocks = count // RBLOCK
    per_owner = rows_in.shape[0]
    mine_rows = count // n_tp

    def at_y(offset, sibling=False):
        chip = lax.rem(y + offset + n_y, n_y)
        return chip * 2 + (1 - core if sibling else core)

    def along_tp(offset):
        return lax.rem(tp + offset + n_tp, n_tp)

    barrier = pltpu.get_barrier_semaphore()
    peers = [(grp, lax.rem(st + k, n_st), tp) for k in range(1, n_st)]
    sides = [1, -1] if n_tp > 2 else [1]
    peers += [(grp, st, along_tp(k)) for k in sides]
    for peer in peers:
        pl.semaphore_signal(barrier, inc=1, device_id=peer, device_id_type=MESH)

    def fetch(k, source, target):
        copy = pltpu.make_async_copy(source, target, in_sem.at[k])
        copy.start()
        return copy

    got_tok = fetch(0, tokens, tok)
    got_wq = fetch(1, w_query, wq)
    got_wk = fetch(2, w_key, wkv.at[:, 0:HD])
    got_wv = fetch(3, w_value, wkv.at[:, HD : 2 * HD])
    got_rows = []
    for p in range(per_owner):
        copy = pltpu.make_async_copy(store.at[p], rows_in.at[p], row_sem.at[p])
        copy.start()
        got_rows.append(copy)
    got_wm = fetch(4, w_mixed, wm)
    got_wg = fetch(5, w_gated, wg)
    got_wgm = fetch(6, w_gate_mix, wgm)
    got_wgr = fetch(7, w_gate_read, wgr)
    got_mixw = fetch(8, mix_weight.at[0], mixw)
    got_wom = fetch(9, w_out_mix, wom)
    got_wor = fetch(10, w_out_read, wor)

    got_tok.wait()
    row_norm(tok, pre_gain[...].reshape(1, -1), normed, count)
    got_wq.wait()
    own_q = dot(normed[...], wq[...]).astype(BF16)
    q_ring[0][...] = own_q.reshape(blocks, RBLOCK, HD)

    pl.semaphore_wait(barrier, len(peers))

    id_copies = []
    for k in range(1, n_st):
        copy = pltpu.make_async_remote_copy(
            ids, ids_all.at[st], ids_send_sem.at[k], ids_recv_sem.at[k],
            device_id=(grp, lax.rem(st + k, n_st), tp), device_id_type=MESH,
        )
        copy.start()
        id_copies.append(copy)
    for b in range(blocks):
        for n in range(NPB):
            ids_all[st, b, n] = ids[b, n]

    cut = blocks // 2
    ring_copies, sib_copies = {}, {}

    def push(j, h, up):
        after = j + 1 if up else (j - 1) % n_y
        piece = pl.ds(h * cut, cut)
        copy = pltpu.make_async_remote_copy(
            q_ring[j].at[piece], q_ring[after].at[piece],
            ring_send_sem.at[after, h], ring_recv_sem.at[after, h],
            device_id=(grp, at_y(1 if up else -1), tp), device_id_type=MESH,
        )
        copy.start()
        ring_copies[after, h] = copy

    def across(j, h):
        piece = pl.ds(h * cut, cut)
        copy = pltpu.make_async_remote_copy(
            q_ring[j].at[piece], q_sib[j].at[piece],
            sib_send_sem.at[j, h], sib_recv_sem.at[j, h],
            device_id=(grp, at_y(0, True), tp), device_id_type=MESH,
        )
        copy.start()
        sib_copies[j, h] = copy

    def onward(j, h):
        if j < half_y and (j + 1 < half_y or h == 0):
            push(j, h, True)
        if (j == 0 or j > half_y) and (n_y - 1 if j == 0 else j - 1) >= half_y:
            if (n_y - 1 if j == 0 else j - 1) > half_y or h == 1:
                push(j, h, False)

    def arrive(k):
        for h in range(2):
            for j in sorted({k, n_y - k}):
                if k == half_y or True:
                    ring_copies[j, h].wait_recv()
                    if j != half_y:
                        onward(j, h)
                    across(j, h)

    for h in range(2):
        onward(0, h)
    for h in range(2):
        across(0, h)

    got_wk.wait()
    got_wv.wait()
    mem_row = mem_gain[...].reshape(1, -1)

    def keys_of(low, high):
        def one(p, carry):
            pltpu.make_async_copy(store.at[p], rows_in.at[p], row_sem.at[p]).wait()
            row_norm(rows_in.at[p], mem_row, rows_norm, PROWS)
            both = dot(rows_norm[...], wkv[...])
            key_of[p] = both[:, :HD].astype(BF16)
            value_of[p] = jnp.transpose(both[:, HD:]).astype(BF16)
            return carry

        lax.fori_loop(low, high, one, 0)

    lanes = lax.broadcasted_iota(jnp.int32, (1, 2 * RBLOCK), 1)
    first_half = lanes < RBLOCK

    def slots_of(reader):
        p0 = p1 = b0 = b1 = seen = jnp.int32(0)
        for b in range(blocks):
            for n in range(NPB):
                local = ids_all[reader, b, n] - st * per_owner
                mine = (local >= 0) & (local < per_owner)
                is0 = mine & (seen == 0)
                is1 = mine & (seen == 1)
                p0, b0 = jnp.where(is0, local, p0), jnp.where(is0, b, b0)
                p1, b1 = jnp.where(is1, local, p1), jnp.where(is1, b, b1)
                seen = seen + jnp.where(mine, 1, 0)
        return p0, p1, b0, b1

    def attend(q_ref, reader):
        p0, p1, b0, b1 = slots_of(reader)
        q = jnp.concatenate([q_ref[b0], q_ref[b1]], axis=0)
        over_keys = ((1,), (1,))
        scores = jnp.where(
            first_half, dot(key_of[p0], q, over_keys), dot(key_of[p1], q, over_keys)
        ) * (HD ** (-0.5))
        top = jnp.max(scores, axis=0, keepdims=True)
        weight = jnp.exp(scores - top)
        total = jnp.sum(weight, axis=0, keepdims=True)
        weight = weight.astype(BF16)
        read = jnp.where(first_half, dot(value_of[p0], weight), dot(value_of[p1], weight))
        return read.astype(BF16), jnp.concatenate([top, total], axis=0)

    ret_copies = []

    def serve(j, sibling):
        reader = at_y(-j, sibling)
        read, stats = attend(q_sib[j] if sibling else q_ring[j], reader)
        if j == 0 and not sibling:
            ret_o[st] = read
            ret_s[st] = stats
            return
        label = j * 2 + (1 if sibling else 0)
        o_send[label] = read
        s_send[label] = stats
        for source, target, send, recv in (
            (o_send, ret_o, ret_send_sem, ret_recv_sem),
            (s_send, ret_s, stat_send_sem, stat_recv_sem),
        ):
            copy = pltpu.make_async_remote_copy(
                source.at[label], target.at[st], send.at[label], recv.at[label],
                device_id=(grp, reader, tp), device_id_type=MESH,
            )
            copy.start()
            ret_copies.append(copy)

    def serve_pair(j):
        serve(j, False)
        for h in range(2):
            sib_copies[j, h].wait_recv()
        serve(j, True)

    half_owner = per_owner // 2
    keys_of(0, half_owner)
    if half_y > 1:
        arrive(1)
    keys_of(half_owner, per_owner)
    for copy in id_copies:
        copy.wait_recv()
    for k in range(1, half_y + 1):
        if k > 1 or half_y == 1:
            arrive(k)
        if k == 1:
            serve_pair(0)
        else:
            for j in sorted({k - 1, n_y - k + 1}):
                serve_pair(j)
    serve_pair(half_y)

    got_wm.wait()
    mixed_in = dot(normed[...], wm[...])
    centred = mixed_in - jnp.mean(mixed_in, axis=-1, keepdims=True)
    variance = jnp.mean(centred * centred, axis=-1, keepdims=True)
    mixed_norm = (centred * lax.rsqrt(variance + eps)).astype(BF16)
    got_mixw.wait()
    row_at = lax.broadcasted_iota(jnp.int32, (SPAN, SPAN), 0)
    col_at = lax.broadcasted_iota(jnp.int32, (SPAN, SPAN), 1)
    causal = jnp.where(col_at <= row_at, mixw[...].astype(F32), 0.0).astype(BF16)
    spatial = jnp.concatenate(
        [dot(causal, mixed_norm[n * SPAN : (n + 1) * SPAN]) for n in range(count // SPAN)], axis=0
    )
    got_wg.wait()
    branch_mix = dot(normed[...], wg[...]) * spatial
    got_wgm.wait()
    gate = dot(normed[...], wgm[...])
    out_mix[...] = (branch_mix * (gate / (1.0 + jnp.exp(-gate)))).astype(BF16)
    got_wgr.wait()
    gate = dot(normed[...], wgr[...])
    gate_t[...] = jnp.transpose(gate / (1.0 + jnp.exp(-gate)))
    got_wom.wait()
    width = part.shape[2]
    for c in range(PIECES):
        part[c] = dot(out_mix[...], wom[:, c * width : (c + 1) * width])

    owners, ranks = [], []
    for e in range(blocks * NPB):
        owner = ids[e // NPB, e % NPB] // per_owner
        rank = jnp.int32(0)
        for before in owners:
            rank = rank + jnp.where(before == owner, 1, 0)
        owners.append(owner)
        ranks.append(rank)
    for copy in ret_copies:
        copy.wait_recv()
    got_wor.wait()
    for pair in range(blocks // 2):
        tops, totals, reads = [], [], []
        for n in range(NPB):
            e0, e1 = pair * 2 * NPB + n, (pair * 2 + 1) * NPB + n

            def placed(ref):
                x0, x1 = ref[owners[e0]].astype(F32), ref[owners[e1]].astype(F32)
                low = jnp.where(ranks[e0] == 0, x0, pltpu.roll(x0, RBLOCK, 1))
                high = jnp.where(ranks[e1] == 1, x1, pltpu.roll(x1, RBLOCK, 1))
                return jnp.where(first_half, low, high)

            stats = placed(ret_s)
            tops.append(stats[0:1])
            totals.append(stats[1:2])
            reads.append(placed(ret_o))
        top = functools.reduce(jnp.maximum, tops)
        scales = [jnp.exp(t - top) for t in tops]
        total = sum(s * t for s, t in zip(scales, totals))
        read = sum(s * r for s, r in zip(scales, reads)) / total
        cols = slice(pair * 2 * RBLOCK, (pair + 1) * 2 * RBLOCK)
        out_read[cols, :] = jnp.transpose(read * gate_t[:, cols]).astype(BF16)

    rs_copies = {}

    def pass_on(c, d, k):
        sign = 1 - 2 * d
        target = along_tp(sign * k)
        lo = 0
        size = mine_rows
        if k == half_tp:
            size = mine_rows // 2
            lo = d * size
        start = pl.multiple_of(target * mine_rows + lo, mine_rows // 2)
        value = part[c, pl.ds(start, size), :]
        if k == half_tp:
            rs_send[d, k - 1, c, lo : lo + size, :] = value.astype(BF16)
        else:
            rs_copies[c, d, k + 1].wait_recv()
            if k + 1 == half_tp:
                cut_rows = mine_rows // 2
                low = d * cut_rows
                rs_send[d, k - 1, c, low : low + cut_rows, :] = (
                    part[c, pl.ds(pl.multiple_of(target * mine_rows + low, cut_rows), cut_rows), :]
                    + rs_recv[d, k, c, low : low + cut_rows, :].astype(F32)
                ).astype(BF16)
                other = cut_rows - low
                rs_send[d, k - 1, c, other : other + cut_rows, :] = part[
                    c, pl.ds(pl.multiple_of(target * mine_rows + other, cut_rows), cut_rows), :
                ].astype(BF16)
            else:
                rs_send[d, k - 1, c] = (value + rs_recv[d, k, c].astype(F32)).astype(BF16)
        copy = pltpu.make_async_remote_copy(
            rs_send.at[d, k - 1, c, pl.ds(lo, size)], rs_recv.at[d, k - 1, c, pl.ds(lo, size)],
            rs_send_sem.at[d, k - 1, c], rs_recv_sem.at[d, k - 1, c],
            device_id=(grp, st, along_tp(sign)), device_id_type=MESH,
        )
        copy.start()
        rs_copies[c, d, k] = copy

    for c in range(PIECES):
        part[c] = part[c] + dot(out_read[...], wor[:, c * width : (c + 1) * width])
        for d in range(2):
            pass_on(c, d, half_tp)
    for k in range(half_tp - 1, 0, -1):
        for c in range(PIECES):
            for d in range(2):
                pass_on(c, d, k)
    here = pl.ds(pl.multiple_of(tp * mine_rows, mine_rows), mine_rows)
    for c in range(PIECES):
        for d in range(2):
            rs_copies[c, d, 1].wait_recv()
        if half_tp == 1:
            cut_rows = mine_rows // 2
            both = jnp.concatenate(
                [rs_recv[0, 0, c, :cut_rows, :], rs_recv[1, 0, c, cut_rows:, :]], axis=0
            ).astype(F32)
        else:
            both = rs_recv[0, 0, c].astype(F32) + rs_recv[1, 0, c].astype(F32)
        out[:, c * width : (c + 1) * width] = (part[c, here, :] + both).astype(BF16)

    for copy in (
        id_copies + list(ring_copies.values()) + list(sib_copies.values())
        + ret_copies + list(rs_copies.values())
    ):
        copy.wait_send()


def local(*args, n_st, n_tp):
    tokens, w_gated, store = args[0], args[2], args[8]
    count, width = tokens.shape
    mix_width = w_gated.shape[1]
    held = store.shape[0]
    blocks = count // RBLOCK
    n_y = n_st // 2
    mine_rows = count // n_tp
    hbm = pl.BlockSpec(memory_space=pltpu.HBM)
    vmem = pl.BlockSpec(memory_space=pltpu.VMEM)
    smem = pl.BlockSpec(memory_space=pltpu.SMEM)
    specs = [hbm] * 15
    specs[1] = specs[9] = vmem
    specs[12] = smem
    dma = pltpu.SemaphoreType.DMA
    columns = width // PIECES
    scratch = dict(
        tok=pltpu.VMEM((count, width), BF16),
        normed=pltpu.VMEM((count, width), BF16),
        wg=pltpu.VMEM((width, mix_width), BF16),
        wm=pltpu.VMEM((width, mix_width), BF16),
        wgm=pltpu.VMEM((width, mix_width), BF16),
        mixw=pltpu.VMEM((SPAN, SPAN), BF16),
        wq=pltpu.VMEM((width, HD), BF16),
        wgr=pltpu.VMEM((width, HD), BF16),
        wkv=pltpu.VMEM((width, 2 * HD), BF16),
        wom=pltpu.VMEM((mix_width, width), BF16),
        wor=pltpu.VMEM((HD, width), BF16),
        rows_in=pltpu.VMEM((held, PROWS, width), BF16),
        rows_norm=pltpu.VMEM((PROWS, width), BF16),
        key_of=pltpu.VMEM((held, PROWS, HD), BF16),
        value_of=pltpu.VMEM((held, HD, PROWS), BF16),
        q_ring=[pltpu.VMEM((blocks, RBLOCK, HD), BF16) for _ in range(n_y)],
        q_sib=[pltpu.VMEM((blocks, RBLOCK, HD), BF16) for _ in range(n_y)],
        ids_all=pltpu.SMEM((n_st, blocks, NPB), jnp.int32),
        o_send=pltpu.VMEM((n_st, HD, 2 * RBLOCK), BF16),
        s_send=pltpu.VMEM((n_st, 2, 2 * RBLOCK), F32),
        ret_o=pltpu.VMEM((n_st, HD, 2 * RBLOCK), BF16),
        ret_s=pltpu.VMEM((n_st, 2, 2 * RBLOCK), F32),
        gate_t=pltpu.VMEM((HD, count), F32),
        out_mix=pltpu.VMEM((count, mix_width), BF16),
        out_read=pltpu.VMEM((count, HD), BF16),
        part=pltpu.VMEM((PIECES, count, columns), F32),
        rs_send=pltpu.VMEM((2, n_tp // 2, PIECES, mine_rows, columns), BF16),
        rs_recv=pltpu.VMEM((2, n_tp // 2, PIECES, mine_rows, columns), BF16),
        in_sem=dma((11,)),
        row_sem=dma((held,)),
        ids_send_sem=dma((n_st,)),
        ids_recv_sem=dma((n_st,)),
        ring_send_sem=dma((n_y, 2)),
        ring_recv_sem=dma((n_y, 2)),
        sib_send_sem=dma((n_y, 2)),
        sib_recv_sem=dma((n_y, 2)),
        ret_send_sem=dma((n_st,)),
        ret_recv_sem=dma((n_st,)),
        stat_send_sem=dma((n_st,)),
        stat_recv_sem=dma((n_st,)),
        rs_send_sem=dma((2, n_tp // 2, PIECES)),
        rs_recv_sem=dma((2, n_tp // 2, PIECES)),
    )
    names = list(scratch)

    def body(*refs):
        kernel(n_st, n_tp, *refs[:16], **dict(zip(names, refs[16:])))

    return pl.pallas_call(
        body,
        out_shape=jax.ShapeDtypeStruct((mine_rows, width), BF16),
        in_specs=specs,
        out_specs=vmem,
        scratch_shapes=list(scratch.values()),
        compiler_params=pltpu.CompilerParams(
            collective_id=0, has_side_effects=True, vmem_limit_bytes=48 * 1024 * 1024
        ),
        name="layer",
    )(*args)


def solution(mesh):
    placed = (
        P(("grp", "st"), None),
        P(),
        P(None, "tp"),
        P(None, "tp"),
        P("tp", None, None),
        P(None, "tp"),
        P(None, "tp"),
        P(None, "tp"),
        P(("grp", "st"), None, None),
        P(),
        P(None, "tp"),
        P(None, "tp"),
        P(("grp", "st"), None),
        P("tp", None),
        P("tp", None),
    )
    body = functools.partial(local, n_st=mesh.shape["st"], n_tp=mesh.shape["tp"])
    return jax.shard_map(
        body, mesh=mesh, in_specs=placed, out_specs=P(("grp", "st", "tp"), None), check_vma=False
    )
```

```python
import functools

import jax
import jax.numpy as jnp
from jax import lax
from jax.experimental import pallas as pl
from jax.experimental.pallas import tpu as pltpu
from jax.sharding import PartitionSpec as P

HD = 128
SPAN = 128
RBLOCK = 64
NPB = 4
PROWS = 128
NORM_ROWS = 32
PIECES = 4

MESH = pl.DeviceIdType.MESH
eps = 1e-06
F32 = jnp.float32
BF16 = jnp.bfloat16


def dot(a, b, dims=((1,), (0,))):
    return lax.dot_general(a, b, (dims, ((), ())), preferred_element_type=F32)


def row_norm(source, gain, target, rows):
    def some(i, carry):
        at = pl.ds(pl.multiple_of(i * NORM_ROWS, NORM_ROWS), NORM_ROWS)
        wide = source[at, :].astype(F32)
        scale = lax.rsqrt(jnp.mean(wide * wide, axis=-1, keepdims=True) + eps)
        target[at, :] = (wide * scale * gain).astype(BF16)
        return carry

    lax.fori_loop(0, rows // NORM_ROWS, some, 0)


def kernel(
    n_st,
    n_tp,
    tokens,
    pre_gain,
    w_gated,
    w_mixed,
    mix_weight,
    w_query,
    w_gate_mix,
    w_gate_read,
    store,
    mem_gain,
    w_key,
    w_value,
    ids,
    w_out_mix,
    w_out_read,
    out,
    tok,
    normed,
    wg,
    wm,
    wgm,
    mixw,
    wq,
    wgr,
    wkv,
    wom,
    wor,
    rows_in,
    rows_norm,
    key_of,
    value_of,
    q_ring,
    q_sib,
    ids_all,
    o_send,
    s_send,
    ret_o,
    ret_s,
    gate_t,
    out_mix,
    out_read,
    part,
    rs_send,
    rs_recv,
    in_sem,
    row_sem,
    ids_send_sem,
    ids_recv_sem,
    ring_send_sem,
    ring_recv_sem,
    sib_send_sem,
    sib_recv_sem,
    ret_send_sem,
    ret_recv_sem,
    stat_send_sem,
    stat_recv_sem,
    rs_send_sem,
    rs_recv_sem,
):
    grp, st, tp = lax.axis_index("grp"), lax.axis_index("st"), lax.axis_index("tp")
    n_y = n_st // 2
    half_y, half_tp = n_y // 2, n_tp // 2
    y, core = st // 2, lax.rem(st, 2)
    count = tok.shape[0]
    blocks = count // RBLOCK
    per_owner = rows_in.shape[0]
    mine_rows = count // n_tp

    def at_y(offset, sibling=False):
        chip = lax.rem(y + offset + n_y, n_y)
        return chip * 2 + (1 - core if sibling else core)

    def along_tp(offset):
        return lax.rem(tp + offset + n_tp, n_tp)

    barrier = pltpu.get_barrier_semaphore()
    peers = [(grp, lax.rem(st + k, n_st), tp) for k in range(1, n_st)]
    sides = [1, -1] if n_tp > 2 else [1]
    peers += [(grp, st, along_tp(k)) for k in sides]
    for peer in peers:
        pl.semaphore_signal(barrier, inc=1, device_id=peer, device_id_type=MESH)

    def fetch(k, source, target):
        copy = pltpu.make_async_copy(source, target, in_sem.at[k])
        copy.start()
        return copy

    got_tok = fetch(0, tokens, tok)
    got_wq = fetch(1, w_query, wq)
    got_wk = fetch(2, w_key, wkv.at[:, 0:HD])
    got_wv = fetch(3, w_value, wkv.at[:, HD : 2 * HD])
    got_rows = []
    for p in range(per_owner):
        copy = pltpu.make_async_copy(store.at[p], rows_in.at[p], row_sem.at[p])
        copy.start()
        got_rows.append(copy)
    got_wm = fetch(4, w_mixed, wm)
    got_wg = fetch(5, w_gated, wg)
    got_wgm = fetch(6, w_gate_mix, wgm)
    got_wgr = fetch(7, w_gate_read, wgr)
    got_mixw = fetch(8, mix_weight.at[0], mixw)
    got_wom = fetch(9, w_out_mix, wom)
    got_wor = fetch(10, w_out_read, wor)

    got_tok.wait()
    row_norm(tok, pre_gain[...].reshape(1, -1), normed, count)
    got_wq.wait()
    own_q = dot(normed[...], wq[...]).astype(BF16)
    q_ring[0][...] = own_q.reshape(blocks, RBLOCK, HD)

    pl.semaphore_wait(barrier, len(peers))

    id_copies = []
    for k in range(1, n_st):
        copy = pltpu.make_async_remote_copy(
            ids, ids_all.at[st], ids_send_sem.at[k], ids_recv_sem.at[k],
            device_id=(grp, lax.rem(st + k, n_st), tp), device_id_type=MESH,
        )
        copy.start()
        id_copies.append(copy)
    for b in range(blocks):
        for n in range(NPB):
            ids_all[st, b, n] = ids[b, n]

    cut = blocks // 2
    ring_copies, sib_copies = {}, {}

    def push(j, h, up):
        after = j + 1 if up else (j - 1) % n_y
        piece = pl.ds(h * cut, cut)
        copy = pltpu.make_async_remote_copy(
            q_ring[j].at[piece], q_ring[after].at[piece],
            ring_send_sem.at[after, h], ring_recv_sem.at[after, h],
            device_id=(grp, at_y(1 if up else -1), tp), device_id_type=MESH,
        )
        copy.start()
        ring_copies[after, h] = copy

    def across(j, h):
        piece = pl.ds(h * cut, cut)
        copy = pltpu.make_async_remote_copy(
            q_ring[j].at[piece], q_sib[j].at[piece],
            sib_send_sem.at[j, h], sib_recv_sem.at[j, h],
            device_id=(grp, at_y(0, True), tp), device_id_type=MESH,
        )
        copy.start()
        sib_copies[j, h] = copy

    def onward(j, h):
        if j < half_y and (j + 1 < half_y or h == 0):
            push(j, h, True)
        if (j == 0 or j > half_y) and (n_y - 1 if j == 0 else j - 1) >= half_y:
            if (n_y - 1 if j == 0 else j - 1) > half_y or h == 1:
                push(j, h, False)

    def arrive(k):
        for h in range(2):
            for j in sorted({k, n_y - k}):
                ring_copies[j, h].wait_recv()
                if j != half_y:
                    onward(j, h)
                across(j, h)

    for h in range(2):
        onward(0, h)
    for h in range(2):
        across(0, h)

    got_wk.wait()
    got_wv.wait()
    mem_row = mem_gain[...].reshape(1, -1)

    def keys_of(low, high):
        def one(p, carry):
            pltpu.make_async_copy(store.at[p], rows_in.at[p], row_sem.at[p]).wait()
            row_norm(rows_in.at[p], mem_row, rows_norm, PROWS)
            both = dot(rows_norm[...], wkv[...])
            key_of[p] = both[:, :HD].astype(BF16)
            value_of[p] = jnp.transpose(both[:, HD:]).astype(BF16)
            return carry

        lax.fori_loop(low, high, one, 0)

    lanes = lax.broadcasted_iota(jnp.int32, (1, 2 * RBLOCK), 1)
    first_half = lanes < RBLOCK

    def slots_of(reader):
        p0 = p1 = b0 = b1 = seen = jnp.int32(0)
        for b in range(blocks):
            for n in range(NPB):
                local = ids_all[reader, b, n] - st * per_owner
                mine = (local >= 0) & (local < per_owner)
                is0 = mine & (seen == 0)
                is1 = mine & (seen == 1)
                p0, b0 = jnp.where(is0, local, p0), jnp.where(is0, b, b0)
                p1, b1 = jnp.where(is1, local, p1), jnp.where(is1, b, b1)
                seen = seen + jnp.where(mine, 1, 0)
        return p0, p1, b0, b1

    def attend(q_ref, reader):
        p0, p1, b0, b1 = slots_of(reader)
        q = jnp.concatenate([q_ref[b0], q_ref[b1]], axis=0)
        over_keys = ((1,), (1,))
        scores = jnp.where(
            first_half, dot(key_of[p0], q, over_keys), dot(key_of[p1], q, over_keys)
        ) * (HD ** (-0.5))
        top = jnp.max(scores, axis=0, keepdims=True)
        weight = jnp.exp(scores - top)
        total = jnp.sum(weight, axis=0, keepdims=True)
        weight = weight.astype(BF16)
        read = jnp.where(first_half, dot(value_of[p0], weight), dot(value_of[p1], weight))
        return read.astype(BF16), jnp.concatenate([top, total], axis=0)

    ret_copies = []

    def serve(j, sibling):
        reader = at_y(-j, sibling)
        read, stats = attend(q_sib[j] if sibling else q_ring[j], reader)
        if j == 0 and not sibling:
            ret_o[st] = read
            ret_s[st] = stats
            return
        label = j * 2 + (1 if sibling else 0)
        o_send[label] = read
        s_send[label] = stats
        for source, target, send, recv in (
            (o_send, ret_o, ret_send_sem, ret_recv_sem),
            (s_send, ret_s, stat_send_sem, stat_recv_sem),
        ):
            copy = pltpu.make_async_remote_copy(
                source.at[label], target.at[st], send.at[label], recv.at[label],
                device_id=(grp, reader, tp), device_id_type=MESH,
            )
            copy.start()
            ret_copies.append(copy)

    def serve_pair(j):
        serve(j, False)
        for h in range(2):
            sib_copies[j, h].wait_recv()
        serve(j, True)

    half_owner = per_owner // 2
    keys_of(0, half_owner)
    if half_y > 1:
        arrive(1)
    keys_of(half_owner, per_owner)
    for copy in id_copies:
        copy.wait_recv()
    for k in range(1, half_y + 1):
        if k > 1 or half_y == 1:
            arrive(k)
        if k == 1:
            serve_pair(0)
        else:
            for j in sorted({k - 1, n_y - k + 1}):
                serve_pair(j)
    serve_pair(half_y)

    got_wm.wait()
    over_width = ((1,), (1,))
    mixed_in = dot(normed[...], wm[...], over_width)
    centred = mixed_in - jnp.mean(mixed_in, axis=-1, keepdims=True)
    variance = jnp.mean(centred * centred, axis=-1, keepdims=True)
    mixed_norm = (centred * lax.rsqrt(variance + eps)).astype(BF16)
    got_mixw.wait()
    row_at = lax.broadcasted_iota(jnp.int32, (SPAN, SPAN), 0)
    col_at = lax.broadcasted_iota(jnp.int32, (SPAN, SPAN), 1)
    causal = jnp.where(col_at <= row_at, mixw[...].astype(F32), 0.0).astype(BF16)
    spatial = jnp.concatenate(
        [dot(causal, mixed_norm[n * SPAN : (n + 1) * SPAN]) for n in range(count // SPAN)], axis=0
    )
    got_wg.wait()
    branch_mix = dot(normed[...], wg[...], over_width) * spatial
    got_wgm.wait()
    gate = dot(normed[...], wgm[...], over_width)
    out_mix[...] = (branch_mix * (gate / (1.0 + jnp.exp(-gate)))).astype(BF16)
    got_wgr.wait()
    gate = dot(normed[...], wgr[...])
    gate_t[...] = jnp.transpose(gate / (1.0 + jnp.exp(-gate)))
    got_wom.wait()
    width = part.shape[2]
    for c in range(PIECES):
        part[c] = dot(out_mix[...], wom[:, c * width : (c + 1) * width])

    owners, ranks = [], []
    for e in range(blocks * NPB):
        owner = ids[e // NPB, e % NPB] // per_owner
        rank = jnp.int32(0)
        for before in owners:
            rank = rank + jnp.where(before == owner, 1, 0)
        owners.append(owner)
        ranks.append(rank)
    for copy in ret_copies:
        copy.wait_recv()
    got_wor.wait()
    for pair in range(blocks // 2):
        tops, totals, reads = [], [], []
        for n in range(NPB):
            e0, e1 = pair * 2 * NPB + n, (pair * 2 + 1) * NPB + n

            def placed(ref):
                x0, x1 = ref[owners[e0]].astype(F32), ref[owners[e1]].astype(F32)
                low = jnp.where(ranks[e0] == 0, x0, pltpu.roll(x0, RBLOCK, 1))
                high = jnp.where(ranks[e1] == 1, x1, pltpu.roll(x1, RBLOCK, 1))
                return jnp.where(first_half, low, high)

            stats = placed(ret_s)
            tops.append(stats[0:1])
            totals.append(stats[1:2])
            reads.append(placed(ret_o))
        top = functools.reduce(jnp.maximum, tops)
        scales = [jnp.exp(t - top) for t in tops]
        total = sum(s * t for s, t in zip(scales, totals))
        read = sum(s * r for s, r in zip(scales, reads)) / total
        cols = slice(pair * 2 * RBLOCK, (pair + 1) * 2 * RBLOCK)
        out_read[cols, :] = jnp.transpose(read * gate_t[:, cols]).astype(BF16)

    rs_copies = {}

    def pass_on(c, d, k):
        sign = 1 - 2 * d
        target = along_tp(sign * k)
        lo = 0
        size = mine_rows
        if k == half_tp:
            size = mine_rows // 2
            lo = d * size
        start = pl.multiple_of(target * mine_rows + lo, mine_rows // 2)
        value = part[c, pl.ds(start, size), :]
        if k == half_tp:
            rs_send[d, k - 1, c, lo : lo + size, :] = value.astype(BF16)
        else:
            rs_copies[c, d, k + 1].wait_recv()
            if k + 1 == half_tp:
                cut_rows = mine_rows // 2
                low = d * cut_rows
                rs_send[d, k - 1, c, low : low + cut_rows, :] = (
                    part[c, pl.ds(pl.multiple_of(target * mine_rows + low, cut_rows), cut_rows), :]
                    + rs_recv[d, k, c, low : low + cut_rows, :].astype(F32)
                ).astype(BF16)
                other = cut_rows - low
                rs_send[d, k - 1, c, other : other + cut_rows, :] = part[
                    c, pl.ds(pl.multiple_of(target * mine_rows + other, cut_rows), cut_rows), :
                ].astype(BF16)
            else:
                rs_send[d, k - 1, c] = (value + rs_recv[d, k, c].astype(F32)).astype(BF16)
        copy = pltpu.make_async_remote_copy(
            rs_send.at[d, k - 1, c, pl.ds(lo, size)], rs_recv.at[d, k - 1, c, pl.ds(lo, size)],
            rs_send_sem.at[d, k - 1, c], rs_recv_sem.at[d, k - 1, c],
            device_id=(grp, st, along_tp(sign)), device_id_type=MESH,
        )
        copy.start()
        rs_copies[c, d, k] = copy

    for c in range(PIECES):
        part[c] = part[c] + dot(out_read[...], wor[:, c * width : (c + 1) * width])
        for d in range(2):
            pass_on(c, d, half_tp)
    for k in range(half_tp - 1, 0, -1):
        for c in range(PIECES):
            for d in range(2):
                pass_on(c, d, k)
    here = pl.ds(pl.multiple_of(tp * mine_rows, mine_rows), mine_rows)
    for c in range(PIECES):
        for d in range(2):
            rs_copies[c, d, 1].wait_recv()
        if half_tp == 1:
            cut_rows = mine_rows // 2
            both = jnp.concatenate(
                [rs_recv[0, 0, c, :cut_rows, :], rs_recv[1, 0, c, cut_rows:, :]], axis=0
            ).astype(F32)
        else:
            both = rs_recv[0, 0, c].astype(F32) + rs_recv[1, 0, c].astype(F32)
        out[:, c * width : (c + 1) * width] = (part[c, here, :] + both).astype(BF16)

    for copy in (
        id_copies + list(ring_copies.values()) + list(sib_copies.values())
        + ret_copies + list(rs_copies.values())
    ):
        copy.wait_send()


def local(*args, n_st, n_tp):
    args = [a.T if k in (2, 3, 6) else a for k, a in enumerate(args)]
    tokens, w_gated, store = args[0], args[2], args[8]
    count, width = tokens.shape
    mix_width = w_gated.shape[0]
    held = store.shape[0]
    blocks = count // RBLOCK
    n_y = n_st // 2
    mine_rows = count // n_tp
    hbm = pl.BlockSpec(memory_space=pltpu.HBM)
    vmem = pl.BlockSpec(memory_space=pltpu.VMEM)
    smem = pl.BlockSpec(memory_space=pltpu.SMEM)
    specs = [hbm] * 15
    specs[1] = specs[9] = vmem
    specs[12] = smem
    dma = pltpu.SemaphoreType.DMA
    columns = width // PIECES
    scratch = dict(
        tok=pltpu.VMEM((count, width), BF16),
        normed=pltpu.VMEM((count, width), BF16),
        wg=pltpu.VMEM((mix_width, width), BF16),
        wm=pltpu.VMEM((mix_width, width), BF16),
        wgm=pltpu.VMEM((mix_width, width), BF16),
        mixw=pltpu.VMEM((SPAN, SPAN), BF16),
        wq=pltpu.VMEM((width, HD), BF16),
        wgr=pltpu.VMEM((width, HD), BF16),
        wkv=pltpu.VMEM((width, 2 * HD), BF16),
        wom=pltpu.VMEM((mix_width, width), BF16),
        wor=pltpu.VMEM((HD, width), BF16),
        rows_in=pltpu.VMEM((held, PROWS, width), BF16),
        rows_norm=pltpu.VMEM((PROWS, width), BF16),
        key_of=pltpu.VMEM((held, PROWS, HD), BF16),
        value_of=pltpu.VMEM((held, HD, PROWS), BF16),
        q_ring=[pltpu.VMEM((blocks, RBLOCK, HD), BF16) for _ in range(n_y)],
        q_sib=[pltpu.VMEM((blocks, RBLOCK, HD), BF16) for _ in range(n_y)],
        ids_all=pltpu.SMEM((n_st, blocks, NPB), jnp.int32),
        o_send=pltpu.VMEM((n_st, HD, 2 * RBLOCK), BF16),
        s_send=pltpu.VMEM((n_st, 2, 2 * RBLOCK), F32),
        ret_o=pltpu.VMEM((n_st, HD, 2 * RBLOCK), BF16),
        ret_s=pltpu.VMEM((n_st, 2, 2 * RBLOCK), F32),
        gate_t=pltpu.VMEM((HD, count), F32),
        out_mix=pltpu.VMEM((count, mix_width), BF16),
        out_read=pltpu.VMEM((count, HD), BF16),
        part=pltpu.VMEM((PIECES, count, columns), F32),
        rs_send=pltpu.VMEM((2, n_tp // 2, PIECES, mine_rows, columns), BF16),
        rs_recv=pltpu.VMEM((2, n_tp // 2, PIECES, mine_rows, columns), BF16),
        in_sem=dma((11,)),
        row_sem=dma((held,)),
        ids_send_sem=dma((n_st,)),
        ids_recv_sem=dma((n_st,)),
        ring_send_sem=dma((n_y, 2)),
        ring_recv_sem=dma((n_y, 2)),
        sib_send_sem=dma((n_y, 2)),
        sib_recv_sem=dma((n_y, 2)),
        ret_send_sem=dma((n_st,)),
        ret_recv_sem=dma((n_st,)),
        stat_send_sem=dma((n_st,)),
        stat_recv_sem=dma((n_st,)),
        rs_send_sem=dma((2, n_tp // 2, PIECES)),
        rs_recv_sem=dma((2, n_tp // 2, PIECES)),
    )
    names = list(scratch)

    def body(*refs):
        kernel(n_st, n_tp, *refs[:16], **dict(zip(names, refs[16:])))

    return pl.pallas_call(
        body,
        out_shape=jax.ShapeDtypeStruct((mine_rows, width), BF16),
        in_specs=specs,
        out_specs=vmem,
        scratch_shapes=list(scratch.values()),
        compiler_params=pltpu.CompilerParams(
            collective_id=0, has_side_effects=True, vmem_limit_bytes=67_000_000
        ),
        name="layer",
    )(*args)


def solution(mesh):
    placed = (
        P(("grp", "st"), None),
        P(),
        P(None, "tp"),
        P(None, "tp"),
        P("tp", None, None),
        P(None, "tp"),
        P(None, "tp"),
        P(None, "tp"),
        P(("grp", "st"), None, None),
        P(),
        P(None, "tp"),
        P(None, "tp"),
        P(("grp", "st"), None),
        P("tp", None),
        P("tp", None),
    )
    body = functools.partial(local, n_st=mesh.shape["st"], n_tp=mesh.shape["tp"])
    return jax.shard_map(
        body, mesh=mesh, in_specs=placed, out_specs=P(("grp", "st", "tp"), None), check_vma=False
    )
```

```python
import functools

import jax
import jax.numpy as jnp
from jax import lax
from jax.experimental import pallas as pl
from jax.experimental.pallas import tpu as pltpu
from jax.sharding import PartitionSpec as P

HD = 128
SPAN = 128
RBLOCK = 64
NPB = 4
PROWS = 128
NORM_ROWS = 32
PIECES = 4

MESH = pl.DeviceIdType.MESH
eps = 1e-06
F32 = jnp.float32
BF16 = jnp.bfloat16


def dot(a, b, dims=((1,), (0,))):
    return lax.dot_general(a, b, (dims, ((), ())), preferred_element_type=F32)


def row_norm(source, gain, target, rows):
    def some(i, carry):
        at = pl.ds(pl.multiple_of(i * NORM_ROWS, NORM_ROWS), NORM_ROWS)
        wide = source[at, :].astype(F32)
        scale = lax.rsqrt(jnp.mean(wide * wide, axis=-1, keepdims=True) + eps)
        target[at, :] = (wide * scale * gain).astype(BF16)
        return carry

    lax.fori_loop(0, rows // NORM_ROWS, some, 0)


def kernel(
    n_st,
    n_tp,
    tokens,
    pre_gain,
    w_gated,
    w_mixed,
    mix_weight,
    w_query,
    w_gate_mix,
    w_gate_read,
    store,
    mem_gain,
    w_key,
    w_value,
    ids,
    w_out_mix,
    w_out_read,
    out,
    tok,
    gains,
    own_ids,
    slot_of,
    normed,
    wg,
    wm,
    wgm,
    mixw,
    wq,
    wgr,
    wkv,
    wom,
    wor,
    rows_in,
    rows_norm,
    key_of,
    value_of,
    q_ring,
    q_sib,
    ids_all,
    o_send,
    s_send,
    ret_o,
    ret_s,
    gate_t,
    out_mix,
    out_read,
    part,
    rs_send,
    rs_recv,
    in_sem,
    row_sem,
    ids_send_sem,
    ids_recv_sem,
    ring_send_sem,
    ring_recv_sem,
    sib_send_sem,
    sib_recv_sem,
    ret_send_sem,
    ret_recv_sem,
    stat_send_sem,
    stat_recv_sem,
    rs_send_sem,
    rs_recv_sem,
):
    grp, st, tp = lax.axis_index("grp"), lax.axis_index("st"), lax.axis_index("tp")
    n_y = n_st // 2
    half_tp = n_tp // 2
    y, core = st // 2, lax.rem(st, 2)
    count = tok.shape[0]
    blocks = count // RBLOCK
    per_owner = rows_in.shape[0]
    mine_rows = count // n_tp

    def at_y(offset, sibling=False):
        chip = lax.rem(y + offset + n_y, n_y)
        return chip * 2 + (1 - core if sibling else core)

    def along_tp(offset):
        return lax.rem(tp + offset + n_tp, n_tp)

    def fetch(k, source, target):
        copy = pltpu.make_async_copy(source, target, in_sem.at[k])
        copy.start()
        return copy

    got_tok = fetch(0, tokens, tok)
    got_pre = fetch(11, pre_gain, gains.at[0])
    got_wq = fetch(1, w_query, wq)
    got_ids = fetch(12, ids, own_ids)

    barrier = pltpu.get_barrier_semaphore()
    peers = [(grp, lax.rem(st + k, n_st), tp) for k in range(1, n_st)]
    sides = [1, -1] if n_tp > 2 else [1]
    peers += [(grp, st, along_tp(k)) for k in sides]
    for peer in peers:
        pl.semaphore_signal(barrier, inc=1, device_id=peer, device_id_type=MESH)

    got_wk = fetch(2, w_key, wkv.at[:, 0:HD])
    got_wv = fetch(3, w_value, wkv.at[:, HD : 2 * HD])
    got_mem = fetch(13, mem_gain, gains.at[1])
    for p in range(per_owner):
        pltpu.make_async_copy(store.at[p], rows_in.at[p], row_sem.at[p]).start()
    got_wm = fetch(4, w_mixed, wm)
    got_wg = fetch(5, w_gated, wg)
    got_wgm = fetch(6, w_gate_mix, wgm)
    got_wgr = fetch(7, w_gate_read, wgr)
    got_mixw = fetch(8, mix_weight.at[0], mixw)
    got_wom = fetch(9, w_out_mix, wom)
    got_wor = fetch(10, w_out_read, wor)

    got_pre.wait()
    got_tok.wait()
    row_norm(tok, gains[0].reshape(1, -1), normed, count)
    got_wq.wait()
    own_q = dot(normed[...], wq[...]).astype(BF16)
    q_ring[0][...] = own_q.reshape(blocks, RBLOCK, HD)
    got_ids.wait()

    pl.semaphore_wait(barrier, len(peers))

    cut = blocks // 2
    ring_copies, sib_copies = {}, {}

    def push(j, after, h, offset):
        piece = pl.ds(h * cut, cut)
        copy = pltpu.make_async_remote_copy(
            q_ring[j].at[piece], q_ring[after].at[piece],
            ring_send_sem.at[after, h], ring_recv_sem.at[after, h],
            device_id=(grp, at_y(offset), tp), device_id_type=MESH,
        )
        copy.start()
        ring_copies[after, h] = copy

    def across(j, h):
        piece = pl.ds(h * cut, cut)
        copy = pltpu.make_async_remote_copy(
            q_ring[j].at[piece], q_sib[j].at[piece],
            sib_send_sem.at[j, h], sib_recv_sem.at[j, h],
            device_id=(grp, at_y(0, True), tp), device_id_type=MESH,
        )
        copy.start()
        sib_copies[j, h] = copy

    for h in range(2):
        push(0, 2, h, 2)
        push(0, n_y - 2, h, -2)
    for h in range(2):
        push(0, 1, h, 1)
        push(0, n_y - 1, h, -1)
    for h in range(2):
        across(0, h)

    id_copies = []
    for k in range(1, n_st):
        copy = pltpu.make_async_remote_copy(
            own_ids, ids_all.at[st], ids_send_sem.at[k], ids_recv_sem.at[k],
            device_id=(grp, lax.rem(st + k, n_st), tp), device_id_type=MESH,
        )
        copy.start()
        id_copies.append(copy)
    for b in range(blocks):
        for n in range(NPB):
            ids_all[st, b, n] = own_ids[b, n]

    got_wk.wait()
    got_wv.wait()
    got_mem.wait()
    mem_row = gains[1].reshape(1, -1)

    def keys_of(p, carry):
        pltpu.make_async_copy(store.at[p], rows_in.at[p], row_sem.at[p]).wait()
        row_norm(rows_in.at[p], mem_row, rows_norm, PROWS)
        both = dot(rows_norm[...], wkv[...])
        key_of[p] = both[:, :HD].astype(BF16)
        value_of[p] = jnp.transpose(both[:, HD:]).astype(BF16)
        return carry

    lax.fori_loop(0, per_owner, keys_of, 0)

    for copy in id_copies:
        copy.wait_recv()

    def slots(reader, carry):
        p0 = p1 = b0 = b1 = seen = jnp.int32(0)
        for b in range(blocks):
            for n in range(NPB):
                local = ids_all[reader, b, n] - st * per_owner
                mine = (local >= 0) & (local < per_owner)
                is0 = mine & (seen == 0)
                is1 = mine & (seen == 1)
                p0, b0 = jnp.where(is0, local, p0), jnp.where(is0, b, b0)
                p1, b1 = jnp.where(is1, local, p1), jnp.where(is1, b, b1)
                seen = seen + jnp.where(mine, 1, 0)
        for k, value in enumerate((p0, p1, b0, b1)):
            slot_of[reader, k] = value
        return carry

    lax.fori_loop(0, n_st, slots, 0)

    lanes = lax.broadcasted_iota(jnp.int32, (1, 2 * RBLOCK), 1)
    first_half = lanes < RBLOCK

    def attend(q_ref, reader):
        p0, p1, b0, b1 = (slot_of[reader, k] for k in range(4))
        q = jnp.concatenate([q_ref[b0], q_ref[b1]], axis=0)
        over_keys = ((1,), (1,))
        scores = jnp.where(
            first_half, dot(key_of[p0], q, over_keys), dot(key_of[p1], q, over_keys)
        ) * (HD ** (-0.5))
        top = jnp.max(scores, axis=0, keepdims=True)
        weight = jnp.exp(scores - top)
        total = jnp.sum(weight, axis=0, keepdims=True)
        weight = weight.astype(BF16)
        read = jnp.where(first_half, dot(value_of[p0], weight), dot(value_of[p1], weight))
        return read.astype(BF16), jnp.concatenate([top, total], axis=0)

    ret_copies = []

    def serve(*labels):
        for j, sibling in labels:
            for h in range(2):
                if sibling:
                    sib_copies[j, h].wait_recv()
        readers = [at_y(-j, sibling) for j, sibling in labels]
        results = [
            attend(q_sib[j] if sibling else q_ring[j], reader)
            for (j, sibling), reader in zip(labels, readers)
        ]
        for (j, sibling), (read, stats) in zip(labels, results):
            if j == 0 and not sibling:
                ret_o[st] = read
                ret_s[st] = stats
            else:
                o_send[j * 2 + sibling] = read
                s_send[j * 2 + sibling] = stats
        for (j, sibling), reader in zip(labels, readers):
            if j == 0 and not sibling:
                continue
            label = j * 2 + sibling
            for source, target, send, recv in (
                (o_send, ret_o, ret_send_sem, ret_recv_sem),
                (s_send, ret_s, stat_send_sem, stat_recv_sem),
            ):
                copy = pltpu.make_async_remote_copy(
                    source.at[label], target.at[st], send.at[label], recv.at[label],
                    device_id=(grp, reader, tp), device_id_type=MESH,
                )
                copy.start()
                ret_copies.append(copy)

    for h in range(2):
        for j, near, far, sign in ((2, 3, 4, 1), (n_y - 2, n_y - 3, 4, -1)):
            ring_copies[j, h].wait_recv()
            if h == (0 if sign > 0 else 1):
                push(j, far, h, 2 * sign)
            push(j, near, h, sign)
            across(j, h)
    for h in range(2):
        for j in (1, n_y - 1):
            ring_copies[j, h].wait_recv()
            across(j, h)
    serve((1, 0), (n_y - 1, 0))
    serve((2, 0), (n_y - 2, 0))
    serve((1, 1), (n_y - 1, 1))
    serve((2, 1), (n_y - 2, 1))
    serve((0, 0), (0, 1))

    got_wm.wait()
    over_width = ((1,), (1,))
    mixed_in = dot(normed[...], wm[...], over_width)
    centred = mixed_in - jnp.mean(mixed_in, axis=-1, keepdims=True)
    variance = jnp.mean(centred * centred, axis=-1, keepdims=True)
    mixed_norm = (centred * lax.rsqrt(variance + eps)).astype(BF16)
    got_mixw.wait()
    row_at = lax.broadcasted_iota(jnp.int32, (SPAN, SPAN), 0)
    col_at = lax.broadcasted_iota(jnp.int32, (SPAN, SPAN), 1)
    causal = jnp.where(col_at <= row_at, mixw[...].astype(F32), 0.0).astype(BF16)
    spatial = jnp.concatenate(
        [dot(causal, mixed_norm[n * SPAN : (n + 1) * SPAN]) for n in range(count // SPAN)], axis=0
    )
    got_wg.wait()
    branch_mix = dot(normed[...], wg[...], over_width) * spatial
    got_wgm.wait()
    gate = dot(normed[...], wgm[...], over_width)
    out_mix[...] = (branch_mix * (gate / (1.0 + jnp.exp(-gate)))).astype(BF16)
    got_wgr.wait()
    gate = dot(normed[...], wgr[...])
    gate_t[...] = jnp.transpose(gate / (1.0 + jnp.exp(-gate)))
    got_wom.wait()
    width = part.shape[2]
    for c in range(PIECES):
        part[c] = dot(out_mix[...], wom[:, c * width : (c + 1) * width])

    for h in range(2):
        for j in (3, n_y - 3):
            ring_copies[j, h].wait_recv()
            across(j, h)
    for h in range(2):
        ring_copies[4, h].wait_recv()
        across(4, h)
    serve((4, 0), (3, 0), (n_y - 3, 0))
    serve((4, 1), (3, 1), (n_y - 3, 1))

    owners, ranks = [], []
    for e in range(blocks * NPB):
        owner = own_ids[e // NPB, e % NPB] // per_owner
        rank = jnp.int32(0)
        for before in owners:
            rank = rank + jnp.where(before == owner, 1, 0)
        owners.append(owner)
        ranks.append(rank)
    for copy in ret_copies:
        copy.wait_recv()
    got_wor.wait()
    for pair in range(blocks // 2):
        tops, totals, reads = [], [], []
        for n in range(NPB):
            e0, e1 = pair * 2 * NPB + n, (pair * 2 + 1) * NPB + n

            def placed(ref):
                x0, x1 = ref[owners[e0]].astype(F32), ref[owners[e1]].astype(F32)
                low = jnp.where(ranks[e0] == 0, x0, pltpu.roll(x0, RBLOCK, 1))
                high = jnp.where(ranks[e1] == 1, x1, pltpu.roll(x1, RBLOCK, 1))
                return jnp.where(first_half, low, high)

            stats = placed(ret_s)
            tops.append(stats[0:1])
            totals.append(stats[1:2])
            reads.append(placed(ret_o))
        top = functools.reduce(jnp.maximum, tops)
        scales = [jnp.exp(t - top) for t in tops]
        total = sum(s * t for s, t in zip(scales, totals))
        read = sum(s * r for s, r in zip(scales, reads)) / total
        cols = slice(pair * 2 * RBLOCK, (pair + 1) * 2 * RBLOCK)
        out_read[cols, :] = jnp.transpose(read * gate_t[:, cols]).astype(BF16)

    rs_copies = {}

    def pass_on(c, d, k):
        sign = 1 - 2 * d
        target = along_tp(sign * k)
        lo = 0
        size = mine_rows
        if k == half_tp:
            size = mine_rows // 2
            lo = d * size
        start = pl.multiple_of(target * mine_rows + lo, mine_rows // 2)
        value = part[c, pl.ds(start, size), :]
        if k == half_tp:
            rs_send[d, k - 1, c, lo : lo + size, :] = value.astype(BF16)
        else:
            rs_copies[c, d, k + 1].wait_recv()
            if k + 1 == half_tp:
                cut_rows = mine_rows // 2
                low = d * cut_rows
                rs_send[d, k - 1, c, low : low + cut_rows, :] = (
                    part[c, pl.ds(pl.multiple_of(target * mine_rows + low, cut_rows), cut_rows), :]
                    + rs_recv[d, k, c, low : low + cut_rows, :].astype(F32)
                ).astype(BF16)
                other = cut_rows - low
                rs_send[d, k - 1, c, other : other + cut_rows, :] = part[
                    c, pl.ds(pl.multiple_of(target * mine_rows + other, cut_rows), cut_rows), :
                ].astype(BF16)
            else:
                rs_send[d, k - 1, c] = (value + rs_recv[d, k, c].astype(F32)).astype(BF16)
        copy = pltpu.make_async_remote_copy(
            rs_send.at[d, k - 1, c, pl.ds(lo, size)], rs_recv.at[d, k - 1, c, pl.ds(lo, size)],
            rs_send_sem.at[d, k - 1, c], rs_recv_sem.at[d, k - 1, c],
            device_id=(grp, st, along_tp(sign)), device_id_type=MESH,
        )
        copy.start()
        rs_copies[c, d, k] = copy

    for c in range(PIECES):
        part[c] = part[c] + dot(out_read[...], wor[:, c * width : (c + 1) * width])
        for d in range(2):
            pass_on(c, d, half_tp)
    for k in range(half_tp - 1, 0, -1):
        for c in range(PIECES):
            for d in range(2):
                pass_on(c, d, k)
    here = pl.ds(pl.multiple_of(tp * mine_rows, mine_rows), mine_rows)
    for c in range(PIECES):
        for d in range(2):
            rs_copies[c, d, 1].wait_recv()
        if half_tp == 1:
            cut_rows = mine_rows // 2
            both = jnp.concatenate(
                [rs_recv[0, 0, c, :cut_rows, :], rs_recv[1, 0, c, cut_rows:, :]], axis=0
            ).astype(F32)
        else:
            both = rs_recv[0, 0, c].astype(F32) + rs_recv[1, 0, c].astype(F32)
        out[:, c * width : (c + 1) * width] = (part[c, here, :] + both).astype(BF16)

    for copy in (
        id_copies + list(ring_copies.values()) + list(sib_copies.values())
        + ret_copies + list(rs_copies.values())
    ):
        copy.wait_send()


def local(*args, n_st, n_tp):
    args = [a.T if k in (2, 3, 6) else a for k, a in enumerate(args)]
    tokens, w_gated, store = args[0], args[2], args[8]
    count, width = tokens.shape
    mix_width = w_gated.shape[0]
    held = store.shape[0]
    blocks = count // RBLOCK
    n_y = n_st // 2
    mine_rows = count // n_tp
    hbm = pl.BlockSpec(memory_space=pltpu.HBM)
    vmem = pl.BlockSpec(memory_space=pltpu.VMEM)
    specs = [hbm] * 15
    dma = pltpu.SemaphoreType.DMA
    columns = width // PIECES
    scratch = dict(
        tok=pltpu.VMEM((count, width), BF16),
        gains=pltpu.VMEM((2, width), F32),
        own_ids=pltpu.SMEM((blocks, NPB), jnp.int32),
        slot_of=pltpu.SMEM((n_st, 4), jnp.int32),
        normed=pltpu.VMEM((count, width), BF16),
        wg=pltpu.VMEM((mix_width, width), BF16),
        wm=pltpu.VMEM((mix_width, width), BF16),
        wgm=pltpu.VMEM((mix_width, width), BF16),
        mixw=pltpu.VMEM((SPAN, SPAN), BF16),
        wq=pltpu.VMEM((width, HD), BF16),
        wgr=pltpu.VMEM((width, HD), BF16),
        wkv=pltpu.VMEM((width, 2 * HD), BF16),
        wom=pltpu.VMEM((mix_width, width), BF16),
        wor=pltpu.VMEM((HD, width), BF16),
        rows_in=pltpu.VMEM((held, PROWS, width), BF16),
        rows_norm=pltpu.VMEM((PROWS, width), BF16),
        key_of=pltpu.VMEM((held, PROWS, HD), BF16),
        value_of=pltpu.VMEM((held, HD, PROWS), BF16),
        q_ring=[pltpu.VMEM((blocks, RBLOCK, HD), BF16) for _ in range(n_y)],
        q_sib=[pltpu.VMEM((blocks, RBLOCK, HD), BF16) for _ in range(n_y)],
        ids_all=pltpu.SMEM((n_st, blocks, NPB), jnp.int32),
        o_send=pltpu.VMEM((n_st, HD, 2 * RBLOCK), BF16),
        s_send=pltpu.VMEM((n_st, 2, 2 * RBLOCK), F32),
        ret_o=pltpu.VMEM((n_st, HD, 2 * RBLOCK), BF16),
        ret_s=pltpu.VMEM((n_st, 2, 2 * RBLOCK), F32),
        gate_t=pltpu.VMEM((HD, count), F32),
        out_mix=pltpu.VMEM((count, mix_width), BF16),
        out_read=pltpu.VMEM((count, HD), BF16),
        part=pltpu.VMEM((PIECES, count, columns), F32),
        rs_send=pltpu.VMEM((2, n_tp // 2, PIECES, mine_rows, columns), BF16),
        rs_recv=pltpu.VMEM((2, n_tp // 2, PIECES, mine_rows, columns), BF16),
        in_sem=dma((14,)),
        row_sem=dma((held,)),
        ids_send_sem=dma((n_st,)),
        ids_recv_sem=dma((n_st,)),
        ring_send_sem=dma((n_y, 2)),
        ring_recv_sem=dma((n_y, 2)),
        sib_send_sem=dma((n_y, 2)),
        sib_recv_sem=dma((n_y, 2)),
        ret_send_sem=dma((n_st,)),
        ret_recv_sem=dma((n_st,)),
        stat_send_sem=dma((n_st,)),
        stat_recv_sem=dma((n_st,)),
        rs_send_sem=dma((2, n_tp // 2, PIECES)),
        rs_recv_sem=dma((2, n_tp // 2, PIECES)),
    )
    names = list(scratch)

    def body(*refs):
        kernel(n_st, n_tp, *refs[:16], **dict(zip(names, refs[16:])))

    return pl.pallas_call(
        body,
        out_shape=jax.ShapeDtypeStruct((mine_rows, width), BF16),
        in_specs=specs,
        out_specs=vmem,
        scratch_shapes=list(scratch.values()),
        compiler_params=pltpu.CompilerParams(
            collective_id=0, has_side_effects=True, vmem_limit_bytes=67_000_000
        ),
        name="layer",
    )(*args)


def solution(mesh):
    placed = (
        P(("grp", "st"), None),
        P(),
        P(None, "tp"),
        P(None, "tp"),
        P("tp", None, None),
        P(None, "tp"),
        P(None, "tp"),
        P(None, "tp"),
        P(("grp", "st"), None, None),
        P(),
        P(None, "tp"),
        P(None, "tp"),
        P(("grp", "st"), None),
        P("tp", None),
        P("tp", None),
    )
    body = functools.partial(local, n_st=mesh.shape["st"], n_tp=mesh.shape["tp"])
    return jax.shard_map(
        body, mesh=mesh, in_specs=placed, out_specs=P(("grp", "st", "tp"), None), check_vma=False
    )
```

```python
import functools

import jax
import jax.numpy as jnp
from jax import lax
from jax.experimental import pallas as pl
from jax.experimental.pallas import tpu as pltpu
from jax.sharding import PartitionSpec as P

HD = 128
SPAN = 128
RBLOCK = 64
NPB = 4
PROWS = 128
NORM_ROWS = 32
PIECES = 2

MESH = pl.DeviceIdType.MESH
eps = 1e-06
F32 = jnp.float32
BF16 = jnp.bfloat16


def dot(a, b, dims=((1,), (0,))):
    return lax.dot_general(a, b, (dims, ((), ())), preferred_element_type=F32)


def row_norm(source, gain, target, rows):
    def some(i, carry):
        at = pl.ds(pl.multiple_of(i * NORM_ROWS, NORM_ROWS), NORM_ROWS)
        wide = source[at, :].astype(F32)
        scale = lax.rsqrt(jnp.mean(wide * wide, axis=-1, keepdims=True) + eps)
        target[at, :] = (wide * scale * gain).astype(BF16)
        return carry

    lax.fori_loop(0, rows // NORM_ROWS, some, 0)


def kernel(
    n_st,
    n_tp,
    tokens,
    pre_gain,
    w_gated,
    w_mixed,
    mix_weight,
    w_query,
    w_gate_mix,
    w_gate_read,
    store,
    mem_gain,
    w_key,
    w_value,
    ids,
    w_out_mix,
    w_out_read,
    out,
    tok,
    gains,
    own_ids,
    slot_of,
    normed,
    wg,
    wm,
    wgm,
    mixw,
    wq,
    wgr,
    wkv,
    wom,
    wor,
    rows_in,
    rows_norm,
    key_of,
    value_of,
    q_ring,
    q_sib,
    ids_all,
    o_send,
    s_send,
    ret_o,
    ret_s,
    gate_t,
    out_mix,
    out_read,
    part,
    rs_send,
    rs_recv,
    in_sem,
    row_sem,
    ids_send_sem,
    ids_recv_sem,
    ring_send_sem,
    ring_recv_sem,
    two_recv_sem,
    sib_send_sem,
    sib_recv_sem,
    ret_send_sem,
    ret_recv_sem,
    stat_send_sem,
    stat_recv_sem,
    rs_send_sem,
    rs_recv_sem,
):
    grp, st, tp = lax.axis_index("grp"), lax.axis_index("st"), lax.axis_index("tp")
    n_y = n_st // 2
    half_tp = n_tp // 2
    y, core = st // 2, lax.rem(st, 2)
    count = tok.shape[0]
    blocks = count // RBLOCK
    per_owner = rows_in.shape[0]
    mine_rows = count // n_tp

    def at_y(offset, sibling=False):
        chip = lax.rem(y + offset + n_y, n_y)
        return chip * 2 + (1 - core if sibling else core)

    def along_tp(offset):
        return lax.rem(tp + offset + n_tp, n_tp)

    def fetch(k, source, target):
        copy = pltpu.make_async_copy(source, target, in_sem.at[k])
        copy.start()
        return copy

    got_tok = fetch(0, tokens, tok)
    got_pre = fetch(11, pre_gain, gains.at[0])
    got_wq = fetch(1, w_query, wq)
    got_ids = fetch(12, ids, own_ids)

    barrier = pltpu.get_barrier_semaphore()
    peers = [(grp, lax.rem(st + k, n_st), tp) for k in range(1, n_st)]
    sides = [1, -1] if n_tp > 2 else [1]
    peers += [(grp, st, along_tp(k)) for k in sides]
    for peer in peers:
        pl.semaphore_signal(barrier, inc=1, device_id=peer, device_id_type=MESH)

    got_wk = fetch(2, w_key, wkv.at[:, 0:HD])
    got_wv = fetch(3, w_value, wkv.at[:, HD : 2 * HD])
    got_mem = fetch(13, mem_gain, gains.at[1])
    for p in range(per_owner):
        pltpu.make_async_copy(store.at[p], rows_in.at[p], row_sem.at[p]).start()
    got_wm = fetch(4, w_mixed, wm)
    got_wg = fetch(5, w_gated, wg)
    got_wgm = fetch(6, w_gate_mix, wgm)
    got_wgr = fetch(7, w_gate_read, wgr)
    got_mixw = fetch(8, mix_weight.at[0], mixw)
    got_wom = fetch(9, w_out_mix, wom)
    got_wor = fetch(10, w_out_read, wor)

    got_pre.wait()
    got_tok.wait()
    row_norm(tok, gains[0].reshape(1, -1), normed, count)
    got_wq.wait()
    own_q = dot(normed[...], wq[...]).astype(BF16)
    q_ring[0][...] = own_q.reshape(blocks, RBLOCK, HD)
    got_ids.wait()

    pl.semaphore_wait(barrier, len(peers))

    for k in range(1, n_st):
        pltpu.make_async_remote_copy(
            own_ids, ids_all.at[st], ids_send_sem, ids_recv_sem,
            device_id=(grp, lax.rem(st + k, n_st), tp), device_id_type=MESH,
        ).start()

    def drain(like, sem):
        pltpu.make_async_copy(like, like, sem).wait()

    cut = blocks // 2

    def push(j, after, h, offset):
        piece = pl.ds(h * cut, cut)
        recv = two_recv_sem.at[after // 4, h] if after in (2, n_y - 2) else ring_recv_sem.at[after]
        pltpu.make_async_remote_copy(
            q_ring[j].at[piece], q_ring[after].at[piece], ring_send_sem, recv,
            device_id=(grp, at_y(offset), tp), device_id_type=MESH,
        ).start()

    def across(j):
        pltpu.make_async_remote_copy(
            q_ring[j], q_sib[j], sib_send_sem, sib_recv_sem.at[j],
            device_id=(grp, at_y(0, True), tp), device_id_type=MESH,
        ).start()

    for h in range(2):
        push(0, 2, h, 2)
        push(0, n_y - 2, h, -2)
    for h in range(2):
        push(0, 1, h, 1)
        push(0, n_y - 1, h, -1)
    across(0)

    for b in range(blocks):
        for n in range(NPB):
            ids_all[st, b, n] = own_ids[b, n]

    got_wk.wait()
    got_wv.wait()
    got_mem.wait()
    mem_row = gains[1].reshape(1, -1)

    def keys_of(p, carry):
        pltpu.make_async_copy(store.at[p], rows_in.at[p], row_sem.at[p]).wait()
        row_norm(rows_in.at[p], mem_row, rows_norm, PROWS)
        both = dot(rows_norm[...], wkv[...])
        key_of[p] = both[:, :HD].astype(BF16)
        value_of[p] = jnp.transpose(both[:, HD:]).astype(BF16)
        return carry

    lax.fori_loop(0, per_owner, keys_of, 0)

    lanes = lax.broadcasted_iota(jnp.int32, (1, 2 * RBLOCK), 1)
    first_half = lanes < RBLOCK

    def attend(q_ref, reader):
        p0, p1, b0, b1 = (slot_of[reader, k] for k in range(4))
        q = jnp.concatenate([q_ref[b0], q_ref[b1]], axis=0)
        over_keys = ((1,), (1,))
        scores = jnp.where(
            first_half, dot(key_of[p0], q, over_keys), dot(key_of[p1], q, over_keys)
        ) * (HD ** (-0.5))
        top = jnp.max(scores, axis=0, keepdims=True)
        weight = jnp.exp(scores - top)
        total = jnp.sum(weight, axis=0, keepdims=True)
        weight = weight.astype(BF16)
        read = jnp.where(first_half, dot(value_of[p0], weight), dot(value_of[p1], weight))
        return read.astype(BF16), jnp.concatenate([top, total], axis=0)

    def serve(*labels):
        for j, sibling in labels:
            if sibling:
                drain(q_sib[j], sib_recv_sem.at[j])
        readers = [at_y(-j, sibling) for j, sibling in labels]
        results = [
            attend(q_sib[j] if sibling else q_ring[j], reader)
            for (j, sibling), reader in zip(labels, readers)
        ]
        for (j, sibling), (read, stats) in zip(labels, results):
            if j == 0 and not sibling:
                ret_o[st] = read
                ret_s[st] = stats
            else:
                o_send[j * 2 + sibling] = read
                s_send[j * 2 + sibling] = stats
        for (j, sibling), reader in zip(labels, readers):
            if j == 0 and not sibling:
                continue
            label = j * 2 + sibling
            for source, target, send, recv in (
                (o_send, ret_o, ret_send_sem, ret_recv_sem),
                (s_send, ret_s, stat_send_sem, stat_recv_sem),
            ):
                pltpu.make_async_remote_copy(
                    source.at[label], target.at[st], send, recv,
                    device_id=(grp, reader, tp), device_id_type=MESH,
                ).start()

    for h in range(2):
        for j, near, far, sign in ((2, 3, 4, 1), (n_y - 2, n_y - 3, 4, -1)):
            drain(q_ring[j].at[pl.ds(h * cut, cut)], two_recv_sem.at[j // 4, h])
            if h == (0 if sign > 0 else 1):
                push(j, far, h, 2 * sign)
            push(j, near, h, sign)
    for j in (1, n_y - 1):
        drain(q_ring[j], ring_recv_sem.at[j])
        across(j)
    for j in (2, n_y - 2):
        across(j)

    drain(ids_all.at[pl.ds(0, n_st - 1)], ids_recv_sem)

    def slots(reader, carry):
        p0 = p1 = b0 = b1 = seen = jnp.int32(0)
        for b in range(blocks):
            for n in range(NPB):
                local = ids_all[reader, b, n] - st * per_owner
                mine = (local >= 0) & (local < per_owner)
                is0 = mine & (seen == 0)
                is1 = mine & (seen == 1)
                p0, b0 = jnp.where(is0, local, p0), jnp.where(is0, b, b0)
                p1, b1 = jnp.where(is1, local, p1), jnp.where(is1, b, b1)
                seen = seen + jnp.where(mine, 1, 0)
        for k, value in enumerate((p0, p1, b0, b1)):
            slot_of[reader, k] = value
        return carry

    lax.fori_loop(0, n_st, slots, 0)

    serve((1, 0), (n_y - 1, 0))
    serve((2, 0), (n_y - 2, 0))
    serve((1, 1), (n_y - 1, 1))
    serve((2, 1), (n_y - 2, 1))
    serve((0, 0), (0, 1))

    got_wm.wait()
    over_width = ((1,), (1,))
    mixed_in = dot(normed[...], wm[...], over_width)
    centred = mixed_in - jnp.mean(mixed_in, axis=-1, keepdims=True)
    variance = jnp.mean(centred * centred, axis=-1, keepdims=True)
    mixed_norm = (centred * lax.rsqrt(variance + eps)).astype(BF16)
    got_mixw.wait()
    row_at = lax.broadcasted_iota(jnp.int32, (SPAN, SPAN), 0)
    col_at = lax.broadcasted_iota(jnp.int32, (SPAN, SPAN), 1)
    causal = jnp.where(col_at <= row_at, mixw[...].astype(F32), 0.0).astype(BF16)
    spatial = jnp.concatenate(
        [dot(causal, mixed_norm[n * SPAN : (n + 1) * SPAN]) for n in range(count // SPAN)], axis=0
    )
    got_wg.wait()
    branch_mix = dot(normed[...], wg[...], over_width) * spatial
    got_wgm.wait()
    gate = dot(normed[...], wgm[...], over_width)
    out_mix[...] = (branch_mix * (gate / (1.0 + jnp.exp(-gate)))).astype(BF16)
    got_wgr.wait()
    gate = dot(normed[...], wgr[...])
    gate_t[...] = jnp.transpose(gate / (1.0 + jnp.exp(-gate)))
    got_wom.wait()
    width = part.shape[2]
    for c in range(PIECES):
        part[c] = dot(out_mix[...], wom[:, c * width : (c + 1) * width])

    for j in (3, n_y - 3, 4):
        drain(q_ring[j], ring_recv_sem.at[j])
        across(j)
    serve((4, 0), (3, 0), (n_y - 3, 0))
    serve((4, 1), (3, 1), (n_y - 3, 1))

    owners, ranks = [], []
    for e in range(blocks * NPB):
        owner = own_ids[e // NPB, e % NPB] // per_owner
        rank = jnp.int32(0)
        for before in owners:
            rank = rank + jnp.where(before == owner, 1, 0)
        owners.append(owner)
        ranks.append(rank)
    drain(ret_o.at[pl.ds(0, n_st - 1)], ret_recv_sem)
    drain(ret_s.at[pl.ds(0, n_st - 1)], stat_recv_sem)
    got_wor.wait()
    for pair in range(blocks // 2):
        tops, totals, reads = [], [], []
        for n in range(NPB):
            e0, e1 = pair * 2 * NPB + n, (pair * 2 + 1) * NPB + n

            def placed(ref):
                x0, x1 = ref[owners[e0]].astype(F32), ref[owners[e1]].astype(F32)
                low = jnp.where(ranks[e0] == 0, x0, pltpu.roll(x0, RBLOCK, 1))
                high = jnp.where(ranks[e1] == 1, x1, pltpu.roll(x1, RBLOCK, 1))
                return jnp.where(first_half, low, high)

            stats = placed(ret_s)
            tops.append(stats[0:1])
            totals.append(stats[1:2])
            reads.append(placed(ret_o))
        top = functools.reduce(jnp.maximum, tops)
        scales = [jnp.exp(t - top) for t in tops]
        total = sum(s * t for s, t in zip(scales, totals))
        read = sum(s * r for s, r in zip(scales, reads)) / total
        cols = slice(pair * 2 * RBLOCK, (pair + 1) * 2 * RBLOCK)
        out_read[cols, :] = jnp.transpose(read * gate_t[:, cols]).astype(BF16)

    rs_copies = {}

    def pass_on(c, d, k):
        sign = 1 - 2 * d
        target = along_tp(sign * k)
        lo = 0
        size = mine_rows
        if k == half_tp:
            size = mine_rows // 2
            lo = d * size
        start = pl.multiple_of(target * mine_rows + lo, mine_rows // 2)
        value = part[c, pl.ds(start, size), :]
        if k == half_tp:
            rs_send[k - 1, d, c, lo : lo + size, :] = value.astype(BF16)
        else:
            rs_copies[c, d, k + 1].wait_recv()
            if k + 1 == half_tp:
                cut_rows = mine_rows // 2
                low = d * cut_rows
                rs_send[k - 1, d, c, low : low + cut_rows, :] = (
                    part[c, pl.ds(pl.multiple_of(target * mine_rows + low, cut_rows), cut_rows), :]
                    + rs_recv[k, d, c, low : low + cut_rows, :].astype(F32)
                ).astype(BF16)
                other = cut_rows - low
                rs_send[k - 1, d, c, other : other + cut_rows, :] = part[
                    c, pl.ds(pl.multiple_of(target * mine_rows + other, cut_rows), cut_rows), :
                ].astype(BF16)
            else:
                rs_send[k - 1, d, c] = (value + rs_recv[k, d, c].astype(F32)).astype(BF16)
        copy = pltpu.make_async_remote_copy(
            rs_send.at[k - 1, d, c, pl.ds(lo, size)], rs_recv.at[k - 1, d, c, pl.ds(lo, size)],
            rs_send_sem.at[k // half_tp], rs_recv_sem.at[k - 1, d, c],
            device_id=(grp, st, along_tp(sign)), device_id_type=MESH,
        )
        copy.start()
        rs_copies[c, d, k] = copy

    for c in range(PIECES):
        part[c] = part[c] + dot(out_read[...], wor[:, c * width : (c + 1) * width])
        for d in range(2):
            pass_on(c, d, half_tp)
    for k in range(half_tp - 1, 0, -1):
        for c in range(PIECES):
            for d in range(2):
                pass_on(c, d, k)
    here = pl.ds(pl.multiple_of(tp * mine_rows, mine_rows), mine_rows)
    for c in range(PIECES):
        for d in range(2):
            rs_copies[c, d, 1].wait_recv()
        if half_tp == 1:
            cut_rows = mine_rows // 2
            both = jnp.concatenate(
                [rs_recv[0, 0, c, :cut_rows, :], rs_recv[0, 1, c, cut_rows:, :]], axis=0
            ).astype(F32)
        else:
            both = rs_recv[0, 0, c].astype(F32) + rs_recv[0, 1, c].astype(F32)
        out[:, c * width : (c + 1) * width] = (part[c, here, :] + both).astype(BF16)

    drain(ids_all.at[pl.ds(0, n_st - 1)], ids_send_sem)
    drain(o_send.at[pl.ds(0, 2 * (n_y - 1))], ring_send_sem)
    drain(o_send, sib_send_sem)
    drain(o_send.at[pl.ds(0, n_st - 1)], ret_send_sem)
    drain(s_send.at[pl.ds(0, n_st - 1)], stat_send_sem)
    drain(rs_send.at[half_tp - 1, 0], rs_send_sem.at[1])
    if half_tp > 1:
        drain(rs_send.at[pl.ds(0, half_tp - 1)], rs_send_sem.at[0])


def local(*args, n_st, n_tp):
    args = [a.T if k in (2, 3, 6) else a for k, a in enumerate(args)]
    tokens, w_gated, store = args[0], args[2], args[8]
    count, width = tokens.shape
    mix_width = w_gated.shape[0]
    held = store.shape[0]
    blocks = count // RBLOCK
    n_y = n_st // 2
    mine_rows = count // n_tp
    hbm = pl.BlockSpec(memory_space=pltpu.HBM)
    vmem = pl.BlockSpec(memory_space=pltpu.VMEM)
    specs = [hbm] * 15
    dma = pltpu.SemaphoreType.DMA
    columns = width // PIECES
    scratch = dict(
        tok=pltpu.VMEM((count, width), BF16),
        gains=pltpu.VMEM((2, width), F32),
        own_ids=pltpu.SMEM((blocks, NPB), jnp.int32),
        slot_of=pltpu.SMEM((n_st, 4), jnp.int32),
        normed=pltpu.VMEM((count, width), BF16),
        wg=pltpu.VMEM((mix_width, width), BF16),
        wm=pltpu.VMEM((mix_width, width), BF16),
        wgm=pltpu.VMEM((mix_width, width), BF16),
        mixw=pltpu.VMEM((SPAN, SPAN), BF16),
        wq=pltpu.VMEM((width, HD), BF16),
        wgr=pltpu.VMEM((width, HD), BF16),
        wkv=pltpu.VMEM((width, 2 * HD), BF16),
        wom=pltpu.VMEM((mix_width, width), BF16),
        wor=pltpu.VMEM((HD, width), BF16),
        rows_in=pltpu.VMEM((held, PROWS, width), BF16),
        rows_norm=pltpu.VMEM((PROWS, width), BF16),
        key_of=pltpu.VMEM((held, PROWS, HD), BF16),
        value_of=pltpu.VMEM((held, HD, PROWS), BF16),
        q_ring=[pltpu.VMEM((blocks, RBLOCK, HD), BF16) for _ in range(n_y)],
        q_sib=[pltpu.VMEM((blocks, RBLOCK, HD), BF16) for _ in range(n_y)],
        ids_all=pltpu.SMEM((n_st, blocks, NPB), jnp.int32),
        o_send=pltpu.VMEM((n_st, HD, 2 * RBLOCK), BF16),
        s_send=pltpu.VMEM((n_st, 2, 2 * RBLOCK), F32),
        ret_o=pltpu.VMEM((n_st, HD, 2 * RBLOCK), BF16),
        ret_s=pltpu.VMEM((n_st, 2, 2 * RBLOCK), F32),
        gate_t=pltpu.VMEM((HD, count), F32),
        out_mix=pltpu.VMEM((count, mix_width), BF16),
        out_read=pltpu.VMEM((count, HD), BF16),
        part=pltpu.VMEM((PIECES, count, columns), F32),
        rs_send=pltpu.VMEM((n_tp // 2, 2, PIECES, mine_rows, columns), BF16),
        rs_recv=pltpu.VMEM((n_tp // 2, 2, PIECES, mine_rows, columns), BF16),
        in_sem=dma((14,)),
        row_sem=dma((held,)),
        ids_send_sem=dma,
        ids_recv_sem=dma,
        ring_send_sem=dma,
        ring_recv_sem=dma((n_y,)),
        two_recv_sem=dma((2, 2)),
        sib_send_sem=dma,
        sib_recv_sem=dma((n_y,)),
        ret_send_sem=dma,
        ret_recv_sem=dma,
        stat_send_sem=dma,
        stat_recv_sem=dma,
        rs_send_sem=dma((2,)),
        rs_recv_sem=dma((n_tp // 2, 2, PIECES)),
    )
    names = list(scratch)

    def body(*refs):
        kernel(n_st, n_tp, *refs[:16], **dict(zip(names, refs[16:])))

    return pl.pallas_call(
        body,
        out_shape=jax.ShapeDtypeStruct((mine_rows, width), BF16),
        in_specs=specs,
        out_specs=vmem,
        scratch_shapes=list(scratch.values()),
        compiler_params=pltpu.CompilerParams(
            collective_id=0, has_side_effects=True, vmem_limit_bytes=67_000_000
        ),
        name="layer",
    )(*args)


def solution(mesh):
    placed = (
        P(("grp", "st"), None),
        P(),
        P(None, "tp"),
        P(None, "tp"),
        P("tp", None, None),
        P(None, "tp"),
        P(None, "tp"),
        P(None, "tp"),
        P(("grp", "st"), None, None),
        P(),
        P(None, "tp"),
        P(None, "tp"),
        P(("grp", "st"), None),
        P("tp", None),
        P("tp", None),
    )
    body = functools.partial(local, n_st=mesh.shape["st"], n_tp=mesh.shape["tp"])
    return jax.shard_map(
        body, mesh=mesh, in_specs=placed, out_specs=P(("grp", "st", "tp"), None), check_vma=False
    )
```

```python
import functools

import jax
import jax.numpy as jnp
from jax import lax
from jax.experimental import pallas as pl
from jax.experimental.pallas import tpu as pltpu
from jax.sharding import PartitionSpec as P

HD = 128
SPAN = 128
RBLOCK = 64
NPB = 4
PROWS = 128
NORM_ROWS = 32
PIECES = 2

MESH = pl.DeviceIdType.MESH
eps = 1e-06
F32 = jnp.float32
BF16 = jnp.bfloat16


def dot(a, b, dims=((1,), (0,))):
    return lax.dot_general(a, b, (dims, ((), ())), preferred_element_type=F32)


def row_norm(source, gain, target, rows):
    def some(i, carry):
        at = pl.ds(pl.multiple_of(i * NORM_ROWS, NORM_ROWS), NORM_ROWS)
        wide = source[at, :].astype(F32)
        scale = lax.rsqrt(jnp.mean(wide * wide, axis=-1, keepdims=True) + eps)
        target[at, :] = (wide * scale * gain).astype(BF16)
        return carry

    lax.fori_loop(0, rows // NORM_ROWS, some, 0)


def kernel(
    n_st,
    n_tp,
    tokens,
    pre_gain,
    w_gated,
    w_mixed,
    mix_weight,
    w_query,
    w_gate_mix,
    w_gate_read,
    store,
    mem_gain,
    w_key,
    w_value,
    ids,
    w_out_mix,
    w_out_read,
    out,
    tok,
    gains,
    own_ids,
    slot_of,
    normed,
    wg,
    wm,
    wgm,
    mixw,
    wq,
    wgr,
    wkv,
    wom,
    wor,
    rows_in,
    rows_norm,
    key_of,
    value_of,
    q_ring,
    q_sib,
    ids_all,
    o_send,
    s_send,
    ret_o,
    ret_s,
    gate_t,
    out_mix,
    out_read,
    part,
    rs_send,
    rs_recv,
    in_sem,
    row_sem,
    ids_send_sem,
    ids_recv_sem,
    ring_send_sem,
    ring_recv_sem,
    two_recv_sem,
    sib_send_sem,
    sib_recv_sem,
    ret_send_sem,
    ret_recv_sem,
    stat_send_sem,
    stat_recv_sem,
    rs_send_sem,
    rs_recv_sem,
):
    grp, st, tp = lax.axis_index("grp"), lax.axis_index("st"), lax.axis_index("tp")
    n_y = n_st // 2
    half_tp = n_tp // 2
    y, core = st // 2, lax.rem(st, 2)
    count = tok.shape[0]
    blocks = count // RBLOCK
    per_owner = rows_in.shape[0]
    mine_rows = count // n_tp

    def at_y(offset, sibling=False):
        chip = lax.rem(y + offset + n_y, n_y)
        return chip * 2 + (1 - core if sibling else core)

    def along_tp(offset):
        return lax.rem(tp + offset + n_tp, n_tp)

    def fetch(k, source, target):
        copy = pltpu.make_async_copy(source, target, in_sem.at[k])
        copy.start()
        return copy

    got_tok = fetch(0, tokens, tok)
    got_pre = fetch(11, pre_gain, gains.at[0])
    got_wq = fetch(1, w_query, wq)
    got_ids = fetch(12, ids, own_ids)

    barrier = pltpu.get_barrier_semaphore()
    peers = [(grp, lax.rem(st + k, n_st), tp) for k in range(1, n_st)]
    sides = [1, -1] if n_tp > 2 else [1]
    peers += [(grp, st, along_tp(k)) for k in sides]
    for peer in peers:
        pl.semaphore_signal(barrier, inc=1, device_id=peer, device_id_type=MESH)

    got_wk = fetch(2, w_key, wkv.at[:, 0:HD])
    got_wv = fetch(3, w_value, wkv.at[:, HD : 2 * HD])
    got_mem = fetch(13, mem_gain, gains.at[1])
    for p in range(per_owner):
        pltpu.make_async_copy(store.at[p], rows_in.at[p], row_sem.at[p]).start()
    got_wm = fetch(4, w_mixed, wm)
    got_wg = fetch(5, w_gated, wg)
    got_wgm = fetch(6, w_gate_mix, wgm)
    got_wgr = fetch(7, w_gate_read, wgr)
    got_mixw = fetch(8, mix_weight.at[0], mixw)
    got_wom = fetch(9, w_out_mix, wom)
    got_wor = fetch(10, w_out_read, wor)

    got_pre.wait()
    got_tok.wait()
    row_norm(tok, gains[0].reshape(1, -1), normed, count)
    got_wq.wait()
    own_q = dot(normed[...], wq[...]).astype(BF16)
    q_ring[0][...] = own_q.reshape(blocks, RBLOCK, HD)
    got_ids.wait()

    pl.semaphore_wait(barrier, len(peers))

    for k in range(1, n_st):
        pltpu.make_async_remote_copy(
            own_ids, ids_all.at[st], ids_send_sem, ids_recv_sem,
            device_id=(grp, lax.rem(st + k, n_st), tp), device_id_type=MESH,
        ).start()

    def drain(like, sem):
        pltpu.make_async_copy(like, like, sem).wait()

    cut = blocks // 2

    def push(j, after, h, offset):
        piece = pl.ds(h * cut, cut)
        recv = two_recv_sem.at[after // 4, h] if after in (2, n_y - 2) else ring_recv_sem.at[after]
        pltpu.make_async_remote_copy(
            q_ring[j].at[piece], q_ring[after].at[piece], ring_send_sem, recv,
            device_id=(grp, at_y(offset), tp), device_id_type=MESH,
        ).start()

    def across(j):
        pltpu.make_async_remote_copy(
            q_ring[j], q_sib[j], sib_send_sem, sib_recv_sem.at[j],
            device_id=(grp, at_y(0, True), tp), device_id_type=MESH,
        ).start()

    for h in range(2):
        push(0, 2, h, 2)
        push(0, n_y - 2, 1 - h, -2)
    for h in range(2):
        push(0, 1, h, 1)
        push(0, n_y - 1, 1 - h, -1)
    across(0)

    for b in range(blocks):
        for n in range(NPB):
            ids_all[st, b, n] = own_ids[b, n]

    got_wk.wait()
    got_wv.wait()
    got_mem.wait()
    mem_row = gains[1].reshape(1, -1)

    def keys_of(p, carry):
        pltpu.make_async_copy(store.at[p], rows_in.at[p], row_sem.at[p]).wait()
        row_norm(rows_in.at[p], mem_row, rows_norm, PROWS)
        both = dot(rows_norm[...], wkv[...])
        key_of[p] = both[:, :HD].astype(BF16)
        value_of[p] = jnp.transpose(both[:, HD:]).astype(BF16)
        return carry

    lax.fori_loop(0, per_owner, keys_of, 0)

    lanes = lax.broadcasted_iota(jnp.int32, (1, 2 * RBLOCK), 1)
    first_half = lanes < RBLOCK

    def attend(q_ref, reader):
        p0, p1, b0, b1 = (slot_of[reader, k] for k in range(4))
        q = jnp.concatenate([q_ref[b0], q_ref[b1]], axis=0)
        over_keys = ((1,), (1,))
        scores = jnp.where(
            first_half, dot(key_of[p0], q, over_keys), dot(key_of[p1], q, over_keys)
        ) * (HD ** (-0.5))
        top = jnp.max(scores, axis=0, keepdims=True)
        weight = jnp.exp(scores - top)
        total = jnp.sum(weight, axis=0, keepdims=True)
        weight = weight.astype(BF16)
        read = jnp.where(first_half, dot(value_of[p0], weight), dot(value_of[p1], weight))
        return read.astype(BF16), jnp.concatenate([top, total], axis=0)

    def serve(*labels):
        for j, sibling in labels:
            if sibling:
                drain(q_sib[j], sib_recv_sem.at[j])
        readers = [at_y(-j, sibling) for j, sibling in labels]
        results = [
            attend(q_sib[j] if sibling else q_ring[j], reader)
            for (j, sibling), reader in zip(labels, readers)
        ]
        for (j, sibling), (read, stats) in zip(labels, results):
            if j == 0 and not sibling:
                ret_o[st] = read
                ret_s[st] = stats
            else:
                o_send[j * 2 + sibling] = read
                s_send[j * 2 + sibling] = stats
        for (j, sibling), reader in zip(labels, readers):
            if j == 0 and not sibling:
                continue
            label = j * 2 + sibling
            for source, target, send, recv in (
                (o_send, ret_o, ret_send_sem, ret_recv_sem),
                (s_send, ret_s, stat_send_sem, stat_recv_sem),
            ):
                pltpu.make_async_remote_copy(
                    source.at[label], target.at[st], send, recv,
                    device_id=(grp, reader, tp), device_id_type=MESH,
                ).start()

    def forward(i):
        for j, near, h, sign in ((2, 3, i, 1), (n_y - 2, n_y - 3, 1 - i, -1)):
            drain(q_ring[j].at[pl.ds(h * cut, cut)], two_recv_sem.at[j // 4, h])
            if i == 0:
                push(j, 4, h, 2 * sign)
            push(j, near, h, sign)

    forward(0)

    drain(ids_all.at[pl.ds(0, n_st - 1)], ids_recv_sem)

    def slots(reader, carry):
        p0 = p1 = b0 = b1 = seen = jnp.int32(0)
        for b in range(blocks):
            for n in range(NPB):
                local = ids_all[reader, b, n] - st * per_owner
                mine = (local >= 0) & (local < per_owner)
                is0 = mine & (seen == 0)
                is1 = mine & (seen == 1)
                p0, b0 = jnp.where(is0, local, p0), jnp.where(is0, b, b0)
                p1, b1 = jnp.where(is1, local, p1), jnp.where(is1, b, b1)
                seen = seen + jnp.where(mine, 1, 0)
        for k, value in enumerate((p0, p1, b0, b1)):
            slot_of[reader, k] = value
        return carry

    lax.fori_loop(0, n_st, slots, 0, unroll=4)

    forward(1)
    for j in (1, n_y - 1):
        drain(q_ring[j], ring_recv_sem.at[j])
        across(j)
    for j in (2, n_y - 2):
        across(j)

    serve((1, 0), (n_y - 1, 0))
    serve((2, 0), (n_y - 2, 0))
    serve((1, 1), (n_y - 1, 1))
    serve((2, 1), (n_y - 2, 1))

    for j in (3, n_y - 3, 4):
        drain(q_ring[j], ring_recv_sem.at[j])
        across(j)
    serve((4, 0), (3, 0), (n_y - 3, 0))
    serve((4, 1), (3, 1), (n_y - 3, 1))
    serve((0, 0), (0, 1))

    got_wm.wait()
    over_width = ((1,), (1,))
    mixed_in = dot(normed[...], wm[...], over_width)
    centred = mixed_in - jnp.mean(mixed_in, axis=-1, keepdims=True)
    variance = jnp.mean(centred * centred, axis=-1, keepdims=True)
    mixed_norm = (centred * lax.rsqrt(variance + eps)).astype(BF16)
    got_mixw.wait()
    row_at = lax.broadcasted_iota(jnp.int32, (SPAN, SPAN), 0)
    col_at = lax.broadcasted_iota(jnp.int32, (SPAN, SPAN), 1)
    causal = jnp.where(col_at <= row_at, mixw[...].astype(F32), 0.0).astype(BF16)
    spatial = jnp.concatenate(
        [dot(causal, mixed_norm[n * SPAN : (n + 1) * SPAN]) for n in range(count // SPAN)], axis=0
    )
    got_wg.wait()
    branch_mix = dot(normed[...], wg[...], over_width) * spatial
    got_wgm.wait()
    gate = dot(normed[...], wgm[...], over_width)
    out_mix[...] = (branch_mix * (gate / (1.0 + jnp.exp(-gate)))).astype(BF16)
    got_wgr.wait()
    gate = dot(normed[...], wgr[...])
    gate_t[...] = jnp.transpose(gate / (1.0 + jnp.exp(-gate)))
    got_wom.wait()
    width = part.shape[2]
    for c in range(PIECES):
        part[c] = dot(out_mix[...], wom[:, c * width : (c + 1) * width])

    owners, ranks = [], []
    for e in range(blocks * NPB):
        owner = own_ids[e // NPB, e % NPB] // per_owner
        rank = jnp.int32(0)
        for before in owners:
            rank = rank + jnp.where(before == owner, 1, 0)
        owners.append(owner)
        ranks.append(rank)
    drain(ret_o.at[pl.ds(0, n_st - 1)], ret_recv_sem)
    drain(ret_s.at[pl.ds(0, n_st - 1)], stat_recv_sem)
    got_wor.wait()
    for pair in range(blocks // 2):
        tops, totals, reads = [], [], []
        for n in range(NPB):
            e0, e1 = pair * 2 * NPB + n, (pair * 2 + 1) * NPB + n

            def placed(ref):
                x0, x1 = ref[owners[e0]].astype(F32), ref[owners[e1]].astype(F32)
                low = jnp.where(ranks[e0] == 0, x0, pltpu.roll(x0, RBLOCK, 1))
                high = jnp.where(ranks[e1] == 1, x1, pltpu.roll(x1, RBLOCK, 1))
                return jnp.where(first_half, low, high)

            stats = placed(ret_s)
            tops.append(stats[0:1])
            totals.append(stats[1:2])
            reads.append(placed(ret_o))
        top = functools.reduce(jnp.maximum, tops)
        scales = [jnp.exp(t - top) for t in tops]
        total = sum(s * t for s, t in zip(scales, totals))
        read = sum(s * r for s, r in zip(scales, reads)) / total
        cols = slice(pair * 2 * RBLOCK, (pair + 1) * 2 * RBLOCK)
        out_read[cols, :] = jnp.transpose(read * gate_t[:, cols]).astype(BF16)

    rs_copies = {}

    def pass_on(c, d, k):
        sign = 1 - 2 * d
        target = along_tp(sign * k)
        lo = 0
        size = mine_rows
        if k == half_tp:
            size = mine_rows // 2
            lo = d * size
        start = pl.multiple_of(target * mine_rows + lo, mine_rows // 2)
        value = part[c, pl.ds(start, size), :]
        if k == half_tp:
            rs_send[k - 1, d, c, lo : lo + size, :] = value.astype(BF16)
        else:
            rs_copies[c, d, k + 1].wait_recv()
            if k + 1 == half_tp:
                cut_rows = mine_rows // 2
                low = d * cut_rows
                rs_send[k - 1, d, c, low : low + cut_rows, :] = (
                    part[c, pl.ds(pl.multiple_of(target * mine_rows + low, cut_rows), cut_rows), :]
                    + rs_recv[k, d, c, low : low + cut_rows, :].astype(F32)
                ).astype(BF16)
                other = cut_rows - low
                rs_send[k - 1, d, c, other : other + cut_rows, :] = part[
                    c, pl.ds(pl.multiple_of(target * mine_rows + other, cut_rows), cut_rows), :
                ].astype(BF16)
            else:
                rs_send[k - 1, d, c] = (value + rs_recv[k, d, c].astype(F32)).astype(BF16)
        copy = pltpu.make_async_remote_copy(
            rs_send.at[k - 1, d, c, pl.ds(lo, size)], rs_recv.at[k - 1, d, c, pl.ds(lo, size)],
            rs_send_sem.at[k // half_tp], rs_recv_sem.at[k - 1, d, c],
            device_id=(grp, st, along_tp(sign)), device_id_type=MESH,
        )
        copy.start()
        rs_copies[c, d, k] = copy

    for c in range(PIECES):
        part[c] = part[c] + dot(out_read[...], wor[:, c * width : (c + 1) * width])
        for d in range(2):
            pass_on(c, d, half_tp)
    for k in range(half_tp - 1, 0, -1):
        for c in range(PIECES):
            for d in range(2):
                pass_on(c, d, k)
    here = pl.ds(pl.multiple_of(tp * mine_rows, mine_rows), mine_rows)
    for c in range(PIECES):
        for d in range(2):
            rs_copies[c, d, 1].wait_recv()
        if half_tp == 1:
            cut_rows = mine_rows // 2
            both = jnp.concatenate(
                [rs_recv[0, 0, c, :cut_rows, :], rs_recv[0, 1, c, cut_rows:, :]], axis=0
            ).astype(F32)
        else:
            both = rs_recv[0, 0, c].astype(F32) + rs_recv[0, 1, c].astype(F32)
        out[:, c * width : (c + 1) * width] = (part[c, here, :] + both).astype(BF16)

    drain(ids_all.at[pl.ds(0, n_st - 1)], ids_send_sem)
    drain(o_send.at[pl.ds(0, 2 * (n_y - 1))], ring_send_sem)
    drain(o_send, sib_send_sem)
    drain(o_send.at[pl.ds(0, n_st - 1)], ret_send_sem)
    drain(s_send.at[pl.ds(0, n_st - 1)], stat_send_sem)
    drain(rs_send.at[half_tp - 1, 0], rs_send_sem.at[1])
    if half_tp > 1:
        drain(rs_send.at[pl.ds(0, half_tp - 1)], rs_send_sem.at[0])


def local(*args, n_st, n_tp):
    args = [a.T if k in (2, 3, 6) else a for k, a in enumerate(args)]
    tokens, w_gated, store = args[0], args[2], args[8]
    count, width = tokens.shape
    mix_width = w_gated.shape[0]
    held = store.shape[0]
    blocks = count // RBLOCK
    n_y = n_st // 2
    mine_rows = count // n_tp
    hbm = pl.BlockSpec(memory_space=pltpu.HBM)
    vmem = pl.BlockSpec(memory_space=pltpu.VMEM)
    specs = [hbm] * 15
    dma = pltpu.SemaphoreType.DMA
    columns = width // PIECES
    scratch = dict(
        tok=pltpu.VMEM((count, width), BF16),
        gains=pltpu.VMEM((2, width), F32),
        own_ids=pltpu.SMEM((blocks, NPB), jnp.int32),
        slot_of=pltpu.SMEM((n_st, 4), jnp.int32),
        normed=pltpu.VMEM((count, width), BF16),
        wg=pltpu.VMEM((mix_width, width), BF16),
        wm=pltpu.VMEM((mix_width, width), BF16),
        wgm=pltpu.VMEM((mix_width, width), BF16),
        mixw=pltpu.VMEM((SPAN, SPAN), BF16),
        wq=pltpu.VMEM((width, HD), BF16),
        wgr=pltpu.VMEM((width, HD), BF16),
        wkv=pltpu.VMEM((width, 2 * HD), BF16),
        wom=pltpu.VMEM((mix_width, width), BF16),
        wor=pltpu.VMEM((HD, width), BF16),
        rows_in=pltpu.VMEM((held, PROWS, width), BF16),
        rows_norm=pltpu.VMEM((PROWS, width), BF16),
        key_of=pltpu.VMEM((held, PROWS, HD), BF16),
        value_of=pltpu.VMEM((held, HD, PROWS), BF16),
        q_ring=[pltpu.VMEM((blocks, RBLOCK, HD), BF16) for _ in range(n_y)],
        q_sib=[pltpu.VMEM((blocks, RBLOCK, HD), BF16) for _ in range(n_y)],
        ids_all=pltpu.SMEM((n_st, blocks, NPB), jnp.int32),
        o_send=pltpu.VMEM((n_st, HD, 2 * RBLOCK), BF16),
        s_send=pltpu.VMEM((n_st, 2, 2 * RBLOCK), F32),
        ret_o=pltpu.VMEM((n_st, HD, 2 * RBLOCK), BF16),
        ret_s=pltpu.VMEM((n_st, 2, 2 * RBLOCK), F32),
        gate_t=pltpu.VMEM((HD, count), F32),
        out_mix=pltpu.VMEM((count, mix_width), BF16),
        out_read=pltpu.VMEM((count, HD), BF16),
        part=pltpu.VMEM((PIECES, count, columns), F32),
        rs_send=pltpu.VMEM((n_tp // 2, 2, PIECES, mine_rows, columns), BF16),
        rs_recv=pltpu.VMEM((n_tp // 2, 2, PIECES, mine_rows, columns), BF16),
        in_sem=dma((14,)),
        row_sem=dma((held,)),
        ids_send_sem=dma,
        ids_recv_sem=dma,
        ring_send_sem=dma,
        ring_recv_sem=dma((n_y,)),
        two_recv_sem=dma((2, 2)),
        sib_send_sem=dma,
        sib_recv_sem=dma((n_y,)),
        ret_send_sem=dma,
        ret_recv_sem=dma,
        stat_send_sem=dma,
        stat_recv_sem=dma,
        rs_send_sem=dma((2,)),
        rs_recv_sem=dma((n_tp // 2, 2, PIECES)),
    )
    names = list(scratch)

    def body(*refs):
        kernel(n_st, n_tp, *refs[:16], **dict(zip(names, refs[16:])))

    return pl.pallas_call(
        body,
        out_shape=jax.ShapeDtypeStruct((mine_rows, width), BF16),
        in_specs=specs,
        out_specs=vmem,
        scratch_shapes=list(scratch.values()),
        compiler_params=pltpu.CompilerParams(
            collective_id=0, has_side_effects=True, vmem_limit_bytes=67_000_000
        ),
        name="layer",
    )(*args)


def solution(mesh):
    placed = (
        P(("grp", "st"), None),
        P(),
        P(None, "tp"),
        P(None, "tp"),
        P("tp", None, None),
        P(None, "tp"),
        P(None, "tp"),
        P(None, "tp"),
        P(("grp", "st"), None, None),
        P(),
        P(None, "tp"),
        P(None, "tp"),
        P(("grp", "st"), None),
        P("tp", None),
        P("tp", None),
    )
    body = functools.partial(local, n_st=mesh.shape["st"], n_tp=mesh.shape["tp"])
    return jax.shard_map(
        body, mesh=mesh, in_specs=placed, out_specs=P(("grp", "st", "tp"), None), check_vma=False
    )
```

```python
import functools

import jax
import jax.numpy as jnp
from jax import lax
from jax.experimental import pallas as pl
from jax.experimental.pallas import tpu as pltpu
from jax.sharding import PartitionSpec as P

HD = 128
SPAN = 128
RBLOCK = 64
NPB = 4
PROWS = 128
NORM_ROWS = 32
PIECES = 2

MESH = pl.DeviceIdType.MESH
eps = 1e-06
F32 = jnp.float32
BF16 = jnp.bfloat16


def dot(a, b, dims=((1,), (0,))):
    return lax.dot_general(a, b, (dims, ((), ())), preferred_element_type=F32)


def row_norm(source, gain, target, rows):
    def some(i, carry):
        at = pl.ds(pl.multiple_of(i * NORM_ROWS, NORM_ROWS), NORM_ROWS)
        wide = source[at, :].astype(F32)
        scale = lax.rsqrt(jnp.mean(wide * wide, axis=-1, keepdims=True) + eps)
        target[at, :] = (wide * scale * gain).astype(BF16)
        return carry

    lax.fori_loop(0, rows // NORM_ROWS, some, 0)


def kernel(
    n_st,
    n_tp,
    tokens,
    pre_gain,
    w_gated,
    w_mixed,
    mix_weight,
    w_query,
    w_gate_mix,
    w_gate_read,
    store,
    mem_gain,
    w_key,
    w_value,
    ids,
    w_out_mix,
    w_out_read,
    out,
    tok,
    gains,
    own_ids,
    slot_of,
    normed,
    wg,
    wm,
    wgm,
    mixw,
    wq,
    wgr,
    wkv,
    wom,
    wor,
    rows_in,
    rows_norm,
    key_of,
    value_of,
    q_ring,
    q_sib,
    ids_all,
    o_send,
    s_send,
    ret_o,
    ret_s,
    gate_t,
    out_mix,
    out_read,
    part,
    rs_send,
    rs_recv,
    in_sem,
    row_sem,
    ids_send_sem,
    ids_recv_sem,
    ring_send_sem,
    ring_recv_sem,
    two_recv_sem,
    sib_send_sem,
    sib_recv_sem,
    ret_send_sem,
    ret_recv_sem,
    stat_send_sem,
    stat_recv_sem,
    rs_send_sem,
    rs_recv_sem,
):
    grp, st, tp = lax.axis_index("grp"), lax.axis_index("st"), lax.axis_index("tp")
    n_y = n_st // 2
    half_tp = n_tp // 2
    y, core = st // 2, lax.rem(st, 2)
    count = tok.shape[0]
    blocks = count // RBLOCK
    per_owner = rows_in.shape[0]
    mine_rows = count // n_tp

    def at_y(offset, sibling=False):
        chip = lax.rem(y + offset + n_y, n_y)
        return chip * 2 + (1 - core if sibling else core)

    def along_tp(offset):
        return lax.rem(tp + offset + n_tp, n_tp)

    def fetch(k, source, target):
        copy = pltpu.make_async_copy(source, target, in_sem.at[k])
        copy.start()
        return copy

    got_tok = fetch(0, tokens, tok)
    got_pre = fetch(11, pre_gain, gains.at[0])
    got_wq = fetch(1, w_query, wq)
    got_ids = fetch(12, ids, own_ids)

    barrier = pltpu.get_barrier_semaphore()
    peers = [(grp, lax.rem(st + k, n_st), tp) for k in range(1, n_st)]
    sides = [1, -1] if n_tp > 2 else [1]
    peers += [(grp, st, along_tp(k)) for k in sides]
    for peer in peers:
        pl.semaphore_signal(barrier, inc=1, device_id=peer, device_id_type=MESH)

    got_wk = fetch(2, w_key, wkv.at[:, 0:HD])
    got_wv = fetch(3, w_value, wkv.at[:, HD : 2 * HD])
    got_mem = fetch(13, mem_gain, gains.at[1])
    for p in range(per_owner):
        pltpu.make_async_copy(store.at[p], rows_in.at[p], row_sem.at[p]).start()
    got_wm = fetch(4, w_mixed, wm)
    got_wg = fetch(5, w_gated, wg)
    got_wgm = fetch(6, w_gate_mix, wgm)
    got_wgr = fetch(7, w_gate_read, wgr)
    got_mixw = fetch(8, mix_weight.at[0], mixw)
    got_wom = fetch(9, w_out_mix, wom)
    got_wor = fetch(10, w_out_read, wor)

    got_pre.wait()
    got_tok.wait()
    row_norm(tok, gains[0].reshape(1, -1), normed, count)
    got_wq.wait()
    own_q = dot(normed[...], wq[...]).astype(BF16)
    q_ring[0][...] = own_q.reshape(blocks, RBLOCK, HD)
    got_ids.wait()

    pl.semaphore_wait(barrier, len(peers))

    for k in range(1, n_st):
        pltpu.make_async_remote_copy(
            own_ids, ids_all.at[st], ids_send_sem, ids_recv_sem,
            device_id=(grp, lax.rem(st + k, n_st), tp), device_id_type=MESH,
        ).start()

    def drain(like, sem):
        pltpu.make_async_copy(like, like, sem).wait()

    cut = blocks // 2

    def push(j, after, h, offset):
        piece = pl.ds(h * cut, cut)
        recv = two_recv_sem.at[after // 4, h] if after in (2, n_y - 2) else ring_recv_sem.at[after]
        pltpu.make_async_remote_copy(
            q_ring[j].at[piece], q_ring[after].at[piece], ring_send_sem, recv,
            device_id=(grp, at_y(offset), tp), device_id_type=MESH,
        ).start()

    def across(j):
        pltpu.make_async_remote_copy(
            q_ring[j], q_sib[j], sib_send_sem, sib_recv_sem.at[j],
            device_id=(grp, at_y(0, True), tp), device_id_type=MESH,
        ).start()

    for h in range(2):
        push(0, 2, h, 2)
        push(0, n_y - 2, 1 - h, -2)
    for h in range(2):
        push(0, 1, h, 1)
        push(0, n_y - 1, 1 - h, -1)
    across(0)

    for b in range(blocks):
        for n in range(NPB):
            ids_all[st, b, n] = own_ids[b, n]

    got_wk.wait()
    got_wv.wait()
    got_mem.wait()
    mem_row = gains[1].reshape(1, -1)

    def keys_of(p, carry):
        pltpu.make_async_copy(store.at[p], rows_in.at[p], row_sem.at[p]).wait()
        row_norm(rows_in.at[p], mem_row, rows_norm, PROWS)
        both = dot(rows_norm[...], wkv[...])
        key_of[p] = both[:, :HD].astype(BF16)
        value_of[p] = jnp.transpose(both[:, HD:]).astype(BF16)
        return carry

    lax.fori_loop(0, per_owner, keys_of, 0)

    lanes = lax.broadcasted_iota(jnp.int32, (1, 2 * RBLOCK), 1)
    first_half = lanes < RBLOCK

    def attend(q_ref, reader):
        p0, p1, b0, b1 = (slot_of[reader, k] for k in range(4))
        q = jnp.concatenate([q_ref[b0], q_ref[b1]], axis=0)
        over_keys = ((1,), (1,))
        scores = jnp.where(
            first_half, dot(key_of[p0], q, over_keys), dot(key_of[p1], q, over_keys)
        ) * (HD ** (-0.5))
        top = jnp.max(scores, axis=0, keepdims=True)
        weight = jnp.exp(scores - top)
        total = jnp.sum(weight, axis=0, keepdims=True)
        weight = weight.astype(BF16)
        read = jnp.where(first_half, dot(value_of[p0], weight), dot(value_of[p1], weight))
        return read.astype(BF16), jnp.concatenate([top, total], axis=0)

    def serve(*labels):
        for j, sibling in labels:
            if sibling:
                drain(q_sib[j], sib_recv_sem.at[j])
        readers = [at_y(-j, sibling) for j, sibling in labels]
        results = [
            attend(q_sib[j] if sibling else q_ring[j], reader)
            for (j, sibling), reader in zip(labels, readers)
        ]
        for (j, sibling), (read, stats) in zip(labels, results):
            if j == 0 and not sibling:
                ret_o[st] = read
                ret_s[st] = stats
            else:
                o_send[j * 2 + sibling] = read
                s_send[j * 2 + sibling] = stats
        for (j, sibling), reader in zip(labels, readers):
            if j == 0 and not sibling:
                continue
            label = j * 2 + sibling
            for source, target, send, recv in (
                (o_send, ret_o, ret_send_sem, ret_recv_sem),
                (s_send, ret_s, stat_send_sem, stat_recv_sem),
            ):
                pltpu.make_async_remote_copy(
                    source.at[label], target.at[st], send, recv,
                    device_id=(grp, reader, tp), device_id_type=MESH,
                ).start()

    def forward(i):
        for j, near, h, sign in ((2, 3, i, 1), (n_y - 2, n_y - 3, 1 - i, -1)):
            drain(q_ring[j].at[pl.ds(h * cut, cut)], two_recv_sem.at[j // 4, h])
            if i == 0:
                push(j, 4, h, 2 * sign)
            push(j, near, h, sign)

    forward(0)

    drain(ids_all.at[pl.ds(0, n_st - 1)], ids_recv_sem)

    def slots(reader, carry):
        p0 = p1 = b0 = b1 = seen = jnp.int32(0)
        for b in range(blocks):
            for n in range(NPB):
                local = ids_all[reader, b, n] - st * per_owner
                mine = (local >= 0) & (local < per_owner)
                is0 = mine & (seen == 0)
                is1 = mine & (seen == 1)
                p0, b0 = jnp.where(is0, local, p0), jnp.where(is0, b, b0)
                p1, b1 = jnp.where(is1, local, p1), jnp.where(is1, b, b1)
                seen = seen + jnp.where(mine, 1, 0)
        for k, value in enumerate((p0, p1, b0, b1)):
            slot_of[reader, k] = value
        return carry

    lax.fori_loop(0, n_st, slots, 0, unroll=4)

    forward(1)
    for j in (1, n_y - 1):
        drain(q_ring[j], ring_recv_sem.at[j])
        across(j)
    for j in (2, n_y - 2):
        across(j)

    serve((1, 0), (n_y - 1, 0))
    serve((2, 0), (n_y - 2, 0))
    serve((1, 1), (n_y - 1, 1))
    serve((2, 1), (n_y - 2, 1))

    for j in (3, n_y - 3, 4):
        drain(q_ring[j], ring_recv_sem.at[j])
        across(j)
    serve((4, 0), (3, 0), (n_y - 3, 0))
    serve((4, 1), (3, 1), (n_y - 3, 1))
    serve((0, 0), (0, 1))

    got_wm.wait()
    over_width = ((1,), (1,))
    mixed_in = dot(normed[...], wm[...], over_width)
    centred = mixed_in - jnp.mean(mixed_in, axis=-1, keepdims=True)
    variance = jnp.mean(centred * centred, axis=-1, keepdims=True)
    mixed_norm = (centred * lax.rsqrt(variance + eps)).astype(BF16)
    got_mixw.wait()
    row_at = lax.broadcasted_iota(jnp.int32, (SPAN, SPAN), 0)
    col_at = lax.broadcasted_iota(jnp.int32, (SPAN, SPAN), 1)
    causal = jnp.where(col_at <= row_at, mixw[...].astype(F32), 0.0).astype(BF16)
    spatial = jnp.concatenate(
        [dot(causal, mixed_norm[n * SPAN : (n + 1) * SPAN]) for n in range(count // SPAN)], axis=0
    )
    got_wg.wait()
    branch_mix = dot(normed[...], wg[...], over_width) * spatial
    got_wgm.wait()
    gate = dot(normed[...], wgm[...], over_width)
    out_mix[...] = (branch_mix * (gate / (1.0 + jnp.exp(-gate)))).astype(BF16)
    got_wgr.wait()
    gate = dot(normed[...], wgr[...])
    gate_t[...] = jnp.transpose(gate / (1.0 + jnp.exp(-gate)))
    got_wom.wait()
    width = part.shape[2]
    for c in range(PIECES):
        part[c] = dot(out_mix[...], wom[:, c * width : (c + 1) * width])

    owners, ranks = [], []
    for e in range(blocks * NPB):
        owner = own_ids[e // NPB, e % NPB] // per_owner
        rank = jnp.int32(0)
        for before in owners:
            rank = rank + jnp.where(before == owner, 1, 0)
        owners.append(owner)
        ranks.append(rank)
    drain(ret_o.at[pl.ds(0, n_st - 1)], ret_recv_sem)
    drain(ret_s.at[pl.ds(0, n_st - 1)], stat_recv_sem)
    got_wor.wait()
    for pair in range(blocks // 2):
        tops, totals, reads = [], [], []
        for n in range(NPB):
            e0, e1 = pair * 2 * NPB + n, (pair * 2 + 1) * NPB + n

            def placed(ref):
                x0, x1 = ref[owners[e0]].astype(F32), ref[owners[e1]].astype(F32)
                low = jnp.where(ranks[e0] == 0, x0, pltpu.roll(x0, RBLOCK, 1))
                high = jnp.where(ranks[e1] == 1, x1, pltpu.roll(x1, RBLOCK, 1))
                return jnp.where(first_half, low, high)

            stats = placed(ret_s)
            tops.append(stats[0:1])
            totals.append(stats[1:2])
            reads.append(placed(ret_o))
        top = functools.reduce(jnp.maximum, tops)
        scales = [jnp.exp(t - top) for t in tops]
        total = sum(s * t for s, t in zip(scales, totals))
        read = sum(s * r for s, r in zip(scales, reads)) / total
        cols = slice(pair * 2 * RBLOCK, (pair + 1) * 2 * RBLOCK)
        out_read[cols, :] = jnp.transpose(read * gate_t[:, cols]).astype(BF16)

    rs_copies = {}

    def pass_on(c, d, k):
        sign = 1 - 2 * d
        target = along_tp(sign * k)
        lo = 0
        size = mine_rows
        if k == half_tp:
            size = mine_rows // 2
            lo = d * size
        start = pl.multiple_of(target * mine_rows + lo, mine_rows // 2)
        value = part[c, pl.ds(start, size), :]
        if k == half_tp:
            rs_send[k - 1, d, c, lo : lo + size, :] = value.astype(BF16)
        else:
            rs_copies[c, d, k + 1].wait_recv()
            if k + 1 == half_tp:
                cut_rows = mine_rows // 2
                low = d * cut_rows
                rs_send[k - 1, d, c, low : low + cut_rows, :] = (
                    part[c, pl.ds(pl.multiple_of(target * mine_rows + low, cut_rows), cut_rows), :]
                    + rs_recv[k, d, c, low : low + cut_rows, :].astype(F32)
                ).astype(BF16)
                other = cut_rows - low
                rs_send[k - 1, d, c, other : other + cut_rows, :] = part[
                    c, pl.ds(pl.multiple_of(target * mine_rows + other, cut_rows), cut_rows), :
                ].astype(BF16)
            else:
                rs_send[k - 1, d, c] = (value + rs_recv[k, d, c].astype(F32)).astype(BF16)
        copy = pltpu.make_async_remote_copy(
            rs_send.at[k - 1, d, c, pl.ds(lo, size)], rs_recv.at[k - 1, d, c, pl.ds(lo, size)],
            rs_send_sem.at[k // half_tp], rs_recv_sem.at[k - 1, d, c],
            device_id=(grp, st, along_tp(sign)), device_id_type=MESH,
        )
        copy.start()
        rs_copies[c, d, k] = copy

    for c in range(PIECES):
        part[c] = part[c] + dot(out_read[...], wor[:, c * width : (c + 1) * width])
        for d in range(2):
            pass_on(c, d, half_tp)
    for k in range(half_tp - 1, 0, -1):
        for c in range(PIECES):
            for d in range(2):
                pass_on(c, d, k)
    here = pl.ds(pl.multiple_of(tp * mine_rows, mine_rows), mine_rows)
    for c in range(PIECES):
        for d in range(2):
            rs_copies[c, d, 1].wait_recv()
        if half_tp == 1:
            cut_rows = mine_rows // 2
            both = jnp.concatenate(
                [rs_recv[0, 0, c, :cut_rows, :], rs_recv[0, 1, c, cut_rows:, :]], axis=0
            ).astype(F32)
        else:
            both = rs_recv[0, 0, c].astype(F32) + rs_recv[0, 1, c].astype(F32)
        out[:, c * width : (c + 1) * width] = (part[c, here, :] + both).astype(BF16)

    drain(ids_all.at[pl.ds(0, n_st - 1)], ids_send_sem)
    drain(o_send.at[pl.ds(0, 2 * (n_y - 1))], ring_send_sem)
    drain(o_send, sib_send_sem)
    drain(o_send.at[pl.ds(0, n_st - 1)], ret_send_sem)
    drain(s_send.at[pl.ds(0, n_st - 1)], stat_send_sem)
    drain(rs_send.at[half_tp - 1, 0], rs_send_sem.at[1])
    if half_tp > 1:
        drain(rs_send.at[pl.ds(0, half_tp - 1)], rs_send_sem.at[0])


def local(*args, n_st, n_tp):
    args = [a.T if k in (2, 3, 6) else a for k, a in enumerate(args)]
    tokens, w_gated, store = args[0], args[2], args[8]
    count, width = tokens.shape
    mix_width = w_gated.shape[0]
    held = store.shape[0]
    blocks = count // RBLOCK
    n_y = n_st // 2
    mine_rows = count // n_tp
    hbm = pl.BlockSpec(memory_space=pltpu.HBM)
    vmem = pl.BlockSpec(memory_space=pltpu.VMEM)
    specs = [hbm] * 15
    dma = pltpu.SemaphoreType.DMA
    columns = width // PIECES
    scratch = dict(
        tok=pltpu.VMEM((count, width), BF16),
        gains=pltpu.VMEM((2, width), F32),
        own_ids=pltpu.SMEM((blocks, NPB), jnp.int32),
        slot_of=pltpu.SMEM((n_st, 4), jnp.int32),
        normed=pltpu.VMEM((count, width), BF16),
        wg=pltpu.VMEM((mix_width, width), BF16),
        wm=pltpu.VMEM((mix_width, width), BF16),
        wgm=pltpu.VMEM((mix_width, width), BF16),
        mixw=pltpu.VMEM((SPAN, SPAN), BF16),
        wq=pltpu.VMEM((width, HD), BF16),
        wgr=pltpu.VMEM((width, HD), BF16),
        wkv=pltpu.VMEM((width, 2 * HD), BF16),
        wom=pltpu.VMEM((mix_width, width), BF16),
        wor=pltpu.VMEM((HD, width), BF16),
        rows_in=pltpu.VMEM((held, PROWS, width), BF16),
        rows_norm=pltpu.VMEM((PROWS, width), BF16),
        key_of=pltpu.VMEM((held, PROWS, HD), BF16),
        value_of=pltpu.VMEM((held, HD, PROWS), BF16),
        q_ring=[pltpu.VMEM((blocks, RBLOCK, HD), BF16) for _ in range(n_y)],
        q_sib=[pltpu.VMEM((blocks, RBLOCK, HD), BF16) for _ in range(n_y)],
        ids_all=pltpu.SMEM((n_st, blocks, NPB), jnp.int32),
        o_send=pltpu.VMEM((n_st, HD, 2 * RBLOCK), BF16),
        s_send=pltpu.VMEM((n_st, 2, 2 * RBLOCK), F32),
        ret_o=pltpu.VMEM((n_st, HD, 2 * RBLOCK), BF16),
        ret_s=pltpu.VMEM((n_st, 2, 2 * RBLOCK), F32),
        gate_t=pltpu.VMEM((HD, count), F32),
        out_mix=pltpu.VMEM((count, mix_width), BF16),
        out_read=pltpu.VMEM((count, HD), BF16),
        part=pltpu.VMEM((PIECES, count, columns), F32),
        rs_send=pltpu.VMEM((n_tp // 2, 2, PIECES, mine_rows, columns), BF16),
        rs_recv=pltpu.VMEM((n_tp // 2, 2, PIECES, mine_rows, columns), BF16),
        in_sem=dma((14,)),
        row_sem=dma((held,)),
        ids_send_sem=dma,
        ids_recv_sem=dma,
        ring_send_sem=dma,
        ring_recv_sem=dma((n_y,)),
        two_recv_sem=dma((2, 2)),
        sib_send_sem=dma,
        sib_recv_sem=dma((n_y,)),
        ret_send_sem=dma,
        ret_recv_sem=dma,
        stat_send_sem=dma,
        stat_recv_sem=dma,
        rs_send_sem=dma((2,)),
        rs_recv_sem=dma((n_tp // 2, 2, PIECES)),
    )
    names = list(scratch)

    def body(*refs):
        kernel(n_st, n_tp, *refs[:16], **dict(zip(names, refs[16:])))

    return pl.pallas_call(
        body,
        out_shape=pltpu.VMEM((mine_rows, width), BF16),
        in_specs=specs,
        out_specs=vmem,
        scratch_shapes=list(scratch.values()),
        compiler_params=pltpu.CompilerParams(
            collective_id=0, has_side_effects=True, vmem_limit_bytes=66_800_000
        ),
        name="layer",
    )(*args)


def solution(mesh):
    placed = (
        P(("grp", "st"), None),
        P(),
        P(None, "tp"),
        P(None, "tp"),
        P("tp", None, None),
        P(None, "tp"),
        P(None, "tp"),
        P(None, "tp"),
        P(("grp", "st"), None, None),
        P(),
        P(None, "tp"),
        P(None, "tp"),
        P(("grp", "st"), None),
        P("tp", None),
        P("tp", None),
    )
    body = functools.partial(local, n_st=mesh.shape["st"], n_tp=mesh.shape["tp"])
    return jax.shard_map(
        body, mesh=mesh, in_specs=placed, out_specs=P(("grp", "st", "tp"), None), check_vma=False
    )
```

```python
import functools

import jax
import jax.numpy as jnp
from jax import lax
from jax.experimental import pallas as pl
from jax.experimental.pallas import tpu as pltpu
from jax.sharding import PartitionSpec as P

HD = 128
SPAN = 128
RBLOCK = 64
NPB = 4
PROWS = 128
NORM_ROWS = 32
PIECES = 2

MESH = pl.DeviceIdType.MESH
eps = 1e-06
F32 = jnp.float32
BF16 = jnp.bfloat16


def dot(a, b, dims=((1,), (0,))):
    return lax.dot_general(a, b, (dims, ((), ())), preferred_element_type=F32)


def row_norm(source, gain, target, low, high):
    for at in range(low, high, NORM_ROWS):
        wide = source[at : at + NORM_ROWS, :].astype(F32)
        scale = lax.rsqrt(jnp.mean(wide * wide, axis=-1, keepdims=True) + eps)
        target[at : at + NORM_ROWS, :] = (wide * scale * gain).astype(BF16)


def kernel(
    n_st,
    n_tp,
    tokens,
    pre_gain,
    w_gated,
    w_mixed,
    mix_weight,
    w_query,
    w_gate_mix,
    w_gate_read,
    store,
    mem_gain,
    w_key,
    w_value,
    ids,
    w_out_mix,
    w_out_read,
    out,
    tok,
    gains,
    own_ids,
    slot_of,
    normed,
    wg,
    wm,
    wgm,
    mixw,
    wq,
    wgr,
    wkv,
    wom,
    wor,
    rows_in,
    norm_even,
    norm_odd,
    key_of,
    value_of,
    q_ring,
    q_sib,
    ids_all,
    o_send,
    s_send,
    ret_o,
    ret_s,
    gate_t,
    out_mix,
    out_read,
    part,
    rs_send,
    rs_recv,
    in_sem,
    row_sem,
    ids_send_sem,
    ids_recv_sem,
    ring_send_sem,
    ring_recv_sem,
    two_recv_sem,
    sib_send_sem,
    sib_recv_sem,
    ret_send_sem,
    ret_recv_sem,
    stat_send_sem,
    stat_recv_sem,
    rs_send_sem,
    rs_recv_sem,
):
    grp, st, tp = lax.axis_index("grp"), lax.axis_index("st"), lax.axis_index("tp")
    n_y = n_st // 2
    half_tp = n_tp // 2
    y, core = st // 2, lax.rem(st, 2)
    count = tok.shape[0]
    blocks = count // RBLOCK
    per_owner = rows_in.shape[0]
    mine_rows = count // n_tp

    def at_y(offset, sibling=False):
        chip = lax.rem(y + offset + n_y, n_y)
        return chip * 2 + (1 - core if sibling else core)

    def along_tp(offset):
        return lax.rem(tp + offset + n_tp, n_tp)

    def fetch(k, source, target):
        copy = pltpu.make_async_copy(source, target, in_sem.at[k])
        copy.start()
        return copy

    got_tok = fetch(0, tokens, tok)
    got_pre = fetch(11, pre_gain, gains.at[0])
    got_wq = fetch(1, w_query, wq)
    got_ids = fetch(12, ids, own_ids)

    barrier = pltpu.get_barrier_semaphore()
    peers = [(grp, lax.rem(st + k, n_st), tp) for k in range(1, n_st)]
    sides = [1, -1] if n_tp > 2 else [1]
    peers += [(grp, st, along_tp(k)) for k in sides]
    for peer in peers:
        pl.semaphore_signal(barrier, inc=1, device_id=peer, device_id_type=MESH)

    got_wk = fetch(2, w_key, wkv.at[:, 0:HD])
    got_wv = fetch(3, w_value, wkv.at[:, HD : 2 * HD])
    got_mem = fetch(13, mem_gain, gains.at[1])
    for p in range(per_owner):
        pltpu.make_async_copy(store.at[p], rows_in.at[p], row_sem.at[p]).start()
    got_wm = fetch(4, w_mixed, wm)
    got_wg = fetch(5, w_gated, wg)
    got_wgm = fetch(6, w_gate_mix, wgm)
    got_wgr = fetch(7, w_gate_read, wgr)
    got_mixw = fetch(8, mix_weight.at[0], mixw)
    got_wom = fetch(9, w_out_mix, wom)
    got_wor = fetch(10, w_out_read, wor)

    got_pre.wait()
    got_tok.wait()
    got_wq.wait()
    cut = blocks // 2
    half = cut * RBLOCK
    for h in range(2):
        rows = slice(h * half, (h + 1) * half)
        row_norm(tok, gains[0].reshape(1, -1), normed, h * half, (h + 1) * half)
        own_q = dot(normed[rows, :], wq[...]).astype(BF16)
        q_ring[0][h * cut : (h + 1) * cut] = own_q.reshape(cut, RBLOCK, HD)
    got_ids.wait()

    pl.semaphore_wait(barrier, len(peers))

    for k in range(1, n_st):
        pltpu.make_async_remote_copy(
            own_ids, ids_all.at[st], ids_send_sem, ids_recv_sem,
            device_id=(grp, lax.rem(st + k, n_st), tp), device_id_type=MESH,
        ).start()

    def drain(like, sem):
        pltpu.make_async_copy(like, like, sem).wait()

    def push(j, after, h, offset):
        piece = pl.ds(h * cut, cut)
        recv = two_recv_sem.at[after // 4, h] if after in (2, n_y - 2) else ring_recv_sem.at[after]
        pltpu.make_async_remote_copy(
            q_ring[j].at[piece], q_ring[after].at[piece], ring_send_sem, recv,
            device_id=(grp, at_y(offset), tp), device_id_type=MESH,
        ).start()

    def across(j):
        pltpu.make_async_remote_copy(
            q_ring[j], q_sib[j], sib_send_sem, sib_recv_sem.at[j],
            device_id=(grp, at_y(0, True), tp), device_id_type=MESH,
        ).start()

    for h in range(2):
        push(0, 2, h, 2)
        push(0, n_y - 2, 1 - h, -2)
    for h in range(2):
        push(0, 1, h, 1)
        push(0, n_y - 1, 1 - h, -1)
    across(0)

    for b in range(blocks):
        for n in range(NPB):
            ids_all[st, b, n] = own_ids[b, n]

    got_wk.wait()
    got_wv.wait()
    got_mem.wait()
    mem_row = gains[1].reshape(1, -1)

    def norm_of(p, target):
        row_norm(rows_in.at[p], mem_row, target, 0, PROWS)

    def keys_of(p, source):
        both = dot(source[...], wkv[...])
        key_of[p] = both[:, :HD].astype(BF16)
        value_of[p] = jnp.transpose(both[:, HD:]).astype(BF16)

    def row_wait(p):
        pltpu.make_async_copy(store.at[p], rows_in.at[p], row_sem.at[p]).wait()

    row_wait(0)
    norm_of(0, norm_even)

    def two(i, carry):
        row_wait(2 * i + 1)
        row_wait(2 * i + 2)
        keys_of(2 * i, norm_even)
        norm_of(2 * i + 1, norm_odd)
        keys_of(2 * i + 1, norm_odd)
        norm_of(2 * i + 2, norm_even)
        return carry

    lax.fori_loop(0, per_owner // 2 - 1, two, 0)
    row_wait(per_owner - 1)
    keys_of(per_owner - 2, norm_even)
    norm_of(per_owner - 1, norm_odd)
    keys_of(per_owner - 1, norm_odd)

    lanes = lax.broadcasted_iota(jnp.int32, (1, 2 * RBLOCK), 1)
    first_half = lanes < RBLOCK

    def attend(q_ref, reader):
        p0, p1, b0, b1 = (slot_of[reader, k] for k in range(4))
        q = jnp.concatenate([q_ref[b0], q_ref[b1]], axis=0)
        over_keys = ((1,), (1,))
        scores = jnp.where(
            first_half, dot(key_of[p0], q, over_keys), dot(key_of[p1], q, over_keys)
        ) * (HD ** (-0.5))
        top = jnp.max(scores, axis=0, keepdims=True)
        weight = jnp.exp(scores - top)
        total = jnp.sum(weight, axis=0, keepdims=True)
        weight = weight.astype(BF16)
        read = jnp.where(first_half, dot(value_of[p0], weight), dot(value_of[p1], weight))
        return read.astype(BF16), jnp.concatenate([top, total], axis=0)

    def serve(*labels):
        for j, sibling in labels:
            if sibling:
                drain(q_sib[j], sib_recv_sem.at[j])
        readers = [at_y(-j, sibling) for j, sibling in labels]
        results = [
            attend(q_sib[j] if sibling else q_ring[j], reader)
            for (j, sibling), reader in zip(labels, readers)
        ]
        for (j, sibling), (read, stats) in zip(labels, results):
            if j == 0 and not sibling:
                ret_o[st] = read
                ret_s[st] = stats
            else:
                o_send[j * 2 + sibling] = read
                s_send[j * 2 + sibling] = stats
        for (j, sibling), reader in zip(labels, readers):
            if j == 0 and not sibling:
                continue
            label = j * 2 + sibling
            for source, target, send, recv in (
                (o_send, ret_o, ret_send_sem, ret_recv_sem),
                (s_send, ret_s, stat_send_sem, stat_recv_sem),
            ):
                pltpu.make_async_remote_copy(
                    source.at[label], target.at[st], send, recv,
                    device_id=(grp, reader, tp), device_id_type=MESH,
                ).start()

    def forward(i):
        for j, near, h, sign in ((2, 3, i, 1), (n_y - 2, n_y - 3, 1 - i, -1)):
            drain(q_ring[j].at[pl.ds(h * cut, cut)], two_recv_sem.at[j // 4, h])
            if i == 0:
                push(j, 4, h, 2 * sign)
            push(j, near, h, sign)

    forward(0)

    drain(ids_all.at[pl.ds(0, n_st - 1)], ids_recv_sem)

    def slots(reader, carry):
        p0 = p1 = b0 = b1 = seen = jnp.int32(0)
        for b in range(blocks):
            for n in range(NPB):
                local = ids_all[reader, b, n] - st * per_owner
                mine = (local >= 0) & (local < per_owner)
                is0 = mine & (seen == 0)
                is1 = mine & (seen == 1)
                p0, b0 = jnp.where(is0, local, p0), jnp.where(is0, b, b0)
                p1, b1 = jnp.where(is1, local, p1), jnp.where(is1, b, b1)
                seen = seen + jnp.where(mine, 1, 0)
        for k, value in enumerate((p0, p1, b0, b1)):
            slot_of[reader, k] = value
        return carry

    lax.fori_loop(0, n_st, slots, 0, unroll=4)

    forward(1)
    for j in (1, n_y - 1):
        drain(q_ring[j], ring_recv_sem.at[j])
        across(j)
    for j in (2, n_y - 2):
        across(j)

    serve((1, 0), (n_y - 1, 0))
    serve((2, 0), (n_y - 2, 0))
    serve((1, 1), (n_y - 1, 1))
    serve((2, 1), (n_y - 2, 1))

    for j in (3, n_y - 3, 4):
        drain(q_ring[j], ring_recv_sem.at[j])
        across(j)
    serve((4, 0), (3, 0), (n_y - 3, 0))
    serve((4, 1), (3, 1), (n_y - 3, 1))
    serve((0, 0), (0, 1))

    got_wm.wait()
    over_width = ((1,), (1,))
    mixed_in = dot(normed[...], wm[...], over_width)
    centred = mixed_in - jnp.mean(mixed_in, axis=-1, keepdims=True)
    variance = jnp.mean(centred * centred, axis=-1, keepdims=True)
    mixed_norm = (centred * lax.rsqrt(variance + eps)).astype(BF16)
    got_mixw.wait()
    row_at = lax.broadcasted_iota(jnp.int32, (SPAN, SPAN), 0)
    col_at = lax.broadcasted_iota(jnp.int32, (SPAN, SPAN), 1)
    causal = jnp.where(col_at <= row_at, mixw[...].astype(F32), 0.0).astype(BF16)
    spatial = jnp.concatenate(
        [dot(causal, mixed_norm[n * SPAN : (n + 1) * SPAN]) for n in range(count // SPAN)], axis=0
    )
    got_wg.wait()
    branch_mix = dot(normed[...], wg[...], over_width) * spatial
    got_wgm.wait()
    gate = dot(normed[...], wgm[...], over_width)
    out_mix[...] = (branch_mix * (gate / (1.0 + jnp.exp(-gate)))).astype(BF16)
    got_wgr.wait()
    gate = dot(normed[...], wgr[...])
    gate_t[...] = jnp.transpose(gate / (1.0 + jnp.exp(-gate)))
    got_wom.wait()
    width = part.shape[2]
    for c in range(PIECES):
        part[c] = dot(out_mix[...], wom[:, c * width : (c + 1) * width])

    owners, ranks = [], []
    for e in range(blocks * NPB):
        owner = own_ids[e // NPB, e % NPB] // per_owner
        rank = jnp.int32(0)
        for before in owners:
            rank = rank + jnp.where(before == owner, 1, 0)
        owners.append(owner)
        ranks.append(rank)
    drain(ret_o.at[pl.ds(0, n_st - 1)], ret_recv_sem)
    drain(ret_s.at[pl.ds(0, n_st - 1)], stat_recv_sem)
    got_wor.wait()
    for pair in range(blocks // 2):
        tops, totals, reads = [], [], []
        for n in range(NPB):
            e0, e1 = pair * 2 * NPB + n, (pair * 2 + 1) * NPB + n

            def placed(ref):
                x0, x1 = ref[owners[e0]].astype(F32), ref[owners[e1]].astype(F32)
                low = jnp.where(ranks[e0] == 0, x0, pltpu.roll(x0, RBLOCK, 1))
                high = jnp.where(ranks[e1] == 1, x1, pltpu.roll(x1, RBLOCK, 1))
                return jnp.where(first_half, low, high)

            stats = placed(ret_s)
            tops.append(stats[0:1])
            totals.append(stats[1:2])
            reads.append(placed(ret_o))
        top = functools.reduce(jnp.maximum, tops)
        scales = [jnp.exp(t - top) for t in tops]
        total = sum(s * t for s, t in zip(scales, totals))
        read = sum(s * r for s, r in zip(scales, reads)) / total
        cols = slice(pair * 2 * RBLOCK, (pair + 1) * 2 * RBLOCK)
        out_read[cols, :] = jnp.transpose(read * gate_t[:, cols]).astype(BF16)

    rs_copies = {}

    def pass_on(c, d, k):
        sign = 1 - 2 * d
        target = along_tp(sign * k)
        lo = 0
        size = mine_rows
        if k == half_tp:
            size = mine_rows // 2
            lo = d * size
        start = pl.multiple_of(target * mine_rows + lo, mine_rows // 2)
        value = part[c, pl.ds(start, size), :]
        if k == half_tp:
            rs_send[k - 1, d, c, lo : lo + size, :] = value.astype(BF16)
        else:
            rs_copies[c, d, k + 1].wait_recv()
            if k + 1 == half_tp:
                cut_rows = mine_rows // 2
                low = d * cut_rows
                rs_send[k - 1, d, c, low : low + cut_rows, :] = (
                    part[c, pl.ds(pl.multiple_of(target * mine_rows + low, cut_rows), cut_rows), :]
                    + rs_recv[k, d, c, low : low + cut_rows, :].astype(F32)
                ).astype(BF16)
                other = cut_rows - low
                rs_send[k - 1, d, c, other : other + cut_rows, :] = part[
                    c, pl.ds(pl.multiple_of(target * mine_rows + other, cut_rows), cut_rows), :
                ].astype(BF16)
            else:
                rs_send[k - 1, d, c] = (value + rs_recv[k, d, c].astype(F32)).astype(BF16)
        copy = pltpu.make_async_remote_copy(
            rs_send.at[k - 1, d, c, pl.ds(lo, size)], rs_recv.at[k - 1, d, c, pl.ds(lo, size)],
            rs_send_sem.at[k // half_tp], rs_recv_sem.at[k - 1, d, c],
            device_id=(grp, st, along_tp(sign)), device_id_type=MESH,
        )
        copy.start()
        rs_copies[c, d, k] = copy

    for c in range(PIECES):
        part[c] = part[c] + dot(out_read[...], wor[:, c * width : (c + 1) * width])
        for d in range(2):
            pass_on(c, d, half_tp)
    for k in range(half_tp - 1, 0, -1):
        for c in range(PIECES):
            for d in range(2):
                pass_on(c, d, k)
    here = pl.ds(pl.multiple_of(tp * mine_rows, mine_rows), mine_rows)
    for c in range(PIECES):
        for d in range(2):
            rs_copies[c, d, 1].wait_recv()
        if half_tp == 1:
            cut_rows = mine_rows // 2
            both = jnp.concatenate(
                [rs_recv[0, 0, c, :cut_rows, :], rs_recv[0, 1, c, cut_rows:, :]], axis=0
            ).astype(F32)
        else:
            both = rs_recv[0, 0, c].astype(F32) + rs_recv[0, 1, c].astype(F32)
        out[:, c * width : (c + 1) * width] = (part[c, here, :] + both).astype(BF16)

    drain(ids_all.at[pl.ds(0, n_st - 1)], ids_send_sem)
    drain(o_send.at[pl.ds(0, 2 * (n_y - 1))], ring_send_sem)
    drain(o_send, sib_send_sem)
    drain(o_send.at[pl.ds(0, n_st - 1)], ret_send_sem)
    drain(s_send.at[pl.ds(0, n_st - 1)], stat_send_sem)
    drain(rs_send.at[half_tp - 1, 0], rs_send_sem.at[1])
    if half_tp > 1:
        drain(rs_send.at[pl.ds(0, half_tp - 1)], rs_send_sem.at[0])


def local(*args, n_st, n_tp):
    args = [a.T if k in (2, 3, 6) else a for k, a in enumerate(args)]
    tokens, w_gated, store = args[0], args[2], args[8]
    count, width = tokens.shape
    mix_width = w_gated.shape[0]
    held = store.shape[0]
    blocks = count // RBLOCK
    n_y = n_st // 2
    mine_rows = count // n_tp
    hbm = pl.BlockSpec(memory_space=pltpu.HBM)
    vmem = pl.BlockSpec(memory_space=pltpu.VMEM)
    specs = [hbm] * 15
    dma = pltpu.SemaphoreType.DMA
    columns = width // PIECES
    scratch = dict(
        tok=pltpu.VMEM((count, width), BF16),
        gains=pltpu.VMEM((2, width), F32),
        own_ids=pltpu.SMEM((blocks, NPB), jnp.int32),
        slot_of=pltpu.SMEM((n_st, 4), jnp.int32),
        normed=pltpu.VMEM((count, width), BF16),
        wg=pltpu.VMEM((mix_width, width), BF16),
        wm=pltpu.VMEM((mix_width, width), BF16),
        wgm=pltpu.VMEM((mix_width, width), BF16),
        mixw=pltpu.VMEM((SPAN, SPAN), BF16),
        wq=pltpu.VMEM((width, HD), BF16),
        wgr=pltpu.VMEM((width, HD), BF16),
        wkv=pltpu.VMEM((width, 2 * HD), BF16),
        wom=pltpu.VMEM((mix_width, width), BF16),
        wor=pltpu.VMEM((HD, width), BF16),
        rows_in=pltpu.VMEM((held, PROWS, width), BF16),
        norm_even=pltpu.VMEM((PROWS, width), BF16),
        norm_odd=pltpu.VMEM((PROWS, width), BF16),
        key_of=pltpu.VMEM((held, PROWS, HD), BF16),
        value_of=pltpu.VMEM((held, HD, PROWS), BF16),
        q_ring=[pltpu.VMEM((blocks, RBLOCK, HD), BF16) for _ in range(n_y)],
        q_sib=[pltpu.VMEM((blocks, RBLOCK, HD), BF16) for _ in range(n_y)],
        ids_all=pltpu.SMEM((n_st, blocks, NPB), jnp.int32),
        o_send=pltpu.VMEM((n_st, HD, 2 * RBLOCK), BF16),
        s_send=pltpu.VMEM((n_st, 2, 2 * RBLOCK), F32),
        ret_o=pltpu.VMEM((n_st, HD, 2 * RBLOCK), BF16),
        ret_s=pltpu.VMEM((n_st, 2, 2 * RBLOCK), F32),
        gate_t=pltpu.VMEM((HD, count), F32),
        out_mix=pltpu.VMEM((count, mix_width), BF16),
        out_read=pltpu.VMEM((count, HD), BF16),
        part=pltpu.VMEM((PIECES, count, columns), F32),
        rs_send=pltpu.VMEM((n_tp // 2, 2, PIECES, mine_rows, columns), BF16),
        rs_recv=pltpu.VMEM((n_tp // 2, 2, PIECES, mine_rows, columns), BF16),
        in_sem=dma((14,)),
        row_sem=dma((held,)),
        ids_send_sem=dma,
        ids_recv_sem=dma,
        ring_send_sem=dma,
        ring_recv_sem=dma((n_y,)),
        two_recv_sem=dma((2, 2)),
        sib_send_sem=dma,
        sib_recv_sem=dma((n_y,)),
        ret_send_sem=dma,
        ret_recv_sem=dma,
        stat_send_sem=dma,
        stat_recv_sem=dma,
        rs_send_sem=dma((2,)),
        rs_recv_sem=dma((n_tp // 2, 2, PIECES)),
    )
    names = list(scratch)

    def body(*refs):
        kernel(n_st, n_tp, *refs[:16], **dict(zip(names, refs[16:])))

    return pl.pallas_call(
        body,
        out_shape=pltpu.VMEM((mine_rows, width), BF16),
        in_specs=specs,
        out_specs=vmem,
        scratch_shapes=list(scratch.values()),
        compiler_params=pltpu.CompilerParams(
            collective_id=0, has_side_effects=True, vmem_limit_bytes=66_800_000
        ),
        name="layer",
    )(*args)


def solution(mesh):
    placed = (
        P(("grp", "st"), None),
        P(),
        P(None, "tp"),
        P(None, "tp"),
        P("tp", None, None),
        P(None, "tp"),
        P(None, "tp"),
        P(None, "tp"),
        P(("grp", "st"), None, None),
        P(),
        P(None, "tp"),
        P(None, "tp"),
        P(("grp", "st"), None),
        P("tp", None),
        P("tp", None),
    )
    body = functools.partial(local, n_st=mesh.shape["st"], n_tp=mesh.shape["tp"])
    return jax.shard_map(
        body, mesh=mesh, in_specs=placed, out_specs=P(("grp", "st", "tp"), None), check_vma=False
    )
```

```python
import functools

import jax
import jax.numpy as jnp
from jax import lax
from jax.experimental import pallas as pl
from jax.experimental.pallas import tpu as pltpu
from jax.sharding import PartitionSpec as P

HD = 128
SPAN = 128
RBLOCK = 64
NPB = 4
PROWS = 128
NORM_ROWS = 32
PIECES = 2

MESH = pl.DeviceIdType.MESH
eps = 1e-06
F32 = jnp.float32
BF16 = jnp.bfloat16


def dot(a, b, dims=((1,), (0,))):
    return lax.dot_general(a, b, (dims, ((), ())), preferred_element_type=F32)


def row_norm(source, gain, target, low, high):
    for at in range(low, high, NORM_ROWS):
        wide = source[at : at + NORM_ROWS, :].astype(F32)
        scale = lax.rsqrt(jnp.mean(wide * wide, axis=-1, keepdims=True) + eps)
        target[at : at + NORM_ROWS, :] = (wide * scale * gain).astype(BF16)


def kernel(
    n_st,
    n_tp,
    tokens,
    pre_gain,
    w_gated,
    w_mixed,
    mix_weight,
    w_query,
    w_gate_mix,
    w_gate_read,
    store,
    mem_gain,
    w_key,
    w_value,
    ids,
    w_out_mix,
    w_out_read,
    out,
    tok,
    gains,
    own_ids,
    slot_of,
    normed,
    wg,
    wm,
    wgm,
    mixw,
    wq,
    wgr,
    wkv,
    wom,
    wor,
    rows_in,
    norm_even,
    norm_odd,
    key_of,
    value_of,
    q_ring,
    q_sib,
    ids_all,
    o_send,
    s_send,
    ret_o,
    ret_s,
    gate_t,
    out_mix,
    out_read,
    part,
    rs_send,
    rs_recv,
    in_sem,
    row_sem,
    ids_send_sem,
    ids_recv_sem,
    ring_send_sem,
    ring_recv_sem,
    two_recv_sem,
    sib_send_sem,
    sib_recv_sem,
    ret_send_sem,
    ret_recv_sem,
    stat_send_sem,
    stat_recv_sem,
    rs_send_sem,
    rs_recv_sem,
):
    grp, st, tp = lax.axis_index("grp"), lax.axis_index("st"), lax.axis_index("tp")
    n_y = n_st // 2
    half_tp = n_tp // 2
    y, core = st // 2, lax.rem(st, 2)
    count = tok.shape[0]
    blocks = count // RBLOCK
    per_owner = rows_in.shape[0]
    mine_rows = count // n_tp

    def at_y(offset, sibling=False):
        chip = lax.rem(y + offset + n_y, n_y)
        return chip * 2 + (1 - core if sibling else core)

    def along_tp(offset):
        return lax.rem(tp + offset + n_tp, n_tp)

    def fetch(k, source, target):
        copy = pltpu.make_async_copy(source, target, in_sem.at[k])
        copy.start()
        return copy

    got_tok = fetch(0, tokens, tok)
    got_pre = fetch(11, pre_gain, gains.at[0])
    got_wq = fetch(1, w_query, wq)
    got_ids = fetch(12, ids, own_ids)

    barrier = pltpu.get_barrier_semaphore()
    peers = [(grp, lax.rem(st + k, n_st), tp) for k in range(1, n_st)]
    sides = [1, -1] if n_tp > 2 else [1]
    peers += [(grp, st, along_tp(k)) for k in sides]
    for peer in peers:
        pl.semaphore_signal(barrier, inc=1, device_id=peer, device_id_type=MESH)

    got_wk = fetch(2, w_key, wkv.at[:, 0:HD])
    got_wv = fetch(3, w_value, wkv.at[:, HD : 2 * HD])
    got_mem = fetch(13, mem_gain, gains.at[1])
    for p in range(per_owner):
        pltpu.make_async_copy(store.at[p], rows_in.at[p], row_sem.at[p]).start()
    got_wm = fetch(4, w_mixed, wm)
    got_wg = fetch(5, w_gated, wg)
    got_wgm = fetch(6, w_gate_mix, wgm)
    got_wgr = fetch(7, w_gate_read, wgr)
    got_mixw = fetch(8, mix_weight.at[0], mixw)
    got_wom = fetch(9, w_out_mix, wom)
    got_wor = fetch(10, w_out_read, wor)

    got_pre.wait()
    got_tok.wait()
    got_wq.wait()
    cut = blocks // 2
    half = cut * RBLOCK
    for h in range(2):
        rows = slice(h * half, (h + 1) * half)
        row_norm(tok, gains[0].reshape(1, -1), normed, h * half, (h + 1) * half)
        own_q = dot(normed[rows, :], wq[...]).astype(BF16)
        q_ring[0][h * cut : (h + 1) * cut] = own_q.reshape(cut, RBLOCK, HD)
    got_ids.wait()

    pl.semaphore_wait(barrier, len(peers))

    for k in range(1, n_st):
        pltpu.make_async_remote_copy(
            own_ids, ids_all.at[st], ids_send_sem, ids_recv_sem,
            device_id=(grp, lax.rem(st + k, n_st), tp), device_id_type=MESH,
        ).start()

    def drain(like, sem):
        pltpu.make_async_copy(like, like, sem).wait()

    def push(j, after, h, offset):
        piece = pl.ds(h * cut, cut)
        recv = two_recv_sem.at[after // 4, h] if after in (2, n_y - 2) else ring_recv_sem.at[after]
        pltpu.make_async_remote_copy(
            q_ring[j].at[piece], q_ring[after].at[piece], ring_send_sem, recv,
            device_id=(grp, at_y(offset), tp), device_id_type=MESH,
        ).start()

    def across(j):
        pltpu.make_async_remote_copy(
            q_ring[j], q_sib[j], sib_send_sem, sib_recv_sem.at[j],
            device_id=(grp, at_y(0, True), tp), device_id_type=MESH,
        ).start()

    for h in range(2):
        push(0, 2, h, 2)
        push(0, n_y - 2, 1 - h, -2)
    for h in range(2):
        push(0, 1, h, 1)
        push(0, n_y - 1, 1 - h, -1)
    across(0)

    for b in range(blocks):
        for n in range(NPB):
            ids_all[st, b, n] = own_ids[b, n]

    got_wk.wait()
    got_wv.wait()
    got_mem.wait()
    mem_row = gains[1].reshape(1, -1)

    def norm_of(p, target):
        row_norm(rows_in.at[p], mem_row, target, 0, PROWS)

    def keys_of(p, source):
        both = dot(source[...], wkv[...])
        key_of[p] = both[:, :HD].astype(BF16)
        value_of[p] = jnp.transpose(both[:, HD:]).astype(BF16)

    def row_wait(p):
        pltpu.make_async_copy(store.at[p], rows_in.at[p], row_sem.at[p]).wait()

    row_wait(0)
    norm_of(0, norm_even)

    def two(i, carry):
        row_wait(2 * i + 1)
        row_wait(2 * i + 2)
        keys_of(2 * i, norm_even)
        norm_of(2 * i + 1, norm_odd)
        keys_of(2 * i + 1, norm_odd)
        norm_of(2 * i + 2, norm_even)
        return carry

    lax.fori_loop(0, per_owner // 2 - 1, two, 0)
    row_wait(per_owner - 1)
    keys_of(per_owner - 2, norm_even)
    norm_of(per_owner - 1, norm_odd)
    keys_of(per_owner - 1, norm_odd)

    lanes = lax.broadcasted_iota(jnp.int32, (1, 2 * RBLOCK), 1)
    first_half = lanes < RBLOCK

    def attend(q_ref, reader):
        p0, p1, b0, b1 = (slot_of[reader, k] for k in range(4))
        q = jnp.concatenate([q_ref[b0], q_ref[b1]], axis=0)
        over_keys = ((1,), (1,))
        scores = jnp.where(
            first_half, dot(key_of[p0], q, over_keys), dot(key_of[p1], q, over_keys)
        ) * (HD ** (-0.5))
        top = jnp.max(scores, axis=0, keepdims=True)
        weight = jnp.exp(scores - top)
        total = jnp.sum(weight, axis=0, keepdims=True)
        weight = weight.astype(BF16)
        read = jnp.where(first_half, dot(value_of[p0], weight), dot(value_of[p1], weight))
        return read.astype(BF16), jnp.concatenate([top, total], axis=0)

    def serve(*labels):
        for j, sibling in labels:
            if sibling:
                drain(q_sib[j], sib_recv_sem.at[j])
        readers = [at_y(-j, sibling) for j, sibling in labels]
        results = [
            attend(q_sib[j] if sibling else q_ring[j], reader)
            for (j, sibling), reader in zip(labels, readers)
        ]
        for (j, sibling), (read, stats) in zip(labels, results):
            if j == 0 and not sibling:
                ret_o[st] = read
                ret_s[st] = stats
            else:
                o_send[j * 2 + sibling] = read
                s_send[j * 2 + sibling] = stats
        for (j, sibling), reader in zip(labels, readers):
            if j == 0 and not sibling:
                continue
            label = j * 2 + sibling
            for source, target, send, recv in (
                (o_send, ret_o, ret_send_sem, ret_recv_sem),
                (s_send, ret_s, stat_send_sem, stat_recv_sem),
            ):
                pltpu.make_async_remote_copy(
                    source.at[label], target.at[st], send, recv,
                    device_id=(grp, reader, tp), device_id_type=MESH,
                ).start()

    def forward(i):
        for j, near, h, sign in ((2, 3, i, 1), (n_y - 2, n_y - 3, 1 - i, -1)):
            drain(q_ring[j].at[pl.ds(h * cut, cut)], two_recv_sem.at[j // 4, h])
            if i == 0:
                push(j, 4, h, 2 * sign)
            push(j, near, h, sign)

    forward(0)

    drain(ids_all.at[pl.ds(0, n_st - 1)], ids_recv_sem)

    def slots(reader, carry):
        first = last = jnp.int32(0)
        codes = []
        for b in range(blocks):
            for n in range(NPB):
                local = ids_all[reader, b, n] - st * per_owner
                mine = (local >= 0) & (local < per_owner)
                code = local * blocks + b
                last = jnp.where(mine, code, last)
                codes.append((mine, code))
        for mine, code in reversed(codes):
            first = jnp.where(mine, code, first)
        slot_of[reader, 0] = first // blocks
        slot_of[reader, 1] = last // blocks
        slot_of[reader, 2] = lax.rem(first, blocks)
        slot_of[reader, 3] = lax.rem(last, blocks)
        return carry

    lax.fori_loop(0, n_st, slots, 0, unroll=4)

    forward(1)
    for j in (1, n_y - 1):
        drain(q_ring[j], ring_recv_sem.at[j])
        across(j)
    for j in (2, n_y - 2):
        across(j)

    serve((1, 0), (n_y - 1, 0), (2, 0), (n_y - 2, 0))
    serve((1, 1), (n_y - 1, 1), (2, 1), (n_y - 2, 1))

    for j in (3, n_y - 3, 4):
        drain(q_ring[j], ring_recv_sem.at[j])
        across(j)
    serve((4, 0), (3, 0), (n_y - 3, 0))
    serve((4, 1), (3, 1), (n_y - 3, 1))
    serve((0, 0), (0, 1))

    got_wm.wait()
    over_width = ((1,), (1,))
    mixed_in = dot(normed[...], wm[...], over_width)
    centred = mixed_in - jnp.mean(mixed_in, axis=-1, keepdims=True)
    variance = jnp.mean(centred * centred, axis=-1, keepdims=True)
    mixed_norm = (centred * lax.rsqrt(variance + eps)).astype(BF16)
    got_mixw.wait()
    row_at = lax.broadcasted_iota(jnp.int32, (SPAN, SPAN), 0)
    col_at = lax.broadcasted_iota(jnp.int32, (SPAN, SPAN), 1)
    causal = jnp.where(col_at <= row_at, mixw[...].astype(F32), 0.0).astype(BF16)
    spatial = jnp.concatenate(
        [dot(causal, mixed_norm[n * SPAN : (n + 1) * SPAN]) for n in range(count // SPAN)], axis=0
    )
    got_wg.wait()
    branch_mix = dot(normed[...], wg[...], over_width) * spatial
    got_wgm.wait()
    gate = dot(normed[...], wgm[...], over_width)
    out_mix[...] = (branch_mix * (gate / (1.0 + jnp.exp(-gate)))).astype(BF16)
    got_wgr.wait()
    gate = dot(normed[...], wgr[...])
    gate_t[...] = jnp.transpose(gate / (1.0 + jnp.exp(-gate)))
    got_wom.wait()
    width = part.shape[2]
    for c in range(PIECES):
        part[c] = dot(out_mix[...], wom[:, c * width : (c + 1) * width])

    owners, ranks = [], []
    for e in range(blocks * NPB):
        owner = own_ids[e // NPB, e % NPB] // per_owner
        rank = jnp.int32(0)
        for before in owners:
            rank = rank + jnp.where(before == owner, 1, 0)
        owners.append(owner)
        ranks.append(rank)
    drain(ret_o.at[pl.ds(0, n_st - 1)], ret_recv_sem)
    drain(ret_s.at[pl.ds(0, n_st - 1)], stat_recv_sem)
    got_wor.wait()
    for pair in range(blocks // 2):
        tops, totals, reads = [], [], []
        for n in range(NPB):
            e0, e1 = pair * 2 * NPB + n, (pair * 2 + 1) * NPB + n

            def placed(ref):
                x0, x1 = ref[owners[e0]].astype(F32), ref[owners[e1]].astype(F32)
                low = jnp.where(ranks[e0] == 0, x0, pltpu.roll(x0, RBLOCK, 1))
                high = jnp.where(ranks[e1] == 1, x1, pltpu.roll(x1, RBLOCK, 1))
                return jnp.where(first_half, low, high)

            stats = placed(ret_s)
            tops.append(stats[0:1])
            totals.append(stats[1:2])
            reads.append(placed(ret_o))
        top = functools.reduce(jnp.maximum, tops)
        scales = [jnp.exp(t - top) for t in tops]
        total = sum(s * t for s, t in zip(scales, totals))
        read = sum(s * r for s, r in zip(scales, reads)) / total
        cols = slice(pair * 2 * RBLOCK, (pair + 1) * 2 * RBLOCK)
        out_read[cols, :] = jnp.transpose(read * gate_t[:, cols]).astype(BF16)

    rs_copies = {}

    def pass_on(c, d, k):
        sign = 1 - 2 * d
        target = along_tp(sign * k)
        lo = 0
        size = mine_rows
        if k == half_tp:
            size = mine_rows // 2
            lo = d * size
        start = pl.multiple_of(target * mine_rows + lo, mine_rows // 2)
        value = part[c, pl.ds(start, size), :]
        if k == half_tp:
            added = first[lo : lo + size, c * width : (c + 1) * width]
            rs_send[k - 1, d, c, lo : lo + size, :] = (value + added).astype(BF16)
        else:
            rs_copies[c, d, k + 1].wait_recv()
            if k + 1 == half_tp:
                cut_rows = mine_rows // 2
                low = d * cut_rows
                rs_send[k - 1, d, c, low : low + cut_rows, :] = (
                    part[c, pl.ds(pl.multiple_of(target * mine_rows + low, cut_rows), cut_rows), :]
                    + rs_recv[k, d, c, low : low + cut_rows, :].astype(F32)
                ).astype(BF16)
                other = cut_rows - low
                rs_send[k - 1, d, c, other : other + cut_rows, :] = part[
                    c, pl.ds(pl.multiple_of(target * mine_rows + other, cut_rows), cut_rows), :
                ].astype(BF16)
            else:
                rs_send[k - 1, d, c] = (value + rs_recv[k, d, c].astype(F32)).astype(BF16)
        copy = pltpu.make_async_remote_copy(
            rs_send.at[k - 1, d, c, pl.ds(lo, size)], rs_recv.at[k - 1, d, c, pl.ds(lo, size)],
            rs_send_sem.at[k // half_tp], rs_recv_sem.at[k - 1, d, c],
            device_id=(grp, st, along_tp(sign)), device_id_type=MESH,
        )
        copy.start()
        rs_copies[c, d, k] = copy

    start = pl.multiple_of(along_tp(half_tp) * mine_rows, mine_rows)
    first = dot(out_read[pl.ds(start, mine_rows), :], wor[...])
    for c in range(PIECES):
        for d in range(2):
            pass_on(c, d, half_tp)
    for c in range(PIECES):
        part[c] = part[c] + dot(out_read[...], wor[:, c * width : (c + 1) * width])
    for k in range(half_tp - 1, 0, -1):
        for c in range(PIECES):
            for d in range(2):
                pass_on(c, d, k)
    here = pl.ds(pl.multiple_of(tp * mine_rows, mine_rows), mine_rows)
    for c in range(PIECES):
        for d in range(2):
            rs_copies[c, d, 1].wait_recv()
        if half_tp == 1:
            cut_rows = mine_rows // 2
            both = jnp.concatenate(
                [rs_recv[0, 0, c, :cut_rows, :], rs_recv[0, 1, c, cut_rows:, :]], axis=0
            ).astype(F32)
        else:
            both = rs_recv[0, 0, c].astype(F32) + rs_recv[0, 1, c].astype(F32)
        out[:, c * width : (c + 1) * width] = (part[c, here, :] + both).astype(BF16)

    drain(ids_all.at[pl.ds(0, n_st - 1)], ids_send_sem)
    drain(o_send.at[pl.ds(0, 2 * (n_y - 1))], ring_send_sem)
    drain(o_send, sib_send_sem)
    drain(o_send.at[pl.ds(0, n_st - 1)], ret_send_sem)
    drain(s_send.at[pl.ds(0, n_st - 1)], stat_send_sem)
    drain(rs_send.at[half_tp - 1, 0], rs_send_sem.at[1])
    if half_tp > 1:
        drain(rs_send.at[pl.ds(0, half_tp - 1)], rs_send_sem.at[0])


def local(*args, n_st, n_tp):
    args = [a.T if k in (2, 3, 6) else a for k, a in enumerate(args)]
    tokens, w_gated, store = args[0], args[2], args[8]
    count, width = tokens.shape
    mix_width = w_gated.shape[0]
    held = store.shape[0]
    blocks = count // RBLOCK
    n_y = n_st // 2
    mine_rows = count // n_tp
    hbm = pl.BlockSpec(memory_space=pltpu.HBM)
    vmem = pl.BlockSpec(memory_space=pltpu.VMEM)
    specs = [hbm] * 15
    dma = pltpu.SemaphoreType.DMA
    columns = width // PIECES
    scratch = dict(
        tok=pltpu.VMEM((count, width), BF16),
        gains=pltpu.VMEM((2, width), F32),
        own_ids=pltpu.SMEM((blocks, NPB), jnp.int32),
        slot_of=pltpu.SMEM((n_st, 4), jnp.int32),
        normed=pltpu.VMEM((count, width), BF16),
        wg=pltpu.VMEM((mix_width, width), BF16),
        wm=pltpu.VMEM((mix_width, width), BF16),
        wgm=pltpu.VMEM((mix_width, width), BF16),
        mixw=pltpu.VMEM((SPAN, SPAN), BF16),
        wq=pltpu.VMEM((width, HD), BF16),
        wgr=pltpu.VMEM((width, HD), BF16),
        wkv=pltpu.VMEM((width, 2 * HD), BF16),
        wom=pltpu.VMEM((mix_width, width), BF16),
        wor=pltpu.VMEM((HD, width), BF16),
        rows_in=pltpu.VMEM((held, PROWS, width), BF16),
        norm_even=pltpu.VMEM((PROWS, width), BF16),
        norm_odd=pltpu.VMEM((PROWS, width), BF16),
        key_of=pltpu.VMEM((held, PROWS, HD), BF16),
        value_of=pltpu.VMEM((held, HD, PROWS), BF16),
        q_ring=[pltpu.VMEM((blocks, RBLOCK, HD), BF16) for _ in range(n_y)],
        q_sib=[pltpu.VMEM((blocks, RBLOCK, HD), BF16) for _ in range(n_y)],
        ids_all=pltpu.SMEM((n_st, blocks, NPB), jnp.int32),
        o_send=pltpu.VMEM((n_st, HD, 2 * RBLOCK), BF16),
        s_send=pltpu.VMEM((n_st, 2, 2 * RBLOCK), F32),
        ret_o=pltpu.VMEM((n_st, HD, 2 * RBLOCK), BF16),
        ret_s=pltpu.VMEM((n_st, 2, 2 * RBLOCK), F32),
        gate_t=pltpu.VMEM((HD, count), F32),
        out_mix=pltpu.VMEM((count, mix_width), BF16),
        out_read=pltpu.VMEM((count, HD), BF16),
        part=pltpu.VMEM((PIECES, count, columns), F32),
        rs_send=pltpu.VMEM((n_tp // 2, 2, PIECES, mine_rows, columns), BF16),
        rs_recv=pltpu.VMEM((n_tp // 2, 2, PIECES, mine_rows, columns), BF16),
        in_sem=dma((14,)),
        row_sem=dma((held,)),
        ids_send_sem=dma,
        ids_recv_sem=dma,
        ring_send_sem=dma,
        ring_recv_sem=dma((n_y,)),
        two_recv_sem=dma((2, 2)),
        sib_send_sem=dma,
        sib_recv_sem=dma((n_y,)),
        ret_send_sem=dma,
        ret_recv_sem=dma,
        stat_send_sem=dma,
        stat_recv_sem=dma,
        rs_send_sem=dma((2,)),
        rs_recv_sem=dma((n_tp // 2, 2, PIECES)),
    )
    names = list(scratch)

    def body(*refs):
        kernel(n_st, n_tp, *refs[:16], **dict(zip(names, refs[16:])))

    return pl.pallas_call(
        body,
        out_shape=pltpu.VMEM((mine_rows, width), BF16),
        in_specs=specs,
        out_specs=vmem,
        scratch_shapes=list(scratch.values()),
        compiler_params=pltpu.CompilerParams(
            collective_id=0, has_side_effects=True, vmem_limit_bytes=66_800_000
        ),
        name="layer",
    )(*args)


def solution(mesh):
    placed = (
        P(("grp", "st"), None),
        P(),
        P(None, "tp"),
        P(None, "tp"),
        P("tp", None, None),
        P(None, "tp"),
        P(None, "tp"),
        P(None, "tp"),
        P(("grp", "st"), None, None),
        P(),
        P(None, "tp"),
        P(None, "tp"),
        P(("grp", "st"), None),
        P("tp", None),
        P("tp", None),
    )
    body = functools.partial(local, n_st=mesh.shape["st"], n_tp=mesh.shape["tp"])
    return jax.shard_map(
        body, mesh=mesh, in_specs=placed, out_specs=P(("grp", "st", "tp"), None), check_vma=False
    )
```

```python
import functools

import jax
import jax.numpy as jnp
from jax import lax
from jax.experimental import pallas as pl
from jax.experimental.pallas import tpu as pltpu
from jax.sharding import PartitionSpec as P

HD = 128
SPAN = 128
RBLOCK = 64
NPB = 4
PROWS = 128
NORM_ROWS = 32
PIECES = 2

MESH = pl.DeviceIdType.MESH
eps = 1e-06
F32 = jnp.float32
BF16 = jnp.bfloat16


def dot(a, b, dims=((1,), (0,))):
    return lax.dot_general(a, b, (dims, ((), ())), preferred_element_type=F32)


def row_norm(source, gain, target, low, high):
    for at in range(low, high, NORM_ROWS):
        wide = source[at : at + NORM_ROWS, :].astype(F32)
        scale = lax.rsqrt(jnp.mean(wide * wide, axis=-1, keepdims=True) + eps)
        target[at : at + NORM_ROWS, :] = (wide * scale * gain).astype(BF16)


def kernel(
    n_st,
    n_tp,
    tokens,
    pre_gain,
    w_gated,
    w_mixed,
    mix_weight,
    w_query,
    w_gate_mix,
    w_gate_read,
    store,
    mem_gain,
    w_key,
    w_value,
    ids,
    w_out_mix,
    w_out_read,
    out,
    tok,
    gains,
    own_ids,
    slot_of,
    normed,
    wg,
    wm,
    wgm,
    mixw,
    wq,
    wgr,
    wkv,
    wom,
    wor,
    rows_in,
    norm_even,
    norm_odd,
    key_of,
    value_of,
    q_ring,
    q_sib,
    ids_all,
    o_send,
    s_send,
    ret_o,
    ret_s,
    gate_t,
    out_mix,
    out_read,
    part,
    rs_send,
    rs_recv,
    in_sem,
    row_sem,
    ids_send_sem,
    ids_recv_sem,
    ring_send_sem,
    ring_recv_sem,
    two_recv_sem,
    sib_send_sem,
    sib_recv_sem,
    ret_send_sem,
    ret_recv_sem,
    stat_send_sem,
    stat_recv_sem,
    rs_send_sem,
    rs_recv_sem,
):
    grp, st, tp = lax.axis_index("grp"), lax.axis_index("st"), lax.axis_index("tp")
    n_y = n_st // 2
    half_tp = n_tp // 2
    y, core = st // 2, lax.rem(st, 2)
    count = tok.shape[0]
    blocks = count // RBLOCK
    per_owner = rows_in.shape[0]
    mine_rows = count // n_tp

    def at_y(offset, sibling=False):
        chip = lax.rem(y + offset + n_y, n_y)
        return chip * 2 + (1 - core if sibling else core)

    def along_tp(offset):
        return lax.rem(tp + offset + n_tp, n_tp)

    def fetch(k, source, target):
        copy = pltpu.make_async_copy(source, target, in_sem.at[k])
        copy.start()
        return copy

    got_tok = fetch(0, tokens, tok)
    got_pre = fetch(11, pre_gain, gains.at[0])
    got_wq = fetch(1, w_query, wq)
    got_ids = fetch(12, ids, own_ids)

    barrier = pltpu.get_barrier_semaphore()
    peers = [(grp, lax.rem(st + k, n_st), tp) for k in range(1, n_st)]
    sides = [1, -1] if n_tp > 2 else [1]
    peers += [(grp, st, along_tp(k)) for k in sides]
    for peer in peers:
        pl.semaphore_signal(barrier, inc=1, device_id=peer, device_id_type=MESH)

    got_wk = fetch(2, w_key, wkv.at[:, 0:HD])
    got_wv = fetch(3, w_value, wkv.at[:, HD : 2 * HD])
    got_mem = fetch(13, mem_gain, gains.at[1])
    for p in range(per_owner):
        pltpu.make_async_copy(store.at[p], rows_in.at[p], row_sem.at[p]).start()
    got_wm = fetch(4, w_mixed, wm)
    got_wg = fetch(5, w_gated, wg)
    got_wgm = fetch(6, w_gate_mix, wgm)
    got_wgr = fetch(7, w_gate_read, wgr)
    got_mixw = fetch(8, mix_weight.at[0], mixw)
    got_wom = fetch(9, w_out_mix, wom)
    got_wor = fetch(10, w_out_read, wor)

    got_pre.wait()
    got_tok.wait()
    got_wq.wait()
    cut = blocks // 2
    half = cut * RBLOCK
    for h in range(2):
        rows = slice(h * half, (h + 1) * half)
        row_norm(tok, gains[0].reshape(1, -1), normed, h * half, (h + 1) * half)
        own_q = dot(normed[rows, :], wq[...]).astype(BF16)
        q_ring[0][h * cut : (h + 1) * cut] = own_q.reshape(cut, RBLOCK, HD)
    got_ids.wait()

    pl.semaphore_wait(barrier, len(peers))

    for k in range(1, n_st):
        pltpu.make_async_remote_copy(
            own_ids, ids_all.at[st], ids_send_sem, ids_recv_sem,
            device_id=(grp, lax.rem(st + k, n_st), tp), device_id_type=MESH,
        ).start()

    def drain(like, sem):
        pltpu.make_async_copy(like, like, sem).wait()

    def push(j, after, h, offset):
        piece = pl.ds(h * cut, cut)
        recv = two_recv_sem.at[after // 4, h] if after in (2, n_y - 2) else ring_recv_sem.at[after]
        pltpu.make_async_remote_copy(
            q_ring[j].at[piece], q_ring[after].at[piece], ring_send_sem, recv,
            device_id=(grp, at_y(offset), tp), device_id_type=MESH,
        ).start()

    def across(j):
        pltpu.make_async_remote_copy(
            q_ring[j], q_sib[j], sib_send_sem, sib_recv_sem.at[j],
            device_id=(grp, at_y(0, True), tp), device_id_type=MESH,
        ).start()

    for h in range(2):
        push(0, 2, h, 2)
        push(0, n_y - 2, 1 - h, -2)
    for h in range(2):
        push(0, 1, h, 1)
        push(0, n_y - 1, 1 - h, -1)
    across(0)

    for b in range(blocks):
        for n in range(NPB):
            ids_all[st, b, n] = own_ids[b, n]

    got_wk.wait()
    got_wv.wait()
    got_mem.wait()
    mem_row = gains[1].reshape(1, -1)

    def norm_of(p, target):
        row_norm(rows_in.at[p], mem_row, target, 0, PROWS)

    def keys_of(p, source):
        both = dot(source[...], wkv[...])
        key_of[p] = both[:, :HD].astype(BF16)
        value_of[p] = jnp.transpose(both[:, HD:]).astype(BF16)

    def row_wait(p):
        pltpu.make_async_copy(store.at[p], rows_in.at[p], row_sem.at[p]).wait()

    row_wait(0)
    norm_of(0, norm_even)

    def two(i, carry):
        row_wait(2 * i + 1)
        row_wait(2 * i + 2)
        keys_of(2 * i, norm_even)
        norm_of(2 * i + 1, norm_odd)
        keys_of(2 * i + 1, norm_odd)
        norm_of(2 * i + 2, norm_even)
        return carry

    lax.fori_loop(0, per_owner // 2 - 1, two, 0)
    row_wait(per_owner - 1)
    keys_of(per_owner - 2, norm_even)
    norm_of(per_owner - 1, norm_odd)
    keys_of(per_owner - 1, norm_odd)

    lanes = lax.broadcasted_iota(jnp.int32, (1, 2 * RBLOCK), 1)
    first_half = lanes < RBLOCK

    def attend(q_ref, reader):
        p0, p1, b0, b1 = (slot_of[reader, k] for k in range(4))
        q = jnp.concatenate([q_ref[b0], q_ref[b1]], axis=0)
        over_keys = ((1,), (1,))
        scores = jnp.where(
            first_half, dot(key_of[p0], q, over_keys), dot(key_of[p1], q, over_keys)
        ) * (HD ** (-0.5))
        top = jnp.max(scores, axis=0, keepdims=True)
        weight = jnp.exp(scores - top)
        total = jnp.sum(weight, axis=0, keepdims=True)
        weight = weight.astype(BF16)
        read = jnp.where(first_half, dot(value_of[p0], weight), dot(value_of[p1], weight))
        return read.astype(BF16), jnp.concatenate([top, total], axis=0)

    def serve(*labels):
        for j, sibling in labels:
            if sibling:
                drain(q_sib[j], sib_recv_sem.at[j])
        readers = [at_y(-j, sibling) for j, sibling in labels]
        results = [
            attend(q_sib[j] if sibling else q_ring[j], reader)
            for (j, sibling), reader in zip(labels, readers)
        ]
        for (j, sibling), (read, stats) in zip(labels, results):
            if j == 0 and not sibling:
                ret_o[st] = read
                ret_s[st] = stats
            else:
                o_send[j * 2 + sibling] = read
                s_send[j * 2 + sibling] = stats
        for source, target, send, recv in (
            (o_send, ret_o, ret_send_sem, ret_recv_sem),
            (s_send, ret_s, stat_send_sem, stat_recv_sem),
        ):
            for (j, sibling), reader in zip(labels, readers):
                if j == 0 and not sibling:
                    continue
                label = j * 2 + sibling
                pltpu.make_async_remote_copy(
                    source.at[label], target.at[st], send, recv,
                    device_id=(grp, reader, tp), device_id_type=MESH,
                ).start()

    def forward(i):
        for j, near, h, sign in ((2, 3, i, 1), (n_y - 2, n_y - 3, 1 - i, -1)):
            drain(q_ring[j].at[pl.ds(h * cut, cut)], two_recv_sem.at[j // 4, h])
            if i == 0:
                push(j, 4, h, 2 * sign)
            push(j, near, h, sign)

    forward(0)

    drain(ids_all.at[pl.ds(0, n_st - 1)], ids_recv_sem)

    def slots(reader, carry):
        first = last = jnp.int32(0)
        codes = []
        for b in range(blocks):
            for n in range(NPB):
                local = ids_all[reader, b, n] - st * per_owner
                mine = (local >= 0) & (local < per_owner)
                code = local * blocks + b
                last = jnp.where(mine, code, last)
                codes.append((mine, code))
        for mine, code in reversed(codes):
            first = jnp.where(mine, code, first)
        slot_of[reader, 0] = first // blocks
        slot_of[reader, 1] = last // blocks
        slot_of[reader, 2] = lax.rem(first, blocks)
        slot_of[reader, 3] = lax.rem(last, blocks)
        return carry

    lax.fori_loop(0, n_st, slots, 0, unroll=4)

    forward(1)
    for j in (1, n_y - 1):
        drain(q_ring[j], ring_recv_sem.at[j])
        across(j)
    for j in (2, n_y - 2):
        across(j)

    serve((1, 0), (n_y - 1, 0), (2, 0), (n_y - 2, 0))
    serve((1, 1), (n_y - 1, 1), (2, 1), (n_y - 2, 1))

    for j in (3, n_y - 3, 4):
        drain(q_ring[j], ring_recv_sem.at[j])
        across(j)
    serve((4, 0), (3, 0), (n_y - 3, 0))
    serve((4, 1), (3, 1), (n_y - 3, 1))
    serve((0, 0), (0, 1))

    got_wm.wait()
    over_width = ((1,), (1,))
    mixed_in = dot(normed[...], wm[...], over_width)
    centred = mixed_in - jnp.mean(mixed_in, axis=-1, keepdims=True)
    variance = jnp.mean(centred * centred, axis=-1, keepdims=True)
    mixed_norm = (centred * lax.rsqrt(variance + eps)).astype(BF16)
    got_mixw.wait()
    row_at = lax.broadcasted_iota(jnp.int32, (SPAN, SPAN), 0)
    col_at = lax.broadcasted_iota(jnp.int32, (SPAN, SPAN), 1)
    causal = jnp.where(col_at <= row_at, mixw[...].astype(F32), 0.0).astype(BF16)
    spatial = jnp.concatenate(
        [dot(causal, mixed_norm[n * SPAN : (n + 1) * SPAN]) for n in range(count // SPAN)], axis=0
    )
    got_wg.wait()
    branch_mix = dot(normed[...], wg[...], over_width) * spatial
    got_wgm.wait()
    gate = dot(normed[...], wgm[...], over_width)
    out_mix[...] = (branch_mix * (gate / (1.0 + jnp.exp(-gate)))).astype(BF16)
    got_wgr.wait()
    gate = dot(normed[...], wgr[...])
    gate_t[...] = jnp.transpose(gate / (1.0 + jnp.exp(-gate)))
    got_wom.wait()
    width = part.shape[2]
    for c in range(PIECES):
        part[c] = dot(out_mix[...], wom[:, c * width : (c + 1) * width])

    owners, ranks = [], []
    for e in range(blocks * NPB):
        owner = own_ids[e // NPB, e % NPB] // per_owner
        rank = jnp.int32(0)
        for before in owners:
            rank = rank + jnp.where(before == owner, 1, 0)
        owners.append(owner)
        ranks.append(rank)
    drain(ret_o.at[pl.ds(0, n_st - 1)], ret_recv_sem)
    drain(ret_s.at[pl.ds(0, n_st - 1)], stat_recv_sem)
    got_wor.wait()
    for pair in range(blocks // 2):
        tops, totals, reads = [], [], []
        for n in range(NPB):
            e0, e1 = pair * 2 * NPB + n, (pair * 2 + 1) * NPB + n

            def placed(ref):
                x0, x1 = ref[owners[e0]].astype(F32), ref[owners[e1]].astype(F32)
                low = jnp.where(ranks[e0] == 0, x0, pltpu.roll(x0, RBLOCK, 1))
                high = jnp.where(ranks[e1] == 1, x1, pltpu.roll(x1, RBLOCK, 1))
                return jnp.where(first_half, low, high)

            stats = placed(ret_s)
            tops.append(stats[0:1])
            totals.append(stats[1:2])
            reads.append(placed(ret_o))
        top = functools.reduce(jnp.maximum, tops)
        scales = [jnp.exp(t - top) for t in tops]
        total = sum(s * t for s, t in zip(scales, totals))
        read = sum(s * r for s, r in zip(scales, reads)) / total
        cols = slice(pair * 2 * RBLOCK, (pair + 1) * 2 * RBLOCK)
        out_read[cols, :] = jnp.transpose(read * gate_t[:, cols]).astype(BF16)

    rs_copies = {}

    def pass_on(c, d, k):
        sign = 1 - 2 * d
        target = along_tp(sign * k)
        lo = 0
        size = mine_rows
        if k == half_tp:
            size = mine_rows // 2
            lo = d * size
        start = pl.multiple_of(target * mine_rows + lo, mine_rows // 2)
        value = part[c, pl.ds(start, size), :]
        if k == half_tp:
            added = first[lo : lo + size, c * width : (c + 1) * width]
            rs_send[k - 1, d, c, lo : lo + size, :] = (value + added).astype(BF16)
        else:
            rs_copies[c, d, k + 1].wait_recv()
            if k + 1 == half_tp:
                cut_rows = mine_rows // 2
                low = d * cut_rows
                rs_send[k - 1, d, c, low : low + cut_rows, :] = (
                    part[c, pl.ds(pl.multiple_of(target * mine_rows + low, cut_rows), cut_rows), :]
                    + rs_recv[k, d, c, low : low + cut_rows, :].astype(F32)
                ).astype(BF16)
                other = cut_rows - low
                rs_send[k - 1, d, c, other : other + cut_rows, :] = part[
                    c, pl.ds(pl.multiple_of(target * mine_rows + other, cut_rows), cut_rows), :
                ].astype(BF16)
            else:
                rs_send[k - 1, d, c] = (value + rs_recv[k, d, c].astype(F32)).astype(BF16)
        copy = pltpu.make_async_remote_copy(
            rs_send.at[k - 1, d, c, pl.ds(lo, size)], rs_recv.at[k - 1, d, c, pl.ds(lo, size)],
            rs_send_sem.at[k // half_tp], rs_recv_sem.at[k - 1, d, c],
            device_id=(grp, st, along_tp(sign)), device_id_type=MESH,
        )
        copy.start()
        rs_copies[c, d, k] = copy

    start = pl.multiple_of(along_tp(half_tp) * mine_rows, mine_rows)
    first = dot(out_read[pl.ds(start, mine_rows), :], wor[...])
    for c in range(PIECES):
        for d in range(2):
            pass_on(c, d, half_tp)
    for c in range(PIECES):
        part[c] = part[c] + dot(out_read[...], wor[:, c * width : (c + 1) * width])
    for k in range(half_tp - 1, 0, -1):
        for c in range(PIECES):
            for d in range(2):
                pass_on(c, d, k)
    here = pl.ds(pl.multiple_of(tp * mine_rows, mine_rows), mine_rows)
    for c in range(PIECES):
        for d in range(2):
            rs_copies[c, d, 1].wait_recv()
        if half_tp == 1:
            cut_rows = mine_rows // 2
            both = jnp.concatenate(
                [rs_recv[0, 0, c, :cut_rows, :], rs_recv[0, 1, c, cut_rows:, :]], axis=0
            ).astype(F32)
        else:
            both = rs_recv[0, 0, c].astype(F32) + rs_recv[0, 1, c].astype(F32)
        out[:, c * width : (c + 1) * width] = (part[c, here, :] + both).astype(BF16)

    drain(ids_all.at[pl.ds(0, n_st - 1)], ids_send_sem)
    drain(o_send.at[pl.ds(0, 2 * (n_y - 1))], ring_send_sem)
    drain(o_send, sib_send_sem)
    drain(o_send.at[pl.ds(0, n_st - 1)], ret_send_sem)
    drain(s_send.at[pl.ds(0, n_st - 1)], stat_send_sem)
    drain(rs_send.at[half_tp - 1, 0], rs_send_sem.at[1])
    if half_tp > 1:
        drain(rs_send.at[pl.ds(0, half_tp - 1)], rs_send_sem.at[0])


def local(*args, n_st, n_tp):
    args = [a.T if k in (2, 3, 6) else a for k, a in enumerate(args)]
    tokens, w_gated, store = args[0], args[2], args[8]
    count, width = tokens.shape
    mix_width = w_gated.shape[0]
    held = store.shape[0]
    blocks = count // RBLOCK
    n_y = n_st // 2
    mine_rows = count // n_tp
    hbm = pl.BlockSpec(memory_space=pltpu.HBM)
    vmem = pl.BlockSpec(memory_space=pltpu.VMEM)
    specs = [hbm] * 15
    dma = pltpu.SemaphoreType.DMA
    columns = width // PIECES
    scratch = dict(
        tok=pltpu.VMEM((count, width), BF16),
        gains=pltpu.VMEM((2, width), F32),
        own_ids=pltpu.SMEM((blocks, NPB), jnp.int32),
        slot_of=pltpu.SMEM((n_st, 4), jnp.int32),
        normed=pltpu.VMEM((count, width), BF16),
        wg=pltpu.VMEM((mix_width, width), BF16),
        wm=pltpu.VMEM((mix_width, width), BF16),
        wgm=pltpu.VMEM((mix_width, width), BF16),
        mixw=pltpu.VMEM((SPAN, SPAN), BF16),
        wq=pltpu.VMEM((width, HD), BF16),
        wgr=pltpu.VMEM((width, HD), BF16),
        wkv=pltpu.VMEM((width, 2 * HD), BF16),
        wom=pltpu.VMEM((mix_width, width), BF16),
        wor=pltpu.VMEM((HD, width), BF16),
        rows_in=pltpu.VMEM((held, PROWS, width), BF16),
        norm_even=pltpu.VMEM((PROWS, width), BF16),
        norm_odd=pltpu.VMEM((PROWS, width), BF16),
        key_of=pltpu.VMEM((held, PROWS, HD), BF16),
        value_of=pltpu.VMEM((held, HD, PROWS), BF16),
        q_ring=[pltpu.VMEM((blocks, RBLOCK, HD), BF16) for _ in range(n_y)],
        q_sib=[pltpu.VMEM((blocks, RBLOCK, HD), BF16) for _ in range(n_y)],
        ids_all=pltpu.SMEM((n_st, blocks, NPB), jnp.int32),
        o_send=pltpu.VMEM((n_st, HD, 2 * RBLOCK), BF16),
        s_send=pltpu.VMEM((n_st, 2, 2 * RBLOCK), F32),
        ret_o=pltpu.VMEM((n_st, HD, 2 * RBLOCK), BF16),
        ret_s=pltpu.VMEM((n_st, 2, 2 * RBLOCK), F32),
        gate_t=pltpu.VMEM((HD, count), F32),
        out_mix=pltpu.VMEM((count, mix_width), BF16),
        out_read=pltpu.VMEM((count, HD), BF16),
        part=pltpu.VMEM((PIECES, count, columns), F32),
        rs_send=pltpu.VMEM((n_tp // 2, 2, PIECES, mine_rows, columns), BF16),
        rs_recv=pltpu.VMEM((n_tp // 2, 2, PIECES, mine_rows, columns), BF16),
        in_sem=dma((14,)),
        row_sem=dma((held,)),
        ids_send_sem=dma,
        ids_recv_sem=dma,
        ring_send_sem=dma,
        ring_recv_sem=dma((n_y,)),
        two_recv_sem=dma((2, 2)),
        sib_send_sem=dma,
        sib_recv_sem=dma((n_y,)),
        ret_send_sem=dma,
        ret_recv_sem=dma,
        stat_send_sem=dma,
        stat_recv_sem=dma,
        rs_send_sem=dma((2,)),
        rs_recv_sem=dma((n_tp // 2, 2, PIECES)),
    )
    names = list(scratch)

    def body(*refs):
        kernel(n_st, n_tp, *refs[:16], **dict(zip(names, refs[16:])))

    return pl.pallas_call(
        body,
        out_shape=pltpu.VMEM((mine_rows, width), BF16),
        in_specs=specs,
        out_specs=vmem,
        scratch_shapes=list(scratch.values()),
        compiler_params=pltpu.CompilerParams(
            collective_id=0, has_side_effects=True, vmem_limit_bytes=66_800_000
        ),
        name="layer",
    )(*args)


def solution(mesh):
    placed = (
        P(("grp", "st"), None),
        P(),
        P(None, "tp"),
        P(None, "tp"),
        P("tp", None, None),
        P(None, "tp"),
        P(None, "tp"),
        P(None, "tp"),
        P(("grp", "st"), None, None),
        P(),
        P(None, "tp"),
        P(None, "tp"),
        P(("grp", "st"), None),
        P("tp", None),
        P("tp", None),
    )
    body = functools.partial(local, n_st=mesh.shape["st"], n_tp=mesh.shape["tp"])
    return jax.shard_map(
        body, mesh=mesh, in_specs=placed, out_specs=P(("grp", "st", "tp"), None), check_vma=False
    )
```
